512 devices in a mesh: sp: 32 (over z, x), tp: 16 (over y, core).
Axes of the slice: x: 4, y: 8, z: 8, core: 2. Of those that a mesh axis runs over, the one named last changes fastest.
Arguments:
- resid: bfloat16 [4096, 2048], P('sp'), may hold values from -8 to 8
- a_val: bfloat16 [4096, 1024], P('sp', 'tp'), may hold values from -8 to 8
- a_gate: bfloat16 [4096, 1024], P('sp', 'tp'), may hold values from -6 to 6
- conv_kernel: bfloat16 [31, 1024], P(None, 'tp'), may hold values from -1 to 1
- conv_bias: float32 [1024], P('tp'), may hold values from -3 to 3
- ln_gain: float32 [1024], P('tp'), may hold values from 0.1 to 1.9
- ln_bias: float32 [1024], P('tp'), may hold values from -3 to 3
- w_out: bfloat16 [1024, 2048], P('tp'), may hold values from -0.1875 to 0.1875
- ffn_gain: float32 [2048], replicated, may hold values from 0.1 to 1.9
- routes: int32 [4096, 4], P('sp'), may hold values from 0 to 31, all different within a row; in each aligned block of 128 rows (0 to 127, 128 to 255, ...) at most 32 rows name the same one
- route_weights: float32 [4096, 4], P('sp'), may hold values from 0.15 to 1.2
- exp_gate: bfloat16 [32, 2048, 4096], P('sp', None, 'tp'), may hold values from -0.125 to 0.125
- exp_up: bfloat16 [32, 2048, 4096], P('sp', None, 'tp'), may hold values from -0.125 to 0.125
- exp_down: bfloat16 [32, 4096, 2048], P('sp', None, 'tp'), may hold values from -0.09375 to 0.09375
- sh_gate: bfloat16 [2048, 512], P(None, 'tp'), may hold values from -0.125 to 0.125
- sh_up: bfloat16 [2048, 512], P(None, 'tp'), may hold values from -0.125 to 0.125
- sh_down: bfloat16 [512, 2048], P(None, 'tp'), may hold values from -0.25 to 0.25
Outputs:
- result: bfloat16 [4096, 2048], P('sp', 'tp')
The draws below stay inside these ranges and needn't reach their ends.
Inputs may be any that keep to these rules, and one draw needn't show every extreme that they name: `routes`: among the 128 rows of one index of sp, each expert is named at most 32 times, a bound that some block reaches; a row names 4 different experts.
All inputs are finite; a program needn't handle non-finite values.
Results may differ from the reference program's by a relative error of at most 0.007.
Values may be sent and summed in bfloat16 or wider, within the bound.
No kernel may reach another device: no remote copies, remote signals or barrier semaphores. Data moves between devices by JAX's collectives and lax.ppermute only.
A program may use at most 64 MiB of HBM per device.

```python
import math
import jax
import jax.numpy as jnp
import numpy as np
from jax import lax

D = 2048
D_A = 1024
D_E = 4096
D_S = 512
CONV_SPAN = 31
TOPK = 4
TOK_SP = 128
EXPERTS = 32
TOKENS = 4096
CAP = 32
N_SP = 32


def rising_field(key, row_count, col_count, lowest, growth):
    subkeys = jax.random.split(jax.random.fold_in(key, 11), 2)
    position = jnp.arange(col_count, dtype=jnp.float32) / col_count
    roughness = jnp.exp(jax.random.uniform(subkeys[1], (col_count,), jnp.float32, -0.35, 0.35))
    values = jax.random.normal(subkeys[0], (row_count, col_count), jnp.float32)
    drawn = values * (lowest * growth ** position * roughness)[None, :]
    return jnp.clip(drawn, -8.0, 8.0)


def draw_resid(key, part):
    return rising_field(jax.random.fold_in(key, 3), TOKENS, D, 0.5, 3.0).astype(jnp.bfloat16)


def draw_a_val(key, part):
    return rising_field(jax.random.fold_in(key, 5), TOKENS, D_A, 0.5, 3.0).astype(jnp.bfloat16)


def shard_levels(rng, dims, cuts, low, top_value):
    level = 1.0
    for axis_at, shards_of in cuts:
        steps = jax.random.uniform(jax.random.fold_in(jax.random.fold_in(rng, 6), axis_at), (shards_of,), jnp.float32, low / len(cuts), top_value / len(cuts))
        level = level * jnp.repeat(jnp.exp(steps), dims[axis_at] // shards_of).reshape((-1,) + (1,) * (len(dims) - 1 - axis_at))
    return level


def deal_out(rng, own, number, rows, amount, top, limit, skew):
    order = jax.random.permutation(rng, amount)
    crowded, usual = load_shares(amount, rows * top, limit, skew, True), load_shares(amount, rows * top, limit, skew, False)
    places = jnp.arange(amount)

    def named(tallies, offset_by):
        used = int((tallies > 0).sum())
        fixed = max(1, used // 4)
        passed = fixed + (places - fixed + offset_by * (used - fixed)) % max(1, amount - fixed)
        return jnp.zeros((amount,), jnp.int32).at[order[jnp.where(places < fixed, places, passed)]].set(jnp.asarray(tallies, jnp.int32))

    tallies = jnp.where(number % 4 == 0, named(crowded, number // 4), named(usual, number - number // 4 - 1))
    mixed = jax.random.permutation(jax.random.fold_in(own, 3), amount)
    source_of, sink = mixed[0:amount // 2 * 2:2], mixed[1:amount // 2 * 2:2]
    margin = jnp.minimum(tallies[source_of] - 1, limit - tallies[sink]) // 2
    margin = jnp.where((source_of == order[0]) | (sink == order[0]) | (tallies[sink] == 0), 0, jnp.maximum(margin, 0))
    passed = jax.random.randint(jax.random.fold_in(own, 4), (amount // 2,), 0, 1 << 20) % (margin + 1)
    tallies = tallies.at[source_of].add(-passed).at[sink].add(passed)
    labels = jnp.searchsorted(jnp.cumsum(tallies), jnp.arange(rows * top), side="right").astype(jnp.int32)
    table = labels.reshape(top, rows).T
    table = table[jax.random.permutation(jax.random.fold_in(own, 1), rows)]
    offset_by = jax.random.randint(jax.random.fold_in(own, 2), (rows, 1), 0, top)
    return jnp.take_along_axis(table, (jnp.arange(top)[None, :] + offset_by) % top, axis=1)


def load_shares(count, total, limit, lean, full):
    weights = [(1 << 20) // math.isqrt(grade ** lean) + 1 for grade in range(1, count + 1)]
    largest = limit if full else min(limit, max(-(-total // count), total * weights[0] // sum(weights)))
    least = 1 if total - largest >= count - 1 else 0
    holding, spare = [largest] + [least] * (count - 1), total - largest - least * (count - 1)
    while spare > 0:
        movable = [i for i in range(1, count) if holding[i] < largest] or [i for i in range(1, count) if holding[i] < limit]
        pool, remaining = sum([weights[i] for i in movable]), spare
        for i in movable:
            addition = min(limit - holding[i], max(1, remaining * weights[i] // pool), spare)
            holding[i] = holding[i] + addition
            spare = spare - addition
    return np.array(holding)


def normal_values(key, shape, spread, limit, cuts=(), kind=jnp.bfloat16):
    values = jax.random.normal(key, shape, jnp.float32) * spread
    if len(cuts) > 0:
        values = shard_levels(key, shape, cuts, -0.22, 0.18) * values
    return jnp.clip(values, min=-limit, max=limit).astype(kind)


def setup_inputs(seed: int = 0) -> dict:
    streams_of = jax.random.split(jax.random.key(seed), 18)
    resid = draw_resid(jax.random.fold_in(streams_of[17], 71), 0)
    a_val = draw_a_val(jax.random.fold_in(streams_of[17], 71), 0)
    a_gate = normal_values(streams_of[2], (TOKENS, D_A), 1.0, 6.0, ((0, 32), (1, 16)))
    conv_kernel = normal_values(streams_of[3], (CONV_SPAN, D_A), CONV_SPAN ** -0.5, 1.0, ((1, 16),))
    conv_bias = normal_values(streams_of[4], (D_A,), 0.5, 3.0, ((0, 16),), jnp.float32)
    ln_gain = jnp.clip(1.0 + 0.18 * jax.random.normal(streams_of[5], (D_A,), jnp.float32), 0.1, 1.9)
    ln_bias = normal_values(streams_of[6], (D_A,), 0.5, 3.0, ((0, 16),), jnp.float32)
    w_out = normal_values(streams_of[7], (D_A, D), D_A ** -0.5, 0.1875, ((0, 16),))
    ffn_gain = jnp.clip(1.0 + 0.18 * jax.random.normal(streams_of[8], (D,), jnp.float32), 0.1, 1.9)
    routes_keys = jax.random.split(jax.random.fold_in(streams_of[9], 1), TOKENS // TOK_SP)
    routes_turns = jax.random.permutation(jax.random.fold_in(streams_of[9], 3), TOKENS // TOK_SP)
    routes = jax.vmap(lambda own, number: deal_out(jax.random.fold_in(streams_of[9], 2), own, number, TOK_SP, EXPERTS, TOPK, CAP, 1))(routes_keys, routes_turns).reshape((TOKENS, TOPK))
    route_weights = jnp.clip(jnp.exp(math.log(1.2) - 2.0794415 * jax.random.uniform(streams_of[10], (TOKENS, TOPK), jnp.float32) ** shard_levels(streams_of[10], (TOKENS, TOPK), ((0, 32),), -0.2, 0.2)), 0.15, 1.2)
    exp_gate = normal_values(streams_of[11], (EXPERTS, D, D_E), D ** -0.5, 0.125, ((0, 32), (2, 16)))
    exp_up = normal_values(streams_of[12], (EXPERTS, D, D_E), D ** -0.5, 0.125, ((0, 32), (2, 16)))
    exp_down = normal_values(streams_of[13], (EXPERTS, D_E, D), D_E ** -0.5, 0.09375, ((0, 32), (2, 16)))
    sh_gate = normal_values(streams_of[14], (D, D_S), D ** -0.5, 0.125, ((1, 16),))
    sh_up = normal_values(streams_of[15], (D, D_S), D ** -0.5, 0.125, ((1, 16),))
    sh_down = normal_values(streams_of[16], (D_S, D), D_S ** -0.5, 0.25, ((1, 16),))
    return dict(resid=resid, a_val=a_val, a_gate=a_gate, conv_kernel=conv_kernel, conv_bias=conv_bias, ln_gain=ln_gain, ln_bias=ln_bias, w_out=w_out, ffn_gain=ffn_gain, routes=routes, route_weights=route_weights, exp_gate=exp_gate, exp_up=exp_up, exp_down=exp_down, sh_gate=sh_gate, sh_up=sh_up, sh_down=sh_down)


LN_EPS = 1e-05
RMS_EPS = 1e-06

def reference(resid, a_val, a_gate, conv_kernel, conv_bias, ln_gain, ln_bias, w_out, ffn_gain, routes, route_weights, exp_gate, exp_up, exp_down, sh_gate, sh_up, sh_down):
    gated_in = (a_val.astype(jnp.float32) * jax.nn.sigmoid(a_gate.astype(jnp.float32))).astype(jnp.bfloat16)
    padded = jnp.pad(gated_in, ((CONV_SPAN - 1, 0), (0, 0))).astype(jnp.float32)
    kernel = conv_kernel.astype(jnp.float32)

    def add_tap(offset, running):
        window_rows = lax.dynamic_slice_in_dim(padded, offset, TOKENS, 0)
        return running + lax.dynamic_slice_in_dim(kernel, offset, 1, 0) * window_rows
    start_sum = jnp.broadcast_to(conv_bias[None, :], (TOKENS, D_A)).astype(jnp.float32)
    conv_out = lax.fori_loop(0, CONV_SPAN, add_tap, start_sum)
    channel_mean = lax.optimization_barrier(jnp.mean(conv_out, axis=1, keepdims=True))
    channel_var = lax.optimization_barrier(jnp.mean(conv_out * conv_out, axis=1, keepdims=True)) - channel_mean * channel_mean
    scaled = (conv_out - channel_mean) * lax.rsqrt(channel_var + LN_EPS) * ln_gain[None, :] + ln_bias[None, :]
    mixed_out = jax.nn.silu(scaled).astype(jnp.bfloat16)
    projected = jnp.dot(mixed_out, w_out, preferred_element_type=jnp.float32)
    middle = (resid.astype(jnp.float32) + projected).astype(jnp.bfloat16)
    middle_f = middle.astype(jnp.float32)
    inverse = lax.rsqrt(lax.optimization_barrier(jnp.mean(middle_f * middle_f, axis=1, keepdims=True)) + RMS_EPS)
    normed = (middle_f * inverse * ffn_gain[None, :]).astype(jnp.bfloat16)
    shared_gate = jnp.dot(normed, sh_gate, preferred_element_type=jnp.float32)
    shared_up = jnp.dot(normed, sh_up, preferred_element_type=jnp.float32)
    shared_hidden = (jax.nn.silu(shared_gate) * shared_up).astype(jnp.bfloat16)
    shared = jnp.dot(shared_hidden, sh_down, preferred_element_type=jnp.float32)
    pair_count = TOK_SP * TOPK
    chosen_all = routes.reshape(N_SP, pair_count)
    expert_ids = jnp.arange(EXPERTS, dtype=jnp.int32)

    def block_places(chosen):
        one_hot = (chosen[:, None] == expert_ids[None, :]).astype(jnp.int32)
        earlier = jnp.cumsum(one_hot, axis=0) - one_hot
        return lax.optimization_barrier(jnp.sum(earlier * one_hot, axis=1)).astype(jnp.int32)
    place_in = lax.map(block_places, chosen_all)
    source_ids = jnp.arange(N_SP, dtype=jnp.int32)[:, None]
    target = source_ids * (EXPERTS * CAP) + chosen_all * CAP + place_in
    pair_ids = source_ids * pair_count + jnp.arange(pair_count, dtype=jnp.int32)[None, :]
    owner_ids = jnp.zeros((N_SP * EXPERTS * CAP,), jnp.int32).at[target.reshape(-1)].set(pair_ids.reshape(-1) + 1)
    owner_ids = owner_ids.reshape(N_SP, EXPERTS, CAP).transpose(1, 0, 2)

    def run_expert(packed):
        owners, gate_weight, up_weight, down_weight = packed
        flat_owner = owners.reshape(-1)
        source_row = jnp.maximum(flat_owner - 1, 0) // TOPK
        rows_in = jnp.where((flat_owner > 0)[:, None], normed[source_row], jnp.zeros((), jnp.bfloat16))
        gate_part = jnp.dot(rows_in, gate_weight, preferred_element_type=jnp.float32)
        up_part = jnp.dot(rows_in, up_weight, preferred_element_type=jnp.float32)
        hidden = (jax.nn.silu(gate_part) * up_part).astype(jnp.bfloat16)
        return jnp.dot(hidden, down_weight, preferred_element_type=jnp.float32).astype(jnp.bfloat16)
    expert_out = lax.map(run_expert, (owner_ids, exp_gate, exp_up, exp_down))
    flat_index = (chosen_all * (N_SP * CAP) + source_ids * CAP + place_in).reshape(-1)
    flat_out = expert_out.reshape(EXPERTS * N_SP * CAP, D)
    routed = jnp.zeros((TOKENS, D), jnp.float32)
    index_grid = flat_index.reshape(TOKENS, TOPK)
    for choice_k in range(TOPK):
        picked = flat_out[index_grid[:, choice_k]].astype(jnp.float32)
        routed = routed + route_weights[:, choice_k][:, None] * picked
    return (middle_f + shared + routed).astype(jnp.bfloat16)
```

```python
import jax
import jax.numpy as jnp
from jax import lax
from jax.experimental import pallas as pl
from jax.experimental.pallas import tpu as pltpu
from jax.sharding import PartitionSpec as P

LN_EPS = 1e-05
RMS_EPS = 1e-06
LANES = 128
F32 = jnp.float32
BF16 = jnp.bfloat16


def rounded(value):
    return lax.reduce_precision(value, exponent_bits=8, mantissa_bits=7)


def in_three(value):
    high = rounded(value)
    mid = rounded(value - high)
    low = value - high - mid
    return high.astype(BF16), mid.astype(BF16), low.astype(BF16)


def silu(v):
    return v / (1.0 + jnp.exp(-v))


def front_kernel(span, packed, wcol, resid, slots, middle_out, send_out, win, conv):
    peers, rows, _ = packed.shape
    tok_rows = resid.shape[0]
    half = packed.shape[2] // 2
    channels = peers * half
    for pair in range(peers // 2):
        one, two = packed[2 * pair], packed[2 * pair + 1]
        at = pair * LANES
        left = jnp.concatenate([one[:, :half], two[:, :half]], axis=1)
        right = jnp.concatenate([one[:, half:], two[:, half:]], axis=1)
        win[0, :, at : at + LANES] = left.astype(F32)
        win[1, :, at : at + LANES] = right.astype(F32)

    def vector(first):
        high, mid, low = (win[1, first + i : first + i + 1, :] for i in range(3))
        return high + mid + low

    conv_rows = 64

    def one_block(i, _):
        cols = pl.ds(pl.multiple_of(i * LANES, LANES), LANES)
        taps = win[1, 0:span, cols]
        b = sum(win[1, span + n : span + n + 1, cols] for n in range(3))
        for r in range(0, tok_rows, conv_rows):
            acc = jnp.broadcast_to(b, (conv_rows, LANES))
            for j in range(span):
                acc = acc + taps[j : j + 1, :] * win[0, r + j : r + j + conv_rows, cols]
            conv[r : r + conv_rows, cols] = acc
        return 0

    lax.fori_loop(0, channels // LANES, one_block, 0)
    gain = vector(span + 3)
    shift = vector(span + 6)
    for r in range(0, tok_rows, 64):
        c = conv[r : r + 64, :]
        mean = jnp.sum(c, axis=1, keepdims=True) * (1.0 / channels)
        var = jnp.sum(c * c, axis=1, keepdims=True) * (1.0 / channels) - mean * mean
        scaled = (c - mean) * lax.rsqrt(var + LN_EPS) * gain + shift
        mixed = silu(scaled).astype(BF16)
        proj = jnp.dot(mixed, wcol[...], preferred_element_type=F32)
        middle_out[r : r + 64, :] = (resid[r : r + 64, :].astype(F32) + proj).astype(BF16)
    middle = middle_out[...]
    block = 256
    for r in range(0, send_out.shape[0], block):
        ids = lax.broadcasted_iota(jnp.int32, (block, tok_rows), 0) + r
        hit = ids == slots[0:1, :]
        for k in range(1, slots.shape[0]):
            hit = hit | (ids == slots[k : k + 1, :])
        pick = jnp.where(hit, 1.0, 0.0).astype(BF16)
        send_out[r : r + block, :] = jnp.dot(pick, middle, preferred_element_type=F32).astype(BF16)


def front(span, packed, wcol, resid, slots, slot_count):
    tok_rows, cols = resid.shape
    channels = packed.shape[0] * packed.shape[2] // 2

    def kernel(*refs):
        front_kernel(span, *refs)

    return pl.pallas_call(
        kernel,
        out_shape=(
            jax.ShapeDtypeStruct((tok_rows, cols), BF16),
            jax.ShapeDtypeStruct((slot_count, cols), BF16),
        ),
        scratch_shapes=[
            pltpu.VMEM((2, packed.shape[1], channels), F32),
            pltpu.VMEM((tok_rows, channels), F32),
        ],
        name="front",
    )(packed, wcol, resid, slots)


def hidden_kernel(width, rows_in, gain, wg, wu, out):
    pieces = rows_in.shape[0]
    squares = jnp.zeros((rows_in.shape[1], LANES), F32)
    for t in range(pieces):
        x = rows_in[t].astype(F32)
        squares = squares + x * x
    mean = jnp.sum(squares, axis=1, keepdims=True) / width
    inverse = lax.rsqrt(mean + RMS_EPS)
    normed = jnp.concatenate(
        [(rows_in[t].astype(F32) * inverse * gain[t : t + 1, :]).astype(BF16) for t in range(pieces)],
        axis=1,
    )
    g = jnp.dot(normed, wg[...], preferred_element_type=F32)
    u = jnp.dot(normed, wu[...], preferred_element_type=F32)
    out[...] = (silu(g) * u).astype(BF16)


def hidden_units(rows_in, gain, wg, wu):
    pieces, rows, lanes = rows_in.shape
    width, units = wg.shape
    block = 256

    def kernel(*refs):
        hidden_kernel(width, *refs)

    return pl.pallas_call(
        kernel,
        grid=(rows // block,),
        in_specs=[
            pl.BlockSpec((pieces, block, lanes), lambda i: (0, i, 0)),
            pl.BlockSpec((pieces, lanes), lambda i: (0, 0)),
            pl.BlockSpec((width, units), lambda i: (0, 0)),
            pl.BlockSpec((width, units), lambda i: (0, 0)),
        ],
        out_specs=pl.BlockSpec((block, units), lambda i: (i, 0)),
        out_shape=jax.ShapeDtypeStruct((rows, units), BF16),
        name="hidden",
    )(rows_in, gain, wg, wu)


def down_kernel(hidden, wd, out):
    whole = jnp.concatenate([hidden[t] for t in range(hidden.shape[0])], axis=1)
    out[...] = jnp.dot(whole, wd[...], preferred_element_type=F32).astype(BF16)


def down(hidden, wd):
    pieces, rows, units = hidden.shape
    block = 256
    return pl.pallas_call(
        down_kernel,
        grid=(rows // block,),
        in_specs=[
            pl.BlockSpec((pieces, block, units), lambda i: (0, i, 0)),
            pl.BlockSpec(wd.shape, lambda i: (0, 0)),
        ],
        out_specs=pl.BlockSpec((block, wd.shape[1]), lambda i: (i, 0)),
        out_shape=jax.ShapeDtypeStruct((rows, wd.shape[1]), BF16),
        name="down",
    )(hidden, wd)


def combine_kernel(returned, slots, weights, middle, shared, out):
    shape = (slots.shape[0], returned.shape[0])
    ids = lax.broadcasted_iota(jnp.int32, shape, 1)
    table = jnp.zeros(shape, F32)
    for k in range(slots.shape[1]):
        table = jnp.where(ids == slots[:, k : k + 1], weights[:, k : k + 1], table)
    routed = jnp.zeros(out.shape, F32)
    for _ in range(3):
        part = table.astype(BF16)
        routed = routed + jnp.dot(part, returned[...], preferred_element_type=F32)
        table = table - part.astype(F32)
    out[...] = (middle[...].astype(F32) + shared[...] + routed).astype(BF16)


def combine(returned, slots, weights, middle, shared):
    return pl.pallas_call(
        combine_kernel,
        out_shape=jax.ShapeDtypeStruct(middle.shape, BF16),
        name="combine",
    )(returned, slots, weights, middle, shared)


def body(
    resid,
    a_val,
    a_gate,
    conv_kernel,
    conv_bias,
    ln_gain,
    ln_bias,
    w_out,
    ffn_gain,
    routes,
    route_weights,
    exp_gate,
    exp_up,
    exp_down,
    sh_gate,
    sh_up,
    sh_down,
):
    tp_count = lax.axis_size("tp")
    tp_place = lax.axis_index("tp")
    sp_count = lax.axis_size("sp")
    tok_rows, model_width = resid.shape
    col_width = model_width // tp_count
    span = conv_kernel.shape[0]
    top_count = routes.shape[1]
    experts_all = exp_gate.shape[0] * sp_count
    capacity = max(2 * tok_rows * top_count // experts_all, tp_count)
    pair_count = tok_rows * top_count
    slot_count = experts_all * capacity

    w_parts = jnp.moveaxis(w_out.reshape(w_out.shape[0], tp_count, col_width), 1, 0)
    wcol = lax.all_to_all(w_parts, "tp", split_axis=0, concat_axis=0, tiled=True)
    wcol = wcol.reshape(w_out.shape[0] * tp_count, col_width)

    gated = (a_val.astype(F32) * jax.nn.sigmoid(a_gate.astype(F32))).astype(BF16)
    halo = span - 1
    pairs = [(i, i + 1) for i in range(sp_count - 1)]
    before = lax.ppermute(gated[tok_rows - halo :], "sp", pairs)
    rows = -(-(halo + tok_rows) // 16) * 16
    vectors = [p[None, :] for v in (conv_bias, ln_gain, ln_bias) for p in in_three(v)]
    right = jnp.concatenate([conv_kernel, *vectors], axis=0)
    right = jnp.pad(right, ((0, rows - right.shape[0]), (0, 0)))
    left = jnp.concatenate([before, gated], axis=0)
    left = jnp.pad(left, ((0, rows - left.shape[0]), (0, 0)))
    packed = lax.all_gather(jnp.concatenate([left, right], axis=1), "tp")

    chosen = routes.reshape(pair_count)
    one_hot = (chosen[:, None] == jnp.arange(experts_all, dtype=jnp.int32)[None, :]).astype(BF16)
    order = jnp.arange(pair_count, dtype=jnp.int32)
    below = (order[:, None] > order[None, :]).astype(BF16)
    earlier = jnp.dot(below, one_hot, preferred_element_type=F32)
    place_in = jnp.sum(earlier * one_hot.astype(F32), axis=1).astype(jnp.int32)
    slots = (chosen * capacity + place_in).reshape(tok_rows, top_count)

    resid_cols = lax.dynamic_slice_in_dim(resid, tp_place * col_width, col_width, 1)
    middle, send = front(span, packed, wcol, resid_cols, slots.T, slot_count)

    landed = lax.all_to_all(
        send.reshape(sp_count, slot_count // sp_count, col_width),
        "sp",
        split_axis=0,
        concat_axis=0,
        tiled=True,
    ).reshape(slot_count, col_width)
    gain = ffn_gain.reshape(tp_count, col_width)
    arrived = lax.all_gather(landed, "tp")
    hidden = hidden_units(arrived, gain, exp_gate[0], exp_up[0])

    middle_late, landed_late = lax.optimization_barrier((middle, landed[:1]))
    middle_all = lax.all_gather(middle_late, "tp")
    middle_f = jnp.moveaxis(middle_all, 0, 1).reshape(tok_rows, model_width).astype(F32)
    squares = jnp.sum(middle_f * middle_f, axis=1, keepdims=True)
    inverse = lax.rsqrt(squares / model_width + RMS_EPS)
    normed = (middle_f * inverse * ffn_gain[None, :]).astype(BF16)
    shared_gate = jnp.dot(normed, sh_gate, preferred_element_type=F32)
    shared_up = jnp.dot(normed, sh_up, preferred_element_type=F32)
    shared_hidden = (jax.nn.silu(shared_gate) * shared_up).astype(BF16)

    hidden_all = lax.all_gather(hidden, "tp")
    shared_late, _ = lax.optimization_barrier((shared_hidden, hidden[:1]))
    shared = jnp.dot(
        lax.all_gather(shared_late, "tp", axis=1, tiled=True),
        sh_down,
        preferred_element_type=F32,
    )
    hidden_all, shared = lax.optimization_barrier((hidden_all, shared))

    expert_out = down(hidden_all, exp_down[0])
    returned = lax.all_to_all(
        expert_out.reshape(sp_count, slot_count // sp_count, col_width),
        "sp",
        split_axis=0,
        concat_axis=0,
        tiled=True,
    ).reshape(slot_count, col_width)
    return combine(returned, slots, route_weights, middle, shared)


def solution(mesh):
    in_specs = (
        P("sp", None),
        P("sp", "tp"),
        P("sp", "tp"),
        P(None, "tp"),
        P("tp"),
        P("tp"),
        P("tp"),
        P("tp", None),
        P(),
        P("sp", None),
        P("sp", None),
        P("sp", None, "tp"),
        P("sp", None, "tp"),
        P("sp", None, "tp"),
        P(None, "tp"),
        P(None, "tp"),
        P(None, "tp"),
    )
    out_specs = P("sp", "tp")
    return jax.shard_map(body, mesh=mesh, in_specs=in_specs, out_specs=out_specs, check_vma=False)
```

```python
import jax
import jax.numpy as jnp
from jax import lax
from jax.experimental import pallas as pl
from jax.experimental.pallas import tpu as pltpu
from jax.sharding import PartitionSpec as P

LN_EPS = 1e-05
RMS_EPS = 1e-06
LANES = 128
F32 = jnp.float32
BF16 = jnp.bfloat16


def rounded(value):
    return lax.reduce_precision(value, exponent_bits=8, mantissa_bits=7)


def in_three(value):
    high = rounded(value)
    mid = rounded(value - high)
    low = value - high - mid
    return high.astype(BF16), mid.astype(BF16), low.astype(BF16)


def silu(v):
    return v / (1.0 + jnp.exp(-v))


def front_kernel(span, packed, wcol, resid, slots, middle_out, send_out, win, conv):
    peers, rows, _ = packed.shape
    tok_rows = resid.shape[0]
    half = packed.shape[2] // 2
    channels = peers * half
    for pair in range(peers // 2):
        one, two = packed[2 * pair], packed[2 * pair + 1]
        at = pair * LANES
        left = jnp.concatenate([one[:, :half], two[:, :half]], axis=1)
        right = jnp.concatenate([one[:, half:], two[:, half:]], axis=1)
        win[0, :, at : at + LANES] = left.astype(F32)
        win[1, :, at : at + LANES] = right.astype(F32)

    def vector(first):
        high, mid, low = (win[1, first + i : first + i + 1, :] for i in range(3))
        return high + mid + low

    conv_rows = 64

    def one_block(i, _):
        cols = pl.ds(pl.multiple_of(i * LANES, LANES), LANES)
        taps = win[1, 0:span, cols]
        b = sum(win[1, span + n : span + n + 1, cols] for n in range(3))
        for r in range(0, tok_rows, conv_rows):
            acc = jnp.broadcast_to(b, (conv_rows, LANES))
            for j in range(span):
                acc = acc + taps[j : j + 1, :] * win[0, r + j : r + j + conv_rows, cols]
            conv[r : r + conv_rows, cols] = acc
        return 0

    lax.fori_loop(0, channels // LANES, one_block, 0)
    gain = vector(span + 3)
    shift = vector(span + 6)
    for r in range(0, tok_rows, 64):
        c = conv[r : r + 64, :]
        mean = jnp.sum(c, axis=1, keepdims=True) * (1.0 / channels)
        var = jnp.sum(c * c, axis=1, keepdims=True) * (1.0 / channels) - mean * mean
        scaled = (c - mean) * lax.rsqrt(var + LN_EPS) * gain + shift
        mixed = silu(scaled).astype(BF16)
        proj = jnp.dot(mixed, wcol[...], preferred_element_type=F32)
        middle_out[r : r + 64, :] = (resid[r : r + 64, :].astype(F32) + proj).astype(BF16)
    middle = middle_out[...]
    block = 256
    for r in range(0, send_out.shape[0], block):
        ids = lax.broadcasted_iota(jnp.int32, (block, tok_rows), 0) + r
        hit = ids == slots[0:1, :]
        for k in range(1, slots.shape[0]):
            hit = hit | (ids == slots[k : k + 1, :])
        pick = jnp.where(hit, 1.0, 0.0).astype(BF16)
        send_out[r : r + block, :] = jnp.dot(pick, middle, preferred_element_type=F32).astype(BF16)


def front(span, packed, wcol, resid, slots, slot_count):
    tok_rows, cols = resid.shape
    channels = packed.shape[0] * packed.shape[2] // 2

    def kernel(*refs):
        front_kernel(span, *refs)

    return pl.pallas_call(
        kernel,
        out_shape=(
            jax.ShapeDtypeStruct((tok_rows, cols), BF16),
            jax.ShapeDtypeStruct((slot_count, cols), BF16),
        ),
        scratch_shapes=[
            pltpu.VMEM((2, packed.shape[1], channels), F32),
            pltpu.VMEM((tok_rows, channels), F32),
        ],
        name="front",
    )(packed, wcol, resid, slots)


def ring_gather(value, split):
    size = lax.axis_size("tp")
    on = [(i, (i + 2) % size) for i in range(size)]
    back = [(i, (i - 2) % size) for i in range(size)]
    swap = [(i, i ^ 1) for i in range(size)]
    own, other = [value], []
    up, down_, fresh = value, value, (value,)
    for hop in range(1, size // 4 + 1):
        if hop == size // 4:
            up, down_ = up[:split], down_[split:]
        up, down_ = lax.ppermute(up, "tp", on), lax.ppermute(down_, "tp", back)
        swapped = [lax.ppermute(p, "tp", swap) for p in fresh]
        up, down_, *swapped = lax.optimization_barrier((up, down_, *swapped))
        other += swapped
        fresh = (up, down_)
        own += fresh
    other += [lax.ppermute(p, "tp", swap) for p in fresh]
    return own[:-2] + other[:-2], own[-2:] + other[-2:]


def places_of(place, size):
    chips = size // 2
    chip, core = place // 2, place % 2
    turns = [0]
    for hop in range(1, chips // 2):
        turns += [chips - hop, hop]
    at = [2 * lax.rem(chip + turn, chips) for turn in [*turns, chips // 2]]
    own, other = [p + core for p in at], [p + 1 - core for p in at]
    return own[:-1] + other[:-1] + [own[-1], other[-1]]


def hidden_kernel(count, width, place, *refs):
    where = places_of(place[0], count + 2)
    wholes, lows, highs = refs[:count], refs[count : count + 2], refs[count + 2 : count + 4]
    late, late_high = refs[count + 4 : 2 * count + 4], refs[2 * count + 4 : 2 * count + 6]
    gain, wg, wu, sg, su, out, shared_out, normed, normed_late = refs[2 * count + 6 :]
    step = pl.program_id(0)

    def fill(parts, target):
        squares = jnp.zeros(parts[0].shape, F32)
        for x in parts:
            squares = squares + x.astype(F32) * x.astype(F32)
        mean = jnp.sum(squares, axis=1, keepdims=True) / width
        inverse = lax.rsqrt(mean + RMS_EPS)
        for n, x in enumerate(parts):
            at = pl.ds(pl.multiple_of(where[n] * LANES, LANES), LANES)
            target[:, at] = (x.astype(F32) * inverse * gain[:, at]).astype(BF16)

    low = step < 2
    far = [jnp.where(low, a[...].astype(F32), b[...].astype(F32)).astype(BF16) for a, b in zip(lows, highs)]
    fill([x[...] for x in wholes] + far, normed)
    g = jnp.dot(normed[...], wg[...], preferred_element_type=F32)
    u = jnp.dot(normed[...], wu[...], preferred_element_type=F32)
    out[...] = (silu(g) * u).astype(BF16)

    @pl.when(step == 0)
    def _():
        fill([x[...] for x in late] + [x[...] for x in late_high], normed_late)
        dims = (((0,), (1,)), ((), ()))
        sg_out = lax.dot_general(sg[...], normed_late[...], dims, preferred_element_type=F32)
        su_out = lax.dot_general(su[...], normed_late[...], dims, preferred_element_type=F32)
        shared_out[...] = (silu(sg_out) * su_out).astype(BF16)


def hidden_units(wholes, halves, place, rows, gain, wg, wu, sg, su):
    block = rows // 4
    late_rows = wholes[0].shape[0] - rows
    width, units = wg.shape
    late_at = rows // late_rows
    late_half = (rows // 2) // late_rows
    lows, highs = [halves[0], halves[2]], [halves[1], halves[3]]

    def kernel(*refs):
        hidden_kernel(len(wholes), width, *refs)

    def fixed(shape):
        return pl.BlockSpec(shape, lambda i, w: (0, 0))

    return pl.pallas_call(
        kernel,
        grid_spec=pltpu.PrefetchScalarGridSpec(
            num_scalar_prefetch=1,
            grid=(4,),
            in_specs=[pl.BlockSpec((block, LANES), lambda i, w: (i, 0)) for _ in wholes]
            + [pl.BlockSpec((block, LANES), lambda i, w: (jnp.minimum(i, 1), 0)) for _ in lows]
            + [pl.BlockSpec((block, LANES), lambda i, w: (jnp.maximum(i - 2, 0), 0)) for _ in highs]
            + [pl.BlockSpec((late_rows, LANES), lambda i, w: (late_at, 0)) for _ in wholes]
            + [pl.BlockSpec((late_rows, LANES), lambda i, w: (late_half, 0)) for _ in highs]
            + [fixed((1, width)), fixed(wg.shape), fixed(wu.shape), fixed(sg.shape), fixed(su.shape)],
            out_specs=[
                pl.BlockSpec((block, units), lambda i, w: (i, 0)),
                pl.BlockSpec((sg.shape[1], late_rows), lambda i, w: (0, 0)),
            ],
            scratch_shapes=[pltpu.VMEM((block, width), BF16), pltpu.VMEM((late_rows, width), BF16)],
        ),
        out_shape=(
            jax.ShapeDtypeStruct((rows, units), BF16),
            jax.ShapeDtypeStruct((sg.shape[1], late_rows), BF16),
        ),
        name="hidden",
    )(place, *wholes, *lows, *highs, *wholes, *highs, gain, wg, wu, sg, su)


def down_kernel(count, place, *refs):
    where = places_of(place[0], count + 2)
    wholes, lows, highs = refs[:count], refs[count : count + 2], refs[count + 2 : count + 4]
    wd, out, whole = refs[count + 4 :]
    units = wholes[0].shape[1]
    low = pl.program_id(0) < 2
    for n, x in enumerate(wholes):
        whole[:, pl.ds(pl.multiple_of(where[n] * units, units), units)] = x[...]
    for n, (a, b) in enumerate(zip(lows, highs)):
        x = jnp.where(low, a[...].astype(F32), b[...].astype(F32)).astype(BF16)
        whole[:, pl.ds(pl.multiple_of(where[count + n] * units, units), units)] = x
    out[...] = jnp.dot(whole[...], wd[...], preferred_element_type=F32).astype(BF16)


def down(wholes, halves, place, wd):
    rows, units = wholes[0].shape
    block = rows // 4
    lows, highs = [halves[0], halves[2]], [halves[1], halves[3]]

    def kernel(*refs):
        down_kernel(len(wholes), *refs)

    return pl.pallas_call(
        kernel,
        grid_spec=pltpu.PrefetchScalarGridSpec(
            num_scalar_prefetch=1,
            grid=(4,),
            in_specs=[pl.BlockSpec((block, units), lambda i, w: (i, 0)) for _ in wholes]
            + [pl.BlockSpec((block, units), lambda i, w: (jnp.minimum(i, 1), 0)) for _ in lows]
            + [pl.BlockSpec((block, units), lambda i, w: (jnp.maximum(i - 2, 0), 0)) for _ in highs]
            + [pl.BlockSpec(wd.shape, lambda i, w: (0, 0))],
            out_specs=pl.BlockSpec((block, wd.shape[1]), lambda i, w: (i, 0)),
            scratch_shapes=[pltpu.VMEM((block, wd.shape[0]), BF16)],
        ),
        out_shape=jax.ShapeDtypeStruct((rows, wd.shape[1]), BF16),
        name="down",
    )(place, *wholes, *lows, *highs, wd)


def combine_kernel(returned, slots, weights, middle, shared_hidden, sh_down, out):
    dims = (((0,), (0,)), ((), ()))
    shared = lax.dot_general(shared_hidden[...], sh_down[...], dims, preferred_element_type=F32)
    shape = (slots.shape[0], returned.shape[0])
    ids = lax.broadcasted_iota(jnp.int32, shape, 1)
    table = jnp.zeros(shape, F32)
    for k in range(slots.shape[1]):
        table = jnp.where(ids == slots[:, k : k + 1], weights[:, k : k + 1], table)
    routed = jnp.zeros(out.shape, F32)
    for _ in range(3):
        part = table.astype(BF16)
        routed = routed + jnp.dot(part, returned[...], preferred_element_type=F32)
        table = table - part.astype(F32)
    out[...] = (middle[...].astype(F32) + shared + routed).astype(BF16)


def combine(returned, slots, weights, middle, shared_hidden, sh_down):
    return pl.pallas_call(
        combine_kernel,
        out_shape=jax.ShapeDtypeStruct(middle.shape, BF16),
        name="combine",
    )(returned, slots, weights, middle, shared_hidden, sh_down)


def body(
    resid,
    a_val,
    a_gate,
    conv_kernel,
    conv_bias,
    ln_gain,
    ln_bias,
    w_out,
    ffn_gain,
    routes,
    route_weights,
    exp_gate,
    exp_up,
    exp_down,
    sh_gate,
    sh_up,
    sh_down,
):
    tp_count = lax.axis_size("tp")
    tp_place = lax.axis_index("tp")
    sp_count = lax.axis_size("sp")
    tok_rows, model_width = resid.shape
    col_width = model_width // tp_count
    span = conv_kernel.shape[0]
    top_count = routes.shape[1]
    experts_all = exp_gate.shape[0] * sp_count
    capacity = max(2 * tok_rows * top_count // experts_all, tp_count)
    pair_count = tok_rows * top_count
    slot_count = experts_all * capacity

    w_parts = jnp.moveaxis(w_out.reshape(w_out.shape[0], tp_count, col_width), 1, 0)
    wcol = lax.all_to_all(w_parts, "tp", split_axis=0, concat_axis=0, tiled=True)
    wcol = wcol.reshape(w_out.shape[0] * tp_count, col_width)

    gated = (a_val.astype(F32) * jax.nn.sigmoid(a_gate.astype(F32))).astype(BF16)
    halo = span - 1
    pairs = [(i, i + 1) for i in range(sp_count - 1)]
    before = lax.ppermute(gated[tok_rows - halo :], "sp", pairs)
    rows = -(-(halo + tok_rows) // 16) * 16
    vectors = [p[None, :] for v in (conv_bias, ln_gain, ln_bias) for p in in_three(v)]
    right = jnp.concatenate([conv_kernel, *vectors], axis=0)
    right = jnp.pad(right, ((0, rows - right.shape[0]), (0, 0)))
    left = jnp.concatenate([before, gated], axis=0)
    left = jnp.pad(left, ((0, rows - left.shape[0]), (0, 0)))
    packed = lax.all_gather(jnp.concatenate([left, right], axis=1), "tp")

    chosen = routes.reshape(pair_count)
    one_hot = (chosen[:, None] == jnp.arange(experts_all, dtype=jnp.int32)[None, :]).astype(BF16)
    order = jnp.arange(pair_count, dtype=jnp.int32)
    below = (order[:, None] > order[None, :]).astype(BF16)
    earlier = jnp.dot(below, one_hot, preferred_element_type=F32)
    place_in = jnp.sum(earlier * one_hot.astype(F32), axis=1).astype(jnp.int32)
    slots = (chosen * capacity + place_in).reshape(tok_rows, top_count)

    resid_cols = lax.dynamic_slice_in_dim(resid, tp_place * col_width, col_width, 1)
    middle, send = front(span, packed, wcol, resid_cols, slots.T, slot_count)

    landed = lax.all_to_all(
        send.reshape(sp_count, slot_count // sp_count, col_width),
        "sp",
        split_axis=0,
        concat_axis=0,
        tiled=True,
    ).reshape(slot_count, col_width)
    place = tp_place.reshape(1).astype(jnp.int32)
    wholes, halves = ring_gather(jnp.concatenate([landed, middle], axis=0), slot_count // 2)
    hidden, shared_hidden = hidden_units(
        wholes, halves, place, slot_count, ffn_gain[None, :], exp_gate[0], exp_up[0], sh_gate, sh_up
    )
    wholes, halves = ring_gather(hidden, slot_count // 2)
    expert_out = down(wholes, halves, place, exp_down[0])
    shared_all = jnp.broadcast_to(shared_hidden, (tp_count, *shared_hidden.shape))
    shared_all = lax.all_to_all(shared_all, "tp", split_axis=0, concat_axis=0, tiled=True)
    shared_all = shared_all.reshape(-1, tok_rows)
    returned = lax.all_to_all(
        expert_out.reshape(sp_count, slot_count // sp_count, col_width),
        "sp",
        split_axis=0,
        concat_axis=0,
        tiled=True,
    ).reshape(slot_count, col_width)
    return combine(returned, slots, route_weights, middle, shared_all, sh_down)


def solution(mesh):
    in_specs = (
        P("sp", None),
        P("sp", "tp"),
        P("sp", "tp"),
        P(None, "tp"),
        P("tp"),
        P("tp"),
        P("tp"),
        P("tp", None),
        P(),
        P("sp", None),
        P("sp", None),
        P("sp", None, "tp"),
        P("sp", None, "tp"),
        P("sp", None, "tp"),
        P(None, "tp"),
        P(None, "tp"),
        P(None, "tp"),
    )
    out_specs = P("sp", "tp")
    return jax.shard_map(body, mesh=mesh, in_specs=in_specs, out_specs=out_specs, check_vma=False)
```

```python
import jax
import jax.numpy as jnp
from jax import lax
from jax.experimental import pallas as pl
from jax.experimental.pallas import tpu as pltpu
from jax.sharding import PartitionSpec as P

LN_EPS = 1e-05
RMS_EPS = 1e-06
LANES = 128
F32 = jnp.float32
BF16 = jnp.bfloat16


def rounded(value):
    return lax.reduce_precision(value, exponent_bits=8, mantissa_bits=7)


def in_three(value):
    high = rounded(value)
    mid = rounded(value - high)
    low = value - high - mid
    return high.astype(BF16), mid.astype(BF16), low.astype(BF16)


def silu(v):
    return v / (1.0 + jnp.exp(-v))


def front_kernel(span, packed, wcol, resid, slots, middle_out, send_out, win, conv):
    peers, rows, _ = packed.shape
    tok_rows = resid.shape[0]
    half = packed.shape[2] // 2
    channels = peers * half
    for pair in range(peers // 2):
        one, two = packed[2 * pair], packed[2 * pair + 1]
        at = pair * LANES
        left = jnp.concatenate([one[:, :half], two[:, :half]], axis=1)
        right = jnp.concatenate([one[:, half:], two[:, half:]], axis=1)
        win[0, :, at : at + LANES] = left.astype(F32)
        win[1, :, at : at + LANES] = right.astype(F32)

    def vector(first):
        high, mid, low = (win[1, first + i : first + i + 1, :] for i in range(3))
        return high + mid + low

    conv_rows = 64

    def one_block(i, _):
        cols = pl.ds(pl.multiple_of(i * LANES, LANES), LANES)
        taps = win[1, 0:span, cols]
        b = sum(win[1, span + n : span + n + 1, cols] for n in range(3))
        for r in range(0, tok_rows, conv_rows):
            acc = jnp.broadcast_to(b, (conv_rows, LANES))
            for j in range(span):
                acc = acc + taps[j : j + 1, :] * win[0, r + j : r + j + conv_rows, cols]
            conv[r : r + conv_rows, cols] = acc
        return 0

    lax.fori_loop(0, channels // LANES, one_block, 0)
    gain = vector(span + 3)
    shift = vector(span + 6)
    for r in range(0, tok_rows, 64):
        c = conv[r : r + 64, :]
        mean = jnp.sum(c, axis=1, keepdims=True) * (1.0 / channels)
        var = jnp.sum(c * c, axis=1, keepdims=True) * (1.0 / channels) - mean * mean
        scaled = (c - mean) * lax.rsqrt(var + LN_EPS) * gain + shift
        mixed = silu(scaled).astype(BF16)
        proj = jnp.dot(mixed, wcol[...], preferred_element_type=F32)
        middle_out[r : r + 64, :] = (resid[r : r + 64, :].astype(F32) + proj).astype(BF16)
    middle = middle_out[...]
    block = 256
    for r in range(0, send_out.shape[0], block):
        ids = lax.broadcasted_iota(jnp.int32, (block, tok_rows), 0) + r
        hit = ids == slots[0:1, :]
        for k in range(1, slots.shape[0]):
            hit = hit | (ids == slots[k : k + 1, :])
        pick = jnp.where(hit, 1.0, 0.0).astype(BF16)
        send_out[r : r + block, :] = jnp.dot(pick, middle, preferred_element_type=F32).astype(BF16)


def front(span, packed, wcol, resid, slots, slot_count):
    tok_rows, cols = resid.shape
    channels = packed.shape[0] * packed.shape[2] // 2

    def kernel(*refs):
        front_kernel(span, *refs)

    return pl.pallas_call(
        kernel,
        out_shape=(
            jax.ShapeDtypeStruct((tok_rows, cols), BF16),
            jax.ShapeDtypeStruct((slot_count, cols), BF16),
        ),
        scratch_shapes=[
            pltpu.VMEM((2, packed.shape[1], channels), F32),
            pltpu.VMEM((tok_rows, channels), F32),
        ],
        name="front",
    )(packed, wcol, resid, slots)


def ring_gather(value, work):
    size = lax.axis_size("tp")
    steps = size // 4
    ring = [(i, (i + (2 if i % 2 == 0 else -2)) % size) for i in range(size)]
    swap = [(i, i ^ 1) for i in range(size)]

    def moved(v):
        return lax.ppermute(v, "tp", ring)

    def swapped(v):
        return lax.ppermute(v, "tp", swap)

    def tied(*vs):
        return lax.optimization_barrier(vs)

    a, b = value, swapped(value)
    pieces = [a, b]
    a_next, b_next = moved(a), moved(b)
    lot = 0
    for step in range(1, steps):
        a, b = a_next, b_next
        a_next, a_other = moved(a), swapped(a)
        b, a_other = tied(b, a_other)
        if step < steps - 1:
            b_next = moved(b)
        b_other = swapped(b)
        if step < steps - 1:
            a_next, b_other = tied(a_next, b_other)
        pieces += [a, b, a_other, b_other]
        if step == steps - 2:
            lot = len(pieces)
    made = work(pieces[:lot])
    a, *made = tied(a_next, *made)
    pieces += [a, swapped(a)]
    return made, pieces[lot:]


def places_of(place, size):
    chips = size // 2
    chip, core = place // 2, place % 2
    way = 2 * core - 1
    at = [2 * chip + core, 2 * chip + 1 - core]
    for step in range(1, chips // 2):
        here = 2 * lax.rem(chip + way * step + chips, chips)
        there = 2 * lax.rem(chip - way * step + chips, chips)
        at += [here + core, here + 1 - core, there + 1 - core, there + core]
    far = 2 * lax.rem(chip + chips // 2, chips)
    return [*at, far + core, far + 1 - core]


def piece(at, width):
    return pl.ds(pl.multiple_of(at * width, width), width)


def products(parts, where, gain, weights, scratch):
    squares = jnp.zeros(parts[0].shape, F32)
    for n, (x, at) in enumerate(zip(parts, where)):
        wide = x.astype(F32)
        squares = squares + wide * wide
        scratch[0:x.shape[0], n * LANES : (n + 1) * LANES] = (wide * gain[:, piece(at, LANES)]).astype(BF16)
    total = jnp.sum(squares, axis=1, keepdims=True)
    rows = scratch[0 : parts[0].shape[0], 0 : len(parts) * LANES]
    return total, [
        jnp.dot(rows, w[0 : len(parts) * LANES, :], preferred_element_type=F32) for w in weights
    ]


def slots_kernel(first, count, width, size, place, *refs):
    where = places_of(place[0], size)[first : first + count]
    last = first + count == size
    now, late = refs[:count], refs[count : 2 * count]
    gain, wg, wu, sg, su = refs[2 * count : 2 * count + 5]
    rest = refs[2 * count + 5 :]
    if last:
        before, rest = rest[:6], rest[6:]
    outs, scratches = rest[: 2 if last else 6], rest[2 if last else 6 :]
    scratch, pg, pu, qg, qu = scratches
    step = pl.program_id(0)

    @pl.when(step == 0)
    def _():
        for n, at in enumerate(where):
            for source, target in ((wg, pg), (wu, pu), (sg, qg), (su, qu)):
                target[n * LANES : (n + 1) * LANES, :] = source[piece(at, LANES), :]

    def block(parts, one, two, prior):
        total, (g, u) = products([x[...] for x in parts], where, gain, (one, two), scratch)
        if prior is not None:
            g, u, total = g + prior[0][...], u + prior[1][...], total + prior[2][:, 0:1]
        return g, u, total

    def finished(g, u, total):
        inverse = lax.rsqrt(total / width + RMS_EPS)
        return (silu(g * inverse) * (u * inverse)).astype(BF16)

    g, u, total = block(now, pg, pu, before[:3] if last else None)
    if last:
        outs[0][...] = finished(g, u, total)
    else:
        outs[0][...], outs[1][...] = g, u
        outs[2][...] = jnp.broadcast_to(total, outs[2].shape)

    @pl.when(step == 0)
    def _():
        g, u, total = block(late, qg, qu, before[3:] if last else None)
        if last:
            outs[1][...] = finished(g, u, total)
        else:
            outs[3][...], outs[4][...] = g, u
            outs[5][...] = jnp.broadcast_to(total, outs[5].shape)


def slots_lot(pieces, first, size, place, rows, gain, wg, wu, sg, su, before=()):
    block = rows // 4
    late_rows = pieces[0].shape[0] - rows
    late_at = rows // late_rows
    width, units = wg.shape
    few = sg.shape[1]
    count = len(pieces)

    def kernel(*refs):
        slots_kernel(first, count, width, size, *refs)

    def whole(shape):
        return pl.BlockSpec(shape, lambda i, p: (0, 0))

    def by_rows(lanes):
        return pl.BlockSpec((block, lanes), lambda i, p: (i, 0))

    sums = [by_rows(units), by_rows(units), by_rows(LANES)]
    sums += [whole((late_rows, few)), whole((late_rows, few)), whole((late_rows, LANES))]
    shapes = [(rows, units), (rows, units), (rows, LANES)]
    shapes += [(late_rows, few), (late_rows, few), (late_rows, LANES)]
    if before:
        out_specs = [by_rows(units), whole((late_rows, few))]
        out_shape = [
            jax.ShapeDtypeStruct((rows, units), BF16),
            jax.ShapeDtypeStruct((late_rows, few), BF16),
        ]
    else:
        out_specs, out_shape = sums, [jax.ShapeDtypeStruct(s, F32) for s in shapes]
    return pl.pallas_call(
        kernel,
        grid_spec=pltpu.PrefetchScalarGridSpec(
            num_scalar_prefetch=1,
            grid=(4,),
            in_specs=[by_rows(LANES) for _ in pieces]
            + [pl.BlockSpec((late_rows, LANES), lambda i, p: (late_at, 0)) for _ in pieces]
            + [whole(gain.shape), whole(wg.shape), whole(wu.shape), whole(sg.shape), whole(su.shape)]
            + (sums if before else []),
            out_specs=out_specs,
            scratch_shapes=[pltpu.VMEM((block, count * LANES), BF16)]
            + [pltpu.VMEM((count * LANES, n), BF16) for n in (units, units, few, few)],
        ),
        out_shape=out_shape,
        name="slots_lot",
    )(place, *pieces, *pieces, gain, wg, wu, sg, su, *before)


def down_kernel(first, count, size, place, *refs):
    where = places_of(place[0], size)[first : first + count]
    pieces, wd, rest = refs[:count], refs[count], refs[count + 1 :]
    before = rest[0] if len(rest) == 4 else None
    out, rows, weights = rest[-3:]
    units = pieces[0].shape[1]

    @pl.when(pl.program_id(0) == 0)
    def _():
        for n, at in enumerate(where):
            weights[n * units : (n + 1) * units, :] = wd[piece(at, units), :]

    for n, x in enumerate(pieces):
        rows[:, n * units : (n + 1) * units] = x[...]
    total = jnp.dot(rows[...], weights[...], preferred_element_type=F32)
    if before is not None:
        total = total + before[...]
    out[...] = total.astype(out.dtype)


def down_lot(pieces, first, size, place, wd, before=None):
    rows, units = pieces[0].shape
    block = rows // 4
    count = len(pieces)
    cols = wd.shape[1]

    def kernel(*refs):
        down_kernel(first, count, size, *refs)

    given = [] if before is None else [before]
    return pl.pallas_call(
        kernel,
        grid_spec=pltpu.PrefetchScalarGridSpec(
            num_scalar_prefetch=1,
            grid=(4,),
            in_specs=[pl.BlockSpec((block, units), lambda i, p: (i, 0)) for _ in pieces]
            + [pl.BlockSpec(wd.shape, lambda i, p: (0, 0))]
            + [pl.BlockSpec((block, cols), lambda i, p: (i, 0)) for _ in given],
            out_specs=pl.BlockSpec((block, cols), lambda i, p: (i, 0)),
            scratch_shapes=[
                pltpu.VMEM((block, count * units), BF16),
                pltpu.VMEM((count * units, cols), BF16),
            ],
        ),
        out_shape=jax.ShapeDtypeStruct((rows, cols), F32 if before is None else BF16),
        name="down_lot",
    )(place, *pieces, wd, *given)


def combine_kernel(returned, slots, weights, middle, shared_hidden, sh_down, out):
    units = shared_hidden.shape[2]
    shared = jnp.zeros(out.shape, F32)
    for n in range(shared_hidden.shape[0]):
        part = sh_down[n * units : (n + 1) * units, :]
        shared = shared + jnp.dot(shared_hidden[n], part, preferred_element_type=F32)
    shape = (slots.shape[0], returned.shape[0])
    ids = lax.broadcasted_iota(jnp.int32, shape, 1)
    table = jnp.zeros(shape, F32)
    for k in range(slots.shape[1]):
        table = jnp.where(ids == slots[:, k : k + 1], weights[:, k : k + 1], table)
    routed = jnp.zeros(out.shape, F32)
    for _ in range(3):
        part = table.astype(BF16)
        routed = routed + jnp.dot(part, returned[...], preferred_element_type=F32)
        table = table - part.astype(F32)
    out[...] = (middle[...].astype(F32) + shared + routed).astype(BF16)


def combine(returned, slots, weights, middle, shared_hidden, sh_down):
    return pl.pallas_call(
        combine_kernel,
        out_shape=jax.ShapeDtypeStruct(middle.shape, BF16),
        name="combine",
    )(returned, slots, weights, middle, shared_hidden, sh_down)


def body(
    resid,
    a_val,
    a_gate,
    conv_kernel,
    conv_bias,
    ln_gain,
    ln_bias,
    w_out,
    ffn_gain,
    routes,
    route_weights,
    exp_gate,
    exp_up,
    exp_down,
    sh_gate,
    sh_up,
    sh_down,
):
    tp_count = lax.axis_size("tp")
    tp_place = lax.axis_index("tp")
    sp_count = lax.axis_size("sp")
    tok_rows, model_width = resid.shape
    col_width = model_width // tp_count
    span = conv_kernel.shape[0]
    top_count = routes.shape[1]
    experts_all = exp_gate.shape[0] * sp_count
    capacity = max(2 * tok_rows * top_count // experts_all, tp_count)
    pair_count = tok_rows * top_count
    slot_count = experts_all * capacity

    w_parts = jnp.moveaxis(w_out.reshape(w_out.shape[0], tp_count, col_width), 1, 0)
    wcol = lax.all_to_all(w_parts, "tp", split_axis=0, concat_axis=0, tiled=True)
    wcol = wcol.reshape(w_out.shape[0] * tp_count, col_width)

    gated = (a_val.astype(F32) * jax.nn.sigmoid(a_gate.astype(F32))).astype(BF16)
    halo = span - 1
    pairs = [(i, i + 1) for i in range(sp_count - 1)]
    before = lax.ppermute(gated[tok_rows - halo :], "sp", pairs)
    rows = -(-(halo + tok_rows) // 16) * 16
    vectors = [p[None, :] for v in (conv_bias, ln_gain, ln_bias) for p in in_three(v)]
    right = jnp.concatenate([conv_kernel, *vectors], axis=0)
    right = jnp.pad(right, ((0, rows - right.shape[0]), (0, 0)))
    left = jnp.concatenate([before, gated], axis=0)
    left = jnp.pad(left, ((0, rows - left.shape[0]), (0, 0)))
    packed = lax.all_gather(jnp.concatenate([left, right], axis=1), "tp")

    chosen = routes.reshape(pair_count)
    one_hot = (chosen[:, None] == jnp.arange(experts_all, dtype=jnp.int32)[None, :]).astype(BF16)
    order = jnp.arange(pair_count, dtype=jnp.int32)
    below = (order[:, None] > order[None, :]).astype(BF16)
    earlier = jnp.dot(below, one_hot, preferred_element_type=F32)
    place_in = jnp.sum(earlier * one_hot.astype(F32), axis=1).astype(jnp.int32)
    slots = (chosen * capacity + place_in).reshape(tok_rows, top_count)

    resid_cols = lax.dynamic_slice_in_dim(resid, tp_place * col_width, col_width, 1)
    middle, send = front(span, packed, wcol, resid_cols, slots.T, slot_count)

    landed = lax.all_to_all(
        send.reshape(sp_count, slot_count // sp_count, col_width),
        "sp",
        split_axis=0,
        concat_axis=0,
        tiled=True,
    ).reshape(slot_count, col_width)
    place = tp_place.reshape(1).astype(jnp.int32)
    fixed = (slot_count, ffn_gain[None, :], exp_gate[0], exp_up[0], sh_gate, sh_up)
    firsts = []

    def slots_begun(pieces):
        firsts.append(len(pieces))
        return slots_lot(pieces, 0, tp_count, place, *fixed)

    sums, pieces = ring_gather(jnp.concatenate([landed, middle], axis=0), slots_begun)
    hidden, shared_hidden = slots_lot(pieces, firsts[0], tp_count, place, *fixed, before=sums)

    def down_begun(pieces):
        return (down_lot(pieces, 0, tp_count, place, exp_down[0]),)

    shared_all = jnp.broadcast_to(shared_hidden, (tp_count, *shared_hidden.shape))
    shared_all = lax.all_to_all(shared_all, "tp", split_axis=0, concat_axis=0, tiled=True)
    sums, pieces = ring_gather(hidden, down_begun)
    expert_out = down_lot(pieces, firsts[0], tp_count, place, exp_down[0], before=sums[0])
    returned = lax.all_to_all(
        expert_out.reshape(sp_count, slot_count // sp_count, col_width),
        "sp",
        split_axis=0,
        concat_axis=0,
        tiled=True,
    ).reshape(slot_count, col_width)
    return combine(returned, slots, route_weights, middle, shared_all, sh_down)


def solution(mesh):
    in_specs = (
        P("sp", None),
        P("sp", "tp"),
        P("sp", "tp"),
        P(None, "tp"),
        P("tp"),
        P("tp"),
        P("tp"),
        P("tp", None),
        P(),
        P("sp", None),
        P("sp", None),
        P("sp", None, "tp"),
        P("sp", None, "tp"),
        P("sp", None, "tp"),
        P(None, "tp"),
        P(None, "tp"),
        P(None, "tp"),
    )
    out_specs = P("sp", "tp")
    return jax.shard_map(body, mesh=mesh, in_specs=in_specs, out_specs=out_specs, check_vma=False)
```

```python
import jax
import jax.numpy as jnp
from jax import lax
from jax.experimental import pallas as pl
from jax.experimental.pallas import tpu as pltpu
from jax.sharding import PartitionSpec as P

LN_EPS = 1e-05
RMS_EPS = 1e-06
LANES = 128
F32 = jnp.float32
BF16 = jnp.bfloat16


def silu(v):
    return v / (1.0 + jnp.exp(-v))


def pack_kernel(before, a_val, a_gate, taps, bias, gain, shift, w_out, out, win, params):
    peers, _, lanes = out.shape
    halo, half = before.shape
    rows = win.shape[0]
    win[...] = jnp.zeros(win.shape, F32)
    params[...] = jnp.zeros(params.shape, F32)
    gate = 1.0 / (1.0 + jnp.exp(-a_gate[...].astype(F32)))
    win[0:halo, :] = before[...].astype(F32)
    win[halo : halo + a_val.shape[0], :] = a_val[...].astype(F32) * gate
    span = taps.shape[0]
    params[0:span, :] = taps[...].astype(F32)
    for n, vector in enumerate((bias, gain, shift)):
        rest = vector[...]
        for part in range(3):
            kept = rest.astype(BF16).astype(F32)
            at = span + 3 * n + part
            params[at : at + 1, :] = kept
            rest = rest - kept

    def folded(v):
        n = v.shape[0] // 2
        return jnp.concatenate([v[0:n, :], v[n : 2 * n, :]], axis=1).astype(BF16)

    head, tail = folded(win[...]), folded(params[...])
    top = rows // 2
    low = top + tail.shape[0]
    for t in range(peers):
        out[t, 0:top, :] = head
        out[t, top:low, :] = tail
        out[t, low : low + w_out.shape[0], :] = w_out[:, t * lanes : (t + 1) * lanes]


PARAM_ROWS = 64


def window_rows(span, tok_rows):
    return -(-(span - 1 + tok_rows) // 32) * 32


def pack(before, a_val, a_gate, taps, bias, gain, shift, w_out, peers):
    rows = window_rows(taps.shape[0], a_val.shape[0])
    lanes = w_out.shape[1] // peers
    total = rows // 2 + PARAM_ROWS // 2 + w_out.shape[0]
    return pl.pallas_call(
        pack_kernel,
        out_shape=jax.ShapeDtypeStruct((peers, total, lanes), BF16),
        scratch_shapes=[
            pltpu.VMEM((rows, a_val.shape[1]), F32),
            pltpu.VMEM((PARAM_ROWS, a_val.shape[1]), F32),
        ],
        name="pack",
    )(before, a_val, a_gate, taps, bias, gain, shift, w_out)


def routing_kernel(capacity, routes, slots_out, pick_out):
    tok_rows, top_count = routes.shape
    experts = pick_out.shape[1] // capacity
    ids = lax.broadcasted_iota(jnp.int32, (tok_rows, experts), 1)
    hits = [ids == routes[:, k : k + 1] for k in range(top_count)]
    named = sum(jnp.where(h, 1.0, 0.0) for h in hits).astype(BF16)
    square = (tok_rows, tok_rows)
    below = lax.broadcasted_iota(jnp.int32, square, 0) > lax.broadcasted_iota(jnp.int32, square, 1)
    earlier = jnp.dot(jnp.where(below, 1.0, 0.0).astype(BF16), named, preferred_element_type=F32)
    wide = lax.broadcasted_iota(jnp.int32, pick_out.shape, 1)
    lane = lax.broadcasted_iota(jnp.int32, slots_out.shape, 1)
    slots = jnp.zeros(slots_out.shape, jnp.int32)
    pick = jnp.zeros(pick_out.shape, F32)
    for k in range(top_count):
        place = jnp.sum(jnp.where(hits[k], earlier, 0.0), axis=1, keepdims=True).astype(jnp.int32)
        slot = routes[:, k : k + 1] * capacity + place
        slots = jnp.where(lane == k, slot, slots)
        pick = jnp.where(wide == slot, 1.0, pick)
    slots_out[...] = slots
    pick_out[...] = pick.astype(BF16)


def routing(routes, capacity, slot_count):
    tok_rows, top_count = routes.shape

    def kernel(*refs):
        routing_kernel(capacity, *refs)

    return pl.pallas_call(
        kernel,
        out_shape=(
            jax.ShapeDtypeStruct((tok_rows, top_count), jnp.int32),
            jax.ShapeDtypeStruct((tok_rows, slot_count), BF16),
        ),
        name="routing",
    )(routes)


def table_kernel(slots, weights, out):
    shape = out.shape[1:]
    ids = lax.broadcasted_iota(jnp.int32, shape, 1)
    table = jnp.zeros(shape, F32)
    for k in range(slots.shape[1]):
        table = jnp.where(ids == slots[:, k : k + 1], weights[:, k : k + 1], table)
    for n in range(out.shape[0]):
        part = table.astype(BF16)
        out[n] = part
        table = table - part.astype(F32)


def weight_table(slots, weights, slot_count):
    return pl.pallas_call(
        table_kernel,
        out_shape=jax.ShapeDtypeStruct((3, slots.shape[0], slot_count), BF16),
        name="table",
    )(slots, weights)


def front_kernel(span, packed, resid, pick, middle_out, send_out, win, params, conv):
    peers = packed.shape[0]
    tok_rows = resid.shape[0]
    half = LANES // 2
    channels = peers * half
    top = win.shape[0] // 2
    fold = PARAM_ROWS // 2
    for pair in range(peers // 2):
        at = slice(pair * LANES, (pair + 1) * LANES)
        one, two = packed[2 * pair, 0 : top + fold, :], packed[2 * pair + 1, 0 : top + fold, :]
        left = jnp.concatenate([one[:, :half], two[:, :half]], axis=1).astype(F32)
        right = jnp.concatenate([one[:, half:], two[:, half:]], axis=1).astype(F32)
        win[0:top, at], win[top : 2 * top, at] = left[0:top], right[0:top]
        params[0:fold, at], params[fold : 2 * fold, at] = left[top:], right[top:]

    def vector(first, cols=slice(None)):
        return sum(params[first + i : first + i + 1, cols] for i in range(3))

    conv_rows = 64

    def one_block(i, _):
        cols = pl.ds(pl.multiple_of(i * LANES, LANES), LANES)
        taps = params[0:span, cols]
        b = vector(span, cols)
        for r in range(0, tok_rows, conv_rows):
            acc = jnp.broadcast_to(b, (conv_rows, LANES))
            for j in range(span):
                acc = acc + taps[j : j + 1, :] * win[r + j : r + j + conv_rows, cols]
            conv[r : r + conv_rows, cols] = acc
        return 0

    lax.fori_loop(0, channels // LANES, one_block, 0)
    gain = vector(span + 3)
    shift = vector(span + 6)
    wcol = packed[:, top + fold :, :].reshape(channels, packed.shape[2])
    for r in range(0, tok_rows, 64):
        c = conv[r : r + 64, :]
        mean = jnp.sum(c, axis=1, keepdims=True) * (1.0 / channels)
        var = jnp.sum(c * c, axis=1, keepdims=True) * (1.0 / channels) - mean * mean
        scaled = (c - mean) * lax.rsqrt(var + LN_EPS) * gain + shift
        mixed = silu(scaled).astype(BF16)
        proj = jnp.dot(mixed, wcol, preferred_element_type=F32)
        middle_out[r : r + 64, :] = (resid[r : r + 64, :].astype(F32) + proj).astype(BF16)
    middle = middle_out[...]
    dims = (((0,), (0,)), ((), ()))
    send_out[...] = lax.dot_general(pick[...], middle, dims, preferred_element_type=F32).astype(BF16)


def front(span, packed, resid, pick):
    tok_rows, cols = resid.shape
    channels = packed.shape[0] * LANES // 2

    def kernel(*refs):
        front_kernel(span, *refs)

    return pl.pallas_call(
        kernel,
        out_shape=(
            jax.ShapeDtypeStruct((tok_rows, cols), BF16),
            jax.ShapeDtypeStruct((pick.shape[1], cols), BF16),
        ),
        scratch_shapes=[
            pltpu.VMEM((window_rows(span, tok_rows), channels), F32),
            pltpu.VMEM((PARAM_ROWS, channels), F32),
            pltpu.VMEM((tok_rows, channels), F32),
        ],
        name="front",
    )(packed, resid, pick)


def hidden_kernel(width, rows_in, gain, wg, wu, out):
    pieces = rows_in.shape[0]
    squares = jnp.zeros((rows_in.shape[1], LANES), F32)
    for t in range(pieces):
        x = rows_in[t].astype(F32)
        squares = squares + x * x
    mean = jnp.sum(squares, axis=1, keepdims=True) / width
    inverse = lax.rsqrt(mean + RMS_EPS)
    normed = jnp.concatenate(
        [(rows_in[t].astype(F32) * inverse * gain[t : t + 1, :]).astype(BF16) for t in range(pieces)],
        axis=1,
    )
    g = jnp.dot(normed, wg[...], preferred_element_type=F32)
    u = jnp.dot(normed, wu[...], preferred_element_type=F32)
    out[...] = (silu(g) * u).astype(BF16)


def hidden_units(rows_in, gain, wg, wu):
    pieces, rows, lanes = rows_in.shape
    width, units = wg.shape
    block = 256

    def kernel(*refs):
        hidden_kernel(width, *refs)

    return pl.pallas_call(
        kernel,
        grid=(rows // block,),
        in_specs=[
            pl.BlockSpec((pieces, block, lanes), lambda i: (0, i, 0)),
            pl.BlockSpec((pieces, lanes), lambda i: (0, 0)),
            pl.BlockSpec((width, units), lambda i: (0, 0)),
            pl.BlockSpec((width, units), lambda i: (0, 0)),
        ],
        out_specs=pl.BlockSpec((block, units), lambda i: (i, 0)),
        out_shape=jax.ShapeDtypeStruct((rows, units), BF16),
        name="hidden",
    )(rows_in, gain, wg, wu)


def down_kernel(hidden, wd, out):
    whole = jnp.concatenate([hidden[t] for t in range(hidden.shape[0])], axis=1)
    out[...] = jnp.dot(whole, wd[...], preferred_element_type=F32).astype(BF16)


def down(hidden, wd):
    pieces, rows, units = hidden.shape
    block = 256
    return pl.pallas_call(
        down_kernel,
        grid=(rows // block,),
        in_specs=[
            pl.BlockSpec((pieces, block, units), lambda i: (0, i, 0)),
            pl.BlockSpec(wd.shape, lambda i: (0, 0)),
        ],
        out_specs=pl.BlockSpec((block, wd.shape[1]), lambda i: (i, 0)),
        out_shape=jax.ShapeDtypeStruct((rows, wd.shape[1]), BF16),
        name="down",
    )(hidden, wd)


def combine_kernel(returned, table, middle, shared, out):
    total = middle[...].astype(F32) + shared[...]
    rows = returned[...]
    for n in range(table.shape[0]):
        total = total + jnp.dot(table[n], rows, preferred_element_type=F32)
    out[...] = total.astype(BF16)


def combine(returned, table, middle, shared):
    return pl.pallas_call(
        combine_kernel,
        out_shape=jax.ShapeDtypeStruct(middle.shape, BF16),
        name="combine",
    )(returned, table, middle, shared)


def body(
    resid,
    a_val,
    a_gate,
    conv_kernel,
    conv_bias,
    ln_gain,
    ln_bias,
    w_out,
    ffn_gain,
    routes,
    route_weights,
    exp_gate,
    exp_up,
    exp_down,
    sh_gate,
    sh_up,
    sh_down,
):
    tp_count = lax.axis_size("tp")
    tp_place = lax.axis_index("tp")
    sp_count = lax.axis_size("sp")
    tok_rows, model_width = resid.shape
    col_width = model_width // tp_count
    span = conv_kernel.shape[0]
    top_count = routes.shape[1]
    experts_all = exp_gate.shape[0] * sp_count
    capacity = max(2 * tok_rows * top_count // experts_all, tp_count)
    slot_count = experts_all * capacity

    halo = span - 1
    late_val, late_gate = a_val[tok_rows - halo :].astype(F32), a_gate[tok_rows - halo :].astype(F32)
    pairs = [(i, i + 1) for i in range(sp_count - 1)]
    before = lax.ppermute((late_val * jax.nn.sigmoid(late_gate)).astype(BF16), "sp", pairs)

    vectors = [v[None, :] for v in (conv_bias, ln_gain, ln_bias)]
    packed = pack(before, a_val, a_gate, conv_kernel, *vectors, w_out, tp_count)
    spread = lax.all_to_all(packed, "tp", split_axis=0, concat_axis=0, tiled=True)

    routes_late, _ = lax.optimization_barrier((routes, packed[0, :1]))
    slots, pick = routing(routes_late, capacity, slot_count)

    resid_cols = lax.dynamic_slice_in_dim(resid, tp_place * col_width, col_width, 1)
    middle, send = front(span, spread, resid_cols, pick)

    landed = lax.all_to_all(
        send.reshape(sp_count, slot_count // sp_count, col_width),
        "sp",
        split_axis=0,
        concat_axis=0,
        tiled=True,
    ).reshape(slot_count, col_width)
    slots_late, weights_late, _ = lax.optimization_barrier((slots, route_weights, middle[:1]))
    table = weight_table(slots_late, weights_late, slot_count)
    landed, table = lax.optimization_barrier((landed, table))
    gain = ffn_gain.reshape(tp_count, col_width)
    arrived = lax.all_gather(landed, "tp")
    hidden = hidden_units(arrived, gain, exp_gate[0], exp_up[0])

    middle_late, landed_late = lax.optimization_barrier((middle, landed[:1]))
    middle_all = lax.all_gather(middle_late, "tp")
    middle_f = jnp.moveaxis(middle_all, 0, 1).reshape(tok_rows, model_width).astype(F32)
    squares = jnp.sum(middle_f * middle_f, axis=1, keepdims=True)
    inverse = lax.rsqrt(squares / model_width + RMS_EPS)
    normed = (middle_f * inverse * ffn_gain[None, :]).astype(BF16)
    shared_gate = jnp.dot(normed, sh_gate, preferred_element_type=F32)
    shared_up = jnp.dot(normed, sh_up, preferred_element_type=F32)
    shared_hidden = (jax.nn.silu(shared_gate) * shared_up).astype(BF16)

    hidden_all = lax.all_gather(hidden, "tp")
    shared_late, _ = lax.optimization_barrier((shared_hidden, hidden[:1]))
    shared_all = lax.all_gather(shared_late, "tp", axis=1, tiled=True)
    hidden_all, shared_all = lax.optimization_barrier((hidden_all, shared_all))

    expert_out = down(hidden_all, exp_down[0])
    returned = lax.all_to_all(
        expert_out.reshape(sp_count, slot_count // sp_count, col_width),
        "sp",
        split_axis=0,
        concat_axis=0,
        tiled=True,
    ).reshape(slot_count, col_width)
    shared_all, _ = lax.optimization_barrier((shared_all, expert_out[:1]))
    shared = jnp.dot(shared_all, sh_down, preferred_element_type=F32)
    return combine(returned, table, middle, shared)


def solution(mesh):
    in_specs = (
        P("sp", None),
        P("sp", "tp"),
        P("sp", "tp"),
        P(None, "tp"),
        P("tp"),
        P("tp"),
        P("tp"),
        P("tp", None),
        P(),
        P("sp", None),
        P("sp", None),
        P("sp", None, "tp"),
        P("sp", None, "tp"),
        P("sp", None, "tp"),
        P(None, "tp"),
        P(None, "tp"),
        P(None, "tp"),
    )
    out_specs = P("sp", "tp")
    return jax.shard_map(body, mesh=mesh, in_specs=in_specs, out_specs=out_specs, check_vma=False)
```

```python
import jax
import jax.numpy as jnp
from jax import lax
from jax.experimental import pallas as pl
from jax.experimental.pallas import tpu as pltpu
from jax.sharding import PartitionSpec as P

LN_EPS = 1e-05
RMS_EPS = 1e-06
LANES = 128
F32 = jnp.float32
BF16 = jnp.bfloat16


def silu(v):
    return v / (1.0 + jnp.exp(-v))


def pack_kernel(before, a_val, a_gate, taps, bias, gain, shift, w_out, out, win, params):
    peers, _, lanes = out.shape
    halo, half = before.shape
    rows = win.shape[0]
    win[...] = jnp.zeros(win.shape, F32)
    params[...] = jnp.zeros(params.shape, F32)
    gate = 1.0 / (1.0 + jnp.exp(-a_gate[...].astype(F32)))
    win[0:halo, :] = before[...].astype(F32)
    win[halo : halo + a_val.shape[0], :] = a_val[...].astype(F32) * gate
    span = taps.shape[0]
    params[0:span, :] = taps[...].astype(F32)
    for n, vector in enumerate((bias, gain, shift)):
        rest = vector[...]
        for part in range(3):
            kept = rest.astype(BF16).astype(F32)
            at = span + 3 * n + part
            params[at : at + 1, :] = kept
            rest = rest - kept

    def folded(v):
        n = v.shape[0] // 2
        return jnp.concatenate([v[0:n, :], v[n : 2 * n, :]], axis=1).astype(BF16)

    head, tail = folded(win[...]), folded(params[...])
    top = rows // 2
    low = top + tail.shape[0]
    for t in range(peers):
        out[t, 0:top, :] = head
        out[t, top:low, :] = tail
        out[t, low : low + w_out.shape[0], :] = w_out[:, t * lanes : (t + 1) * lanes]


PARAM_ROWS = 64
FOLDED = 16
ASIDE = (96, 112)


def window_rows(span, tok_rows):
    return -(-(span - 1 + tok_rows) // 32) * 32


def pack(before, a_val, a_gate, taps, bias, gain, shift, w_out, peers):
    rows = window_rows(taps.shape[0], a_val.shape[0])
    lanes = w_out.shape[1] // peers
    total = rows // 2 + PARAM_ROWS // 2 + w_out.shape[0]
    return pl.pallas_call(
        pack_kernel,
        out_shape=jax.ShapeDtypeStruct((peers, total, lanes), BF16),
        scratch_shapes=[
            pltpu.VMEM((rows, a_val.shape[1]), F32),
            pltpu.VMEM((PARAM_ROWS, a_val.shape[1]), F32),
        ],
        name="pack",
    )(before, a_val, a_gate, taps, bias, gain, shift, w_out)


def routing_kernel(capacity, routes, slots_out, pick_out):
    tok_rows, top_count = routes.shape
    experts = pick_out.shape[1] // capacity
    ids = lax.broadcasted_iota(jnp.int32, (tok_rows, experts), 1)
    hits = [ids == routes[:, k : k + 1] for k in range(top_count)]
    named = sum(jnp.where(h, 1.0, 0.0) for h in hits).astype(BF16)
    square = (tok_rows, tok_rows)
    below = lax.broadcasted_iota(jnp.int32, square, 0) > lax.broadcasted_iota(jnp.int32, square, 1)
    earlier = jnp.dot(jnp.where(below, 1.0, 0.0).astype(BF16), named, preferred_element_type=F32)
    wide = lax.broadcasted_iota(jnp.int32, pick_out.shape, 1)
    lane = lax.broadcasted_iota(jnp.int32, slots_out.shape, 1)
    slots = jnp.zeros(slots_out.shape, jnp.int32)
    pick = jnp.zeros(pick_out.shape, F32)
    for k in range(top_count):
        place = jnp.sum(jnp.where(hits[k], earlier, 0.0), axis=1, keepdims=True).astype(jnp.int32)
        slot = routes[:, k : k + 1] * capacity + place
        slots = jnp.where(lane == k, slot, slots)
        pick = jnp.where(wide == slot, 1.0, pick)
    slots_out[...] = slots
    pick_out[...] = pick.astype(BF16)


def routing(routes, capacity, slot_count):
    tok_rows, top_count = routes.shape

    def kernel(*refs):
        routing_kernel(capacity, *refs)

    return pl.pallas_call(
        kernel,
        out_shape=(
            jax.ShapeDtypeStruct((tok_rows, top_count), jnp.int32),
            jax.ShapeDtypeStruct((tok_rows, slot_count), BF16),
        ),
        name="routing",
    )(routes)


def table_kernel(slots, weights, out):
    shape = out.shape[1:]
    ids = lax.broadcasted_iota(jnp.int32, shape, 1)
    table = jnp.zeros(shape, F32)
    for k in range(slots.shape[1]):
        table = jnp.where(ids == slots[:, k : k + 1], weights[:, k : k + 1], table)
    for n in range(out.shape[0]):
        part = table.astype(BF16)
        out[n] = part
        table = table - part.astype(F32)


def weight_table(slots, weights, slot_count):
    return pl.pallas_call(
        table_kernel,
        out_shape=jax.ShapeDtypeStruct((3, slots.shape[0], slot_count), BF16),
        name="table",
    )(slots, weights)


def front_kernel(span, packed, resid, pick, middle_out, send_out, win, params, conv):
    peers = packed.shape[0]
    tok_rows = resid.shape[0]
    half = LANES // 2
    channels = peers * half
    top = win.shape[0] // 2
    fold = PARAM_ROWS // 2
    for pair in range(peers // 2):
        at = slice(pair * LANES, (pair + 1) * LANES)
        one, two = packed[2 * pair, 0 : top + fold, :], packed[2 * pair + 1, 0 : top + fold, :]
        left = jnp.concatenate([one[:, :half], two[:, :half]], axis=1).astype(F32)
        right = jnp.concatenate([one[:, half:], two[:, half:]], axis=1).astype(F32)
        win[0:top, at], win[top : 2 * top, at] = left[0:top], right[0:top]
        params[0:fold, at], params[fold : 2 * fold, at] = left[top:], right[top:]

    def vector(first, cols=slice(None)):
        return sum(params[first + i : first + i + 1, cols] for i in range(3))

    conv_rows = 64

    def one_block(i, _):
        cols = pl.ds(pl.multiple_of(i * LANES, LANES), LANES)
        taps = params[0:span, cols]
        b = vector(span, cols)
        for r in range(0, tok_rows, conv_rows):
            acc = jnp.broadcast_to(b, (conv_rows, LANES))
            for j in range(span):
                acc = acc + taps[j : j + 1, :] * win[r + j : r + j + conv_rows, cols]
            conv[r : r + conv_rows, cols] = acc
        return 0

    lax.fori_loop(0, channels // LANES, one_block, 0)
    gain = vector(span + 3)
    shift = vector(span + 6)
    wcol = packed[:, top + fold :, :].reshape(channels, packed.shape[2])
    for r in range(0, tok_rows, 64):
        c = conv[r : r + 64, :]
        mean = jnp.sum(c, axis=1, keepdims=True) * (1.0 / channels)
        var = jnp.sum(c * c, axis=1, keepdims=True) * (1.0 / channels) - mean * mean
        scaled = (c - mean) * lax.rsqrt(var + LN_EPS) * gain + shift
        mixed = silu(scaled).astype(BF16)
        proj = jnp.dot(mixed, wcol, preferred_element_type=F32)
        middle_out[r : r + 64, :] = (resid[r : r + 64, :].astype(F32) + proj).astype(BF16)
    middle = middle_out[...]
    dims = (((0,), (0,)), ((), ()))
    send_out[...] = lax.dot_general(pick[...], middle, dims, preferred_element_type=F32).astype(BF16)


def front(span, packed, resid, pick):
    tok_rows, cols = resid.shape
    channels = packed.shape[0] * LANES // 2

    def kernel(*refs):
        front_kernel(span, *refs)

    return pl.pallas_call(
        kernel,
        out_shape=(
            jax.ShapeDtypeStruct((tok_rows, cols), BF16),
            jax.ShapeDtypeStruct((pick.shape[1], cols), BF16),
        ),
        scratch_shapes=[
            pltpu.VMEM((window_rows(span, tok_rows), channels), F32),
            pltpu.VMEM((PARAM_ROWS, channels), F32),
            pltpu.VMEM((tok_rows, channels), F32),
        ],
        name="front",
    )(packed, resid, pick)


def normed_rows(pieces, width, gain):
    squares = jnp.zeros(pieces[0].shape, F32)
    for x in pieces:
        squares = squares + x.astype(F32) * x.astype(F32)
    mean = jnp.sum(squares, axis=1, keepdims=True) / width
    inverse = lax.rsqrt(mean + RMS_EPS)
    cols = [gain[:, n * LANES : (n + 1) * LANES] for n in range(len(pieces))]
    scaled = [(x.astype(F32) * inverse * c).astype(BF16) for x, c in zip(pieces, cols)]
    return jnp.concatenate(scaled, axis=1)


def gated_units(rows, w_gate, w_up):
    g = jnp.dot(rows, w_gate, preferred_element_type=F32)
    u = jnp.dot(rows, w_up, preferred_element_type=F32)
    return (silu(g) * u).astype(BF16)


def hidden_kernel(rows_in, gain, wg, wu, out):
    rows = normed_rows([rows_in[t] for t in range(rows_in.shape[0])], wg.shape[0], gain)
    out[...] = gated_units(rows, wg[...], wu[...])


def hidden_units(rows_in, gain, wg, wu, blocks):
    pieces, rows, lanes = rows_in.shape
    width, units = wg.shape
    block = rows // blocks
    return pl.pallas_call(
        hidden_kernel,
        grid=(blocks,),
        in_specs=[
            pl.BlockSpec((pieces, block, lanes), lambda i: (0, i, 0)),
            pl.BlockSpec((1, width), lambda i: (0, 0)),
            pl.BlockSpec((width, units), lambda i: (0, 0)),
            pl.BlockSpec((width, units), lambda i: (0, 0)),
        ],
        out_specs=pl.BlockSpec((block, units), lambda i: (i, 0)),
        out_shape=jax.ShapeDtypeStruct((rows, units), BF16),
        name="hidden",
    )(rows_in, gain, wg, wu)


def side_hidden_kernel(one, two, gain, wg, wu, sg, su, one_out, two_out):
    width, units = wg.shape
    few = sg.shape[1]
    slots = one_out.shape[0] - FOLDED
    rows = normed_rows([one[t] for t in range(one.shape[0])], width, gain)
    one_out[0:slots, :] = gated_units(rows[0:slots, :], wg[...], wu[...])
    shared = gated_units(rows[slots:, :], sg[...], su[...])
    parts = [shared[j * FOLDED : (j + 1) * FOLDED, :].astype(F32) for j in range(units // few)]
    one_out[slots:, :] = jnp.concatenate(parts, axis=1).astype(BF16)
    rows = normed_rows([two[t] for t in range(two.shape[0])], width, gain)
    two_out[...] = gated_units(rows, wg[...], wu[...])


def side_hidden(one, two, gain, wg, wu, sg, su, tok_rows):
    units = wg.shape[1]
    slots = one.shape[1] - tok_rows
    return pl.pallas_call(
        side_hidden_kernel,
        out_shape=(
            jax.ShapeDtypeStruct((slots + FOLDED, units), BF16),
            jax.ShapeDtypeStruct((two.shape[1], units), BF16),
        ),
        name="side_hidden",
    )(one, two, gain, wg, wu, sg, su)


def side_down_kernel(one, two, wd, sh_down, out, shared_out):
    peers, rows, units = one.shape
    slots = rows - FOLDED
    few = sh_down.shape[0] // peers
    folds = units // few
    whole = jnp.concatenate([one[t, 0:slots, :] for t in range(peers)], axis=1)
    out[0:slots, :] = jnp.dot(whole, wd[...], preferred_element_type=F32).astype(BF16)
    whole = jnp.concatenate([two[t] for t in range(peers)], axis=1)
    out[slots:, :] = jnp.dot(whole, wd[...], preferred_element_type=F32).astype(BF16)
    shape = (folds * FOLDED, units)
    own = lax.broadcasted_iota(jnp.int32, shape, 0) // FOLDED == lax.broadcasted_iota(jnp.int32, shape, 1) // few
    shared = jnp.zeros(shared_out.shape, F32)
    for t in range(peers):
        packed = one[t, slots:, :].astype(F32)
        spread = jnp.where(own, jnp.concatenate([packed] * folds, axis=0), 0.0).astype(BF16)
        weights = jnp.concatenate([sh_down[t * few : (t + 1) * few, :]] * folds, axis=0)
        shared = shared + jnp.dot(spread, weights, preferred_element_type=F32)
    shared_out[...] = shared


def side_down(one, two, wd, sh_down, tok_rows):
    slots = one.shape[1] - FOLDED + two.shape[1]
    return pl.pallas_call(
        side_down_kernel,
        out_shape=(
            jax.ShapeDtypeStruct((slots, wd.shape[1]), BF16),
            jax.ShapeDtypeStruct((tok_rows, wd.shape[1]), F32),
        ),
        name="side_down",
    )(one, two, wd, sh_down)


def down_kernel(hidden, wd, aside, out):
    slots = aside.shape[0]
    block = hidden.shape[1]
    step = pl.program_id(0)

    @pl.when(step == 0)
    def _():
        out[0:slots, :] = aside[...]

    whole = jnp.concatenate([hidden[t] for t in range(hidden.shape[0])], axis=1)
    at = pl.ds(pl.multiple_of(slots + step * block, 16), block)
    out[at, :] = jnp.dot(whole, wd[...], preferred_element_type=F32).astype(BF16)


def down(hidden, wd, aside, blocks):
    pieces, rows, units = hidden.shape
    block = rows // blocks
    total = (aside.shape[0] + rows, wd.shape[1])
    return pl.pallas_call(
        down_kernel,
        grid=(blocks,),
        in_specs=[
            pl.BlockSpec((pieces, block, units), lambda i: (0, i, 0)),
            pl.BlockSpec(wd.shape, lambda i: (0, 0)),
            pl.BlockSpec(aside.shape, lambda i: (0, 0)),
        ],
        out_specs=pl.BlockSpec(total, lambda i: (0, 0)),
        out_shape=jax.ShapeDtypeStruct(total, BF16),
        name="down",
    )(hidden, wd, aside)


def combine_kernel(returned, table, middle, shared, out):
    total = middle[...].astype(F32) + shared[...]
    rows = returned[...]
    for n in range(table.shape[0]):
        total = total + jnp.dot(table[n], rows, preferred_element_type=F32)
    out[...] = total.astype(BF16)


def combine(returned, table, middle, shared):
    return pl.pallas_call(
        combine_kernel,
        out_shape=jax.ShapeDtypeStruct(middle.shape, BF16),
        name="combine",
    )(returned, table, middle, shared)


def body(
    resid,
    a_val,
    a_gate,
    conv_kernel,
    conv_bias,
    ln_gain,
    ln_bias,
    w_out,
    ffn_gain,
    routes,
    route_weights,
    exp_gate,
    exp_up,
    exp_down,
    sh_gate,
    sh_up,
    sh_down,
):
    tp_count = lax.axis_size("tp")
    tp_place = lax.axis_index("tp")
    sp_count = lax.axis_size("sp")
    tok_rows, model_width = resid.shape
    col_width = model_width // tp_count
    span = conv_kernel.shape[0]
    top_count = routes.shape[1]
    experts_all = exp_gate.shape[0] * sp_count
    capacity = max(2 * tok_rows * top_count // experts_all, tp_count)
    slot_count = experts_all * capacity

    halo = span - 1
    late_val, late_gate = a_val[tok_rows - halo :].astype(F32), a_gate[tok_rows - halo :].astype(F32)
    pairs = [(i, i + 1) for i in range(sp_count - 1)]
    before = lax.ppermute((late_val * jax.nn.sigmoid(late_gate)).astype(BF16), "sp", pairs)

    vectors = [v[None, :] for v in (conv_bias, ln_gain, ln_bias)]
    packed = pack(before, a_val, a_gate, conv_kernel, *vectors, w_out, tp_count)
    spread = lax.all_to_all(packed, "tp", split_axis=0, concat_axis=0, tiled=True)

    routes_late, _ = lax.optimization_barrier((routes, packed[0, :1]))
    slots, pick = routing(routes_late, capacity, slot_count)

    resid_cols = lax.dynamic_slice_in_dim(resid, tp_place * col_width, col_width, 1)
    middle, send = front(span, spread, resid_cols, pick)

    landed = lax.all_to_all(
        send.reshape(sp_count, slot_count // sp_count, col_width),
        "sp",
        split_axis=0,
        concat_axis=0,
        tiled=True,
    ).reshape(slot_count, col_width)
    slots_late, weights_late, _ = lax.optimization_barrier((slots, route_weights, middle[:1]))
    table = weight_table(slots_late, weights_late, slot_count)
    landed, table = lax.optimization_barrier((landed, table))
    first, aside = ASIDE[0], sum(ASIDE)
    gain = ffn_gain[None, :]
    experts = (gain, exp_gate[0], exp_up[0])
    arrived = lax.all_gather(landed[aside:], "tp")
    one = lax.all_gather(jnp.concatenate([landed[:first], middle], axis=0), "tp")
    two = lax.all_gather(landed[first:aside], "tp")
    one, two = side_hidden(one, two, *experts, sh_gate, sh_up, tok_rows)
    arrived, one, two = lax.optimization_barrier((arrived, one, two))
    hidden = hidden_units(arrived, *experts, 3)

    hidden_all = lax.all_gather(hidden, "tp")
    one, two, _ = lax.optimization_barrier((one, two, hidden[:1]))
    side_out, shared = side_down(
        lax.all_gather(one, "tp"), lax.all_gather(two, "tp"), exp_down[0], sh_down, tok_rows
    )
    hidden_all, side_out = lax.optimization_barrier((hidden_all, side_out))
    expert_out = down(hidden_all, exp_down[0], side_out, 3)
    returned = lax.all_to_all(
        expert_out.reshape(sp_count, slot_count // sp_count, col_width),
        "sp",
        split_axis=0,
        concat_axis=0,
        tiled=True,
    ).reshape(slot_count, col_width)
    return combine(returned, table, middle, shared)


def solution(mesh):
    in_specs = (
        P("sp", None),
        P("sp", "tp"),
        P("sp", "tp"),
        P(None, "tp"),
        P("tp"),
        P("tp"),
        P("tp"),
        P("tp", None),
        P(),
        P("sp", None),
        P("sp", None),
        P("sp", None, "tp"),
        P("sp", None, "tp"),
        P("sp", None, "tp"),
        P(None, "tp"),
        P(None, "tp"),
        P(None, "tp"),
    )
    out_specs = P("sp", "tp")
    return jax.shard_map(body, mesh=mesh, in_specs=in_specs, out_specs=out_specs, check_vma=False)
```

```python
import jax
import jax.numpy as jnp
from jax import lax
from jax.experimental import pallas as pl
from jax.experimental.pallas import tpu as pltpu
from jax.sharding import PartitionSpec as P

LN_EPS = 1e-05
RMS_EPS = 1e-06
LANES = 128
F32 = jnp.float32
BF16 = jnp.bfloat16


def silu(v):
    return v / (1.0 + jnp.exp(-v))


def pack_kernel(before, a_val, a_gate, taps, bias, gain, shift, out, win, params):
    peers = out.shape[0]
    halo, half = before.shape
    rows = win.shape[0]
    win[...] = jnp.zeros(win.shape, F32)
    params[...] = jnp.zeros(params.shape, F32)
    gate = 1.0 / (1.0 + jnp.exp(-a_gate[...].astype(F32)))
    win[0:halo, :] = before[...].astype(F32)
    win[halo : halo + a_val.shape[0], :] = a_val[...].astype(F32) * gate
    span = taps.shape[0]
    params[0:span, :] = taps[...].astype(F32)
    for n, vector in enumerate((bias, gain, shift)):
        rest = vector[...]
        for part in range(3):
            kept = rest.astype(BF16).astype(F32)
            at = span + 3 * n + part
            params[at : at + 1, :] = kept
            rest = rest - kept

    def folded(v):
        n = v.shape[0] // 2
        return jnp.concatenate([v[0:n, :], v[n : 2 * n, :]], axis=1).astype(BF16)

    head, tail = folded(win[...]), folded(params[...])
    top = rows // 2
    for t in range(peers):
        out[t, 0:top, :] = head
        out[t, top:, :] = tail


PARAM_ROWS = 64
FOLDED = 16
DOWN_BLOCKS = 3
ASIDE = (64, 96)


def window_rows(span, tok_rows):
    return -(-(span - 1 + tok_rows) // 32) * 32


def pack(before, a_val, a_gate, taps, bias, gain, shift, peers):
    rows = window_rows(taps.shape[0], a_val.shape[0])
    total = (rows + PARAM_ROWS) // 2
    return pl.pallas_call(
        pack_kernel,
        out_shape=jax.ShapeDtypeStruct((peers, total, LANES), BF16),
        scratch_shapes=[
            pltpu.VMEM((rows, a_val.shape[1]), F32),
            pltpu.VMEM((PARAM_ROWS, a_val.shape[1]), F32),
        ],
        name="pack",
    )(before, a_val, a_gate, taps, bias, gain, shift)


def routing_kernel(capacity, routes, slots_out, pick_out):
    tok_rows, top_count = routes.shape
    slot_count = pick_out.shape[0]
    experts = slot_count // capacity
    ids = lax.broadcasted_iota(jnp.int32, (tok_rows, experts), 1)
    hits = [ids == routes[:, k : k + 1] for k in range(top_count)]
    named = sum(jnp.where(h, 1.0, 0.0) for h in hits).astype(BF16)
    square = (tok_rows, tok_rows)
    below = lax.broadcasted_iota(jnp.int32, square, 0) > lax.broadcasted_iota(jnp.int32, square, 1)
    earlier = jnp.dot(jnp.where(below, 1.0, 0.0).astype(BF16), named, preferred_element_type=F32)
    wide = lax.broadcasted_iota(jnp.int32, (tok_rows, slot_count), 1)
    lane = lax.broadcasted_iota(jnp.int32, slots_out.shape, 1)
    slots = jnp.zeros(slots_out.shape, jnp.int32)
    pick = jnp.zeros(wide.shape, F32)
    for k in range(top_count):
        place = jnp.sum(jnp.where(hits[k], earlier, 0.0), axis=1, keepdims=True).astype(jnp.int32)
        slot = routes[:, k : k + 1] * capacity + place
        slots = jnp.where(lane == k, slot, slots)
        pick = jnp.where(wide == slot, 1.0, pick)
    slots_out[...] = slots
    for at in range(0, slot_count, tok_rows):
        pick_out[at : at + tok_rows, :] = pick[:, at : at + tok_rows].T.astype(BF16)


def routing(routes, capacity, slot_count):
    tok_rows, top_count = routes.shape

    def kernel(*refs):
        routing_kernel(capacity, *refs)

    return pl.pallas_call(
        kernel,
        out_shape=(
            jax.ShapeDtypeStruct((tok_rows, top_count), jnp.int32),
            jax.ShapeDtypeStruct((slot_count, tok_rows), BF16),
        ),
        name="routing",
    )(routes)


def table_kernel(slots, weights, out):
    shape = out.shape[1:]
    ids = lax.broadcasted_iota(jnp.int32, shape, 1)
    table = jnp.zeros(shape, F32)
    for k in range(slots.shape[1]):
        table = jnp.where(ids == slots[:, k : k + 1], weights[:, k : k + 1], table)
    for n in range(out.shape[0]):
        part = table.astype(BF16)
        out[n] = part
        table = table - part.astype(F32)


def weight_table(slots, weights, slot_count):
    return pl.pallas_call(
        table_kernel,
        out_shape=jax.ShapeDtypeStruct((3, slots.shape[0], slot_count), BF16),
        name="table",
    )(slots, weights)


def front_kernel(span, packed, wcol, resid, pick, middle_out, send_out, win, params, conv):
    peers = packed.shape[0]
    tok_rows = resid.shape[0]
    half = LANES // 2
    channels = peers * half
    top = win.shape[0] // 2
    fold = PARAM_ROWS // 2
    for pair in range(peers // 2):
        at = slice(pair * LANES, (pair + 1) * LANES)
        one, two = packed[2 * pair, 0 : top + fold, :], packed[2 * pair + 1, 0 : top + fold, :]
        left = jnp.concatenate([one[:, :half], two[:, :half]], axis=1).astype(F32)
        right = jnp.concatenate([one[:, half:], two[:, half:]], axis=1).astype(F32)
        win[0:top, at], win[top : 2 * top, at] = left[0:top], right[0:top]
        params[0:fold, at], params[fold : 2 * fold, at] = left[top:], right[top:]

    def vector(first, cols=slice(None)):
        return sum(params[first + i : first + i + 1, cols] for i in range(3))

    conv_rows = 64

    def one_block(i, _):
        cols = pl.ds(pl.multiple_of(i * LANES, LANES), LANES)
        taps = params[0:span, cols]
        b = vector(span, cols)
        for r in range(0, tok_rows, conv_rows):
            acc = jnp.broadcast_to(b, (conv_rows, LANES))
            for j in range(span):
                acc = acc + taps[j : j + 1, :] * win[r + j : r + j + conv_rows, cols]
            conv[r : r + conv_rows, cols] = acc
        return 0

    lax.fori_loop(0, channels // LANES, one_block, 0)
    gain = vector(span + 3)
    shift = vector(span + 6)
    for r in range(0, tok_rows, 64):
        c = conv[r : r + 64, :]
        mean = jnp.sum(c, axis=1, keepdims=True) * (1.0 / channels)
        var = jnp.sum(c * c, axis=1, keepdims=True) * (1.0 / channels) - mean * mean
        scaled = (c - mean) * lax.rsqrt(var + LN_EPS) * gain + shift
        mixed = silu(scaled).astype(BF16)
        proj = jnp.dot(mixed, wcol[...], preferred_element_type=F32)
        middle_out[r : r + 64, :] = (resid[r : r + 64, :].astype(F32) + proj).astype(BF16)
    middle = middle_out[...]
    send_out[...] = jnp.dot(pick[...], middle, preferred_element_type=F32).astype(BF16)


def front(span, packed, wcol, resid, pick):
    tok_rows, cols = resid.shape
    channels = packed.shape[0] * LANES // 2

    def kernel(*refs):
        front_kernel(span, *refs)

    return pl.pallas_call(
        kernel,
        out_shape=(
            jax.ShapeDtypeStruct((tok_rows, cols), BF16),
            jax.ShapeDtypeStruct((pick.shape[0], cols), BF16),
        ),
        scratch_shapes=[
            pltpu.VMEM((window_rows(span, tok_rows), channels), F32),
            pltpu.VMEM((PARAM_ROWS, channels), F32),
            pltpu.VMEM((tok_rows, channels), F32),
        ],
        name="front",
    )(packed, wcol, resid, pick)


def normed_rows(pieces, width, gain):
    squares = jnp.zeros(pieces[0].shape, F32)
    for x in pieces:
        squares = squares + x.astype(F32) * x.astype(F32)
    mean = jnp.sum(squares, axis=1, keepdims=True) / width
    inverse = lax.rsqrt(mean + RMS_EPS)
    cols = [gain[:, n * LANES : (n + 1) * LANES] for n in range(len(pieces))]
    scaled = [(x.astype(F32) * inverse * c).astype(BF16) for x, c in zip(pieces, cols)]
    return jnp.concatenate(scaled, axis=1)


def gated_units(rows, w_gate, w_up):
    g = jnp.dot(rows, w_gate, preferred_element_type=F32)
    u = jnp.dot(rows, w_up, preferred_element_type=F32)
    return (silu(g) * u).astype(BF16)


def hidden_kernel(rows_in, gain, wg, wu, aside_out, out):
    step = pl.program_id(0)
    block = rows_in.shape[1]
    aside = aside_out.shape[0]
    rows = normed_rows([rows_in[t] for t in range(rows_in.shape[0])], wg.shape[0], gain)
    units = gated_units(rows, wg[...], wu[...])

    @pl.when(step == 0)
    def _():
        aside_out[...] = units[0:aside, :]
        out[0 : block - aside, :] = units[aside:, :]

    @pl.when(step > 0)
    def _():
        out[pl.ds(pl.multiple_of(step * block - aside, 16), block), :] = units


def hidden_units(rows_in, gain, wg, wu, blocks, aside):
    pieces, rows, lanes = rows_in.shape
    width, units = wg.shape
    block = rows // blocks
    return pl.pallas_call(
        hidden_kernel,
        grid=(blocks,),
        in_specs=[
            pl.BlockSpec((pieces, block, lanes), lambda i: (0, i, 0)),
            pl.BlockSpec((1, width), lambda i: (0, 0)),
            pl.BlockSpec((width, units), lambda i: (0, 0)),
            pl.BlockSpec((width, units), lambda i: (0, 0)),
        ],
        out_specs=[
            pl.BlockSpec((aside, units), lambda i: (0, 0)),
            pl.BlockSpec((rows - aside, units), lambda i: (0, 0)),
        ],
        out_shape=(
            jax.ShapeDtypeStruct((aside, units), BF16),
            jax.ShapeDtypeStruct((rows - aside, units), BF16),
        ),
        name="hidden",
    )(rows_in, gain, wg, wu)


def side_hidden_kernel(one, gain, wg, wu, sg, su, out):
    width, units = wg.shape
    few = sg.shape[1]
    slots = out.shape[0] - FOLDED
    rows = normed_rows([one[t] for t in range(one.shape[0])], width, gain)
    out[0:slots, :] = gated_units(rows[0:slots, :], wg[...], wu[...])
    shared = gated_units(rows[slots:, :], sg[...], su[...])
    parts = [shared[j * FOLDED : (j + 1) * FOLDED, :].astype(F32) for j in range(units // few)]
    out[slots:, :] = jnp.concatenate(parts, axis=1).astype(BF16)


def side_hidden(one, gain, wg, wu, sg, su, tok_rows):
    slots = one.shape[1] - tok_rows
    return pl.pallas_call(
        side_hidden_kernel,
        out_shape=jax.ShapeDtypeStruct((slots + FOLDED, wg.shape[1]), BF16),
        name="side_hidden",
    )(one, gain, wg, wu, sg, su)


def side_down_kernel(one, two, wd, sh_down, out, shared_out):
    peers, rows, units = one.shape
    slots = rows - FOLDED
    few = sh_down.shape[0] // peers
    folds = units // few
    whole = jnp.concatenate([one[t, 0:slots, :] for t in range(peers)], axis=1)
    out[0:slots, :] = jnp.dot(whole, wd[...], preferred_element_type=F32).astype(BF16)
    whole = jnp.concatenate([two[t] for t in range(peers)], axis=1)
    out[slots:, :] = jnp.dot(whole, wd[...], preferred_element_type=F32).astype(BF16)
    shape = (folds * FOLDED, units)
    own = lax.broadcasted_iota(jnp.int32, shape, 0) // FOLDED == lax.broadcasted_iota(jnp.int32, shape, 1) // few
    shared = jnp.zeros(shared_out.shape, F32)
    for t in range(peers):
        packed = one[t, slots:, :].astype(F32)
        spread = jnp.where(own, jnp.concatenate([packed] * folds, axis=0), 0.0).astype(BF16)
        weights = jnp.concatenate([sh_down[t * few : (t + 1) * few, :]] * folds, axis=0)
        shared = shared + jnp.dot(spread, weights, preferred_element_type=F32)
    shared_out[...] = shared


def side_down(one, two, wd, sh_down, tok_rows):
    slots = one.shape[1] - FOLDED + two.shape[1]
    return pl.pallas_call(
        side_down_kernel,
        out_shape=(
            jax.ShapeDtypeStruct((slots, wd.shape[1]), BF16),
            jax.ShapeDtypeStruct((tok_rows, wd.shape[1]), F32),
        ),
        name="side_down",
    )(one, two, wd, sh_down)


def down_kernel(hidden, wd, aside, out):
    slots = aside.shape[0]
    block = hidden.shape[1]
    step = pl.program_id(0)

    @pl.when(step == 0)
    def _():
        out[0:slots, :] = aside[...]

    whole = jnp.concatenate([hidden[t] for t in range(hidden.shape[0])], axis=1)
    at = pl.ds(pl.multiple_of(slots + step * block, 16), block)
    out[at, :] = jnp.dot(whole, wd[...], preferred_element_type=F32).astype(BF16)


def down(hidden, wd, aside, blocks):
    pieces, rows, units = hidden.shape
    block = rows // blocks
    total = (aside.shape[0] + rows, wd.shape[1])
    return pl.pallas_call(
        down_kernel,
        grid=(blocks,),
        in_specs=[
            pl.BlockSpec((pieces, block, units), lambda i: (0, i, 0)),
            pl.BlockSpec(wd.shape, lambda i: (0, 0)),
            pl.BlockSpec(aside.shape, lambda i: (0, 0)),
        ],
        out_specs=pl.BlockSpec(total, lambda i: (0, 0)),
        out_shape=jax.ShapeDtypeStruct(total, BF16),
        name="down",
    )(hidden, wd, aside)


def combine_kernel(returned, table, middle, shared, out):
    total = middle[...].astype(F32) + shared[...]
    rows = returned[...]
    for n in range(table.shape[0]):
        total = total + jnp.dot(table[n], rows, preferred_element_type=F32)
    out[...] = total.astype(BF16)


def combine(returned, table, middle, shared):
    return pl.pallas_call(
        combine_kernel,
        out_shape=jax.ShapeDtypeStruct(middle.shape, BF16),
        name="combine",
    )(returned, table, middle, shared)


def body(
    resid,
    a_val,
    a_gate,
    conv_kernel,
    conv_bias,
    ln_gain,
    ln_bias,
    w_out,
    ffn_gain,
    routes,
    route_weights,
    exp_gate,
    exp_up,
    exp_down,
    sh_gate,
    sh_up,
    sh_down,
):
    tp_count = lax.axis_size("tp")
    tp_place = lax.axis_index("tp")
    sp_count = lax.axis_size("sp")
    tok_rows, model_width = resid.shape
    col_width = model_width // tp_count
    span = conv_kernel.shape[0]
    top_count = routes.shape[1]
    experts_all = exp_gate.shape[0] * sp_count
    capacity = max(2 * tok_rows * top_count // experts_all, tp_count)
    slot_count = experts_all * capacity

    w_parts = jnp.moveaxis(w_out.reshape(w_out.shape[0], tp_count, col_width), 1, 0)
    wcol = lax.all_to_all(w_parts, "tp", split_axis=0, concat_axis=0, tiled=True)
    wcol = wcol.reshape(w_out.shape[0] * tp_count, col_width)

    halo = span - 1
    late_val, late_gate = a_val[tok_rows - halo :].astype(F32), a_gate[tok_rows - halo :].astype(F32)
    pairs = [(i, i + 1) for i in range(sp_count - 1)]
    before = lax.ppermute((late_val * jax.nn.sigmoid(late_gate)).astype(BF16), "sp", pairs)

    vectors = [v[None, :] for v in (conv_bias, ln_gain, ln_bias)]
    packed = pack(before, a_val, a_gate, conv_kernel, *vectors, tp_count)
    spread = lax.all_to_all(packed, "tp", split_axis=0, concat_axis=0, tiled=True)

    routes_late, _ = lax.optimization_barrier((routes, packed[0, :1]))
    slots, pick = routing(routes_late, capacity, slot_count)

    resid_cols = lax.dynamic_slice_in_dim(resid, tp_place * col_width, col_width, 1)
    middle, send = front(span, spread, wcol, resid_cols, pick)

    landed = lax.all_to_all(
        send.reshape(sp_count, slot_count // sp_count, col_width),
        "sp",
        split_axis=0,
        concat_axis=0,
        tiled=True,
    ).reshape(slot_count, col_width)
    slots_late, weights_late, _ = lax.optimization_barrier((slots, route_weights, middle[:1]))
    table = weight_table(slots_late, weights_late, slot_count)
    landed, table = lax.optimization_barrier((landed, table))
    first = ASIDE[0]
    gain = ffn_gain[None, :]
    experts = (gain, exp_gate[0], exp_up[0])
    arrived = lax.all_gather(landed[first:], "tp")
    one = lax.all_gather(jnp.concatenate([landed[:first], middle], axis=0), "tp")
    one = side_hidden(one, *experts, sh_gate, sh_up, tok_rows)
    arrived, one = lax.optimization_barrier((arrived, one))
    two, hidden = hidden_units(arrived, *experts, 4, ASIDE[1])

    hidden_all = lax.all_gather(hidden, "tp")
    one, two = lax.optimization_barrier((one, two))
    side_out, shared = side_down(
        lax.all_gather(one, "tp"), lax.all_gather(two, "tp"), exp_down[0], sh_down, tok_rows
    )
    hidden_all, side_out = lax.optimization_barrier((hidden_all, side_out))
    expert_out = down(hidden_all, exp_down[0], side_out, DOWN_BLOCKS)
    returned = lax.all_to_all(
        expert_out.reshape(sp_count, slot_count // sp_count, col_width),
        "sp",
        split_axis=0,
        concat_axis=0,
        tiled=True,
    ).reshape(slot_count, col_width)
    return combine(returned, table, middle, shared)


def solution(mesh):
    in_specs = (
        P("sp", None),
        P("sp", "tp"),
        P("sp", "tp"),
        P(None, "tp"),
        P("tp"),
        P("tp"),
        P("tp"),
        P("tp", None),
        P(),
        P("sp", None),
        P("sp", None),
        P("sp", None, "tp"),
        P("sp", None, "tp"),
        P("sp", None, "tp"),
        P(None, "tp"),
        P(None, "tp"),
        P(None, "tp"),
    )
    out_specs = P("sp", "tp")
    return jax.shard_map(body, mesh=mesh, in_specs=in_specs, out_specs=out_specs, check_vma=False)
```

```python
import jax
import jax.numpy as jnp
from jax import lax
from jax.experimental import pallas as pl
from jax.experimental.pallas import tpu as pltpu
from jax.sharding import PartitionSpec as P

LN_EPS = 1e-05
RMS_EPS = 1e-06
LANES = 128
F32 = jnp.float32
BF16 = jnp.bfloat16


def silu(v):
    return v / (1.0 + jnp.exp(-v))


def pack_kernel(before, a_val, a_gate, taps, bias, gain, shift, w_out, out, win, params):
    peers, _, lanes = out.shape
    halo, half = before.shape
    rows = win.shape[0]
    win[...] = jnp.zeros(win.shape, F32)
    params[...] = jnp.zeros(params.shape, F32)
    gate = 1.0 / (1.0 + jnp.exp(-a_gate[...].astype(F32)))
    win[0:halo, :] = before[...].astype(F32)
    win[halo : halo + a_val.shape[0], :] = a_val[...].astype(F32) * gate
    span = taps.shape[0]
    params[0:span, :] = taps[...].astype(F32)
    for n, vector in enumerate((bias, gain, shift)):
        rest = vector[...]
        for part in range(3):
            kept = rest.astype(BF16).astype(F32)
            at = span + 3 * n + part
            params[at : at + 1, :] = kept
            rest = rest - kept

    def folded(v):
        n = v.shape[0] // 2
        return jnp.concatenate([v[0:n, :], v[n : 2 * n, :]], axis=1).astype(BF16)

    head, tail = folded(win[...]), folded(params[...])
    top = rows // 2
    low = top + tail.shape[0]
    for t in range(peers):
        out[t, 0:top, :] = head
        out[t, top:low, :] = tail
        out[t, low : low + w_out.shape[0], :] = w_out[:, t * lanes : (t + 1) * lanes]


PARAM_ROWS = 64


def window_rows(span, tok_rows):
    return -(-(span - 1 + tok_rows) // 32) * 32


def pack(before, a_val, a_gate, taps, bias, gain, shift, w_out, peers):
    rows = window_rows(taps.shape[0], a_val.shape[0])
    lanes = w_out.shape[1] // peers
    total = rows // 2 + PARAM_ROWS // 2 + w_out.shape[0]
    return pl.pallas_call(
        pack_kernel,
        out_shape=jax.ShapeDtypeStruct((peers, total, lanes), BF16),
        scratch_shapes=[
            pltpu.VMEM((rows, a_val.shape[1]), F32),
            pltpu.VMEM((PARAM_ROWS, a_val.shape[1]), F32),
        ],
        name="pack",
    )(before, a_val, a_gate, taps, bias, gain, shift, w_out)


def routing_kernel(capacity, routes, slots_out, pick_out):
    tok_rows, top_count = routes.shape
    experts = pick_out.shape[1] // capacity
    ids = lax.broadcasted_iota(jnp.int32, (tok_rows, experts), 1)
    hits = [ids == routes[:, k : k + 1] for k in range(top_count)]
    named = sum(jnp.where(h, 1.0, 0.0) for h in hits).astype(BF16)
    square = (tok_rows, tok_rows)
    below = lax.broadcasted_iota(jnp.int32, square, 0) > lax.broadcasted_iota(jnp.int32, square, 1)
    earlier = jnp.dot(jnp.where(below, 1.0, 0.0).astype(BF16), named, preferred_element_type=F32)
    wide = lax.broadcasted_iota(jnp.int32, pick_out.shape, 1)
    lane = lax.broadcasted_iota(jnp.int32, slots_out.shape, 1)
    slots = jnp.zeros(slots_out.shape, jnp.int32)
    pick = jnp.zeros(pick_out.shape, F32)
    for k in range(top_count):
        place = jnp.sum(jnp.where(hits[k], earlier, 0.0), axis=1, keepdims=True).astype(jnp.int32)
        slot = routes[:, k : k + 1] * capacity + place
        slots = jnp.where(lane == k, slot, slots)
        pick = jnp.where(wide == slot, 1.0, pick)
    slots_out[...] = slots
    pick_out[...] = pick.astype(BF16)


def routing(routes, capacity, slot_count):
    tok_rows, top_count = routes.shape

    def kernel(*refs):
        routing_kernel(capacity, *refs)

    return pl.pallas_call(
        kernel,
        out_shape=(
            jax.ShapeDtypeStruct((tok_rows, top_count), jnp.int32),
            jax.ShapeDtypeStruct((tok_rows, slot_count), BF16),
        ),
        name="routing",
    )(routes)


def table_kernel(slots, weights, out):
    shape = out.shape[1:]
    ids = lax.broadcasted_iota(jnp.int32, shape, 1)
    table = jnp.zeros(shape, F32)
    for k in range(slots.shape[1]):
        table = jnp.where(ids == slots[:, k : k + 1], weights[:, k : k + 1], table)
    for n in range(out.shape[0]):
        part = table.astype(BF16)
        out[n] = part
        table = table - part.astype(F32)


def weight_table(slots, weights, slot_count):
    return pl.pallas_call(
        table_kernel,
        out_shape=jax.ShapeDtypeStruct((3, slots.shape[0], slot_count), BF16),
        name="table",
    )(slots, weights)


def front_kernel(span, packed, resid, pick, middle_out, send_out, win, params, conv):
    peers = packed.shape[0]
    tok_rows = resid.shape[0]
    half = LANES // 2
    channels = peers * half
    top = win.shape[0] // 2
    fold = PARAM_ROWS // 2
    for pair in range(peers // 2):
        at = slice(pair * LANES, (pair + 1) * LANES)
        one, two = packed[2 * pair, 0 : top + fold, :], packed[2 * pair + 1, 0 : top + fold, :]
        left = jnp.concatenate([one[:, :half], two[:, :half]], axis=1).astype(F32)
        right = jnp.concatenate([one[:, half:], two[:, half:]], axis=1).astype(F32)
        win[0:top, at], win[top : 2 * top, at] = left[0:top], right[0:top]
        params[0:fold, at], params[fold : 2 * fold, at] = left[top:], right[top:]

    def vector(first, cols=slice(None)):
        return sum(params[first + i : first + i + 1, cols] for i in range(3))

    conv_rows = 64

    def one_block(i, _):
        cols = pl.ds(pl.multiple_of(i * LANES, LANES), LANES)
        taps = params[0:span, cols]
        b = vector(span, cols)
        for r in range(0, tok_rows, conv_rows):
            acc = jnp.broadcast_to(b, (conv_rows, LANES))
            for j in range(span):
                acc = acc + taps[j : j + 1, :] * win[r + j : r + j + conv_rows, cols]
            conv[r : r + conv_rows, cols] = acc
        return 0

    lax.fori_loop(0, channels // LANES, one_block, 0)
    gain = vector(span + 3)
    shift = vector(span + 6)
    wcol = packed[:, top + fold :, :].reshape(channels, packed.shape[2])
    for r in range(0, tok_rows, 64):
        c = conv[r : r + 64, :]
        mean = jnp.sum(c, axis=1, keepdims=True) * (1.0 / channels)
        var = jnp.sum(c * c, axis=1, keepdims=True) * (1.0 / channels) - mean * mean
        scaled = (c - mean) * lax.rsqrt(var + LN_EPS) * gain + shift
        mixed = silu(scaled).astype(BF16)
        proj = jnp.dot(mixed, wcol, preferred_element_type=F32)
        middle_out[r : r + 64, :] = (resid[r : r + 64, :].astype(F32) + proj).astype(BF16)
    middle = middle_out[...]
    dims = (((0,), (0,)), ((), ()))
    send_out[...] = lax.dot_general(pick[...], middle, dims, preferred_element_type=F32).astype(BF16)


def front(span, packed, resid, pick):
    tok_rows, cols = resid.shape
    channels = packed.shape[0] * LANES // 2

    def kernel(*refs):
        front_kernel(span, *refs)

    return pl.pallas_call(
        kernel,
        out_shape=(
            jax.ShapeDtypeStruct((tok_rows, cols), BF16),
            jax.ShapeDtypeStruct((pick.shape[1], cols), BF16),
        ),
        scratch_shapes=[
            pltpu.VMEM((window_rows(span, tok_rows), channels), F32),
            pltpu.VMEM((PARAM_ROWS, channels), F32),
            pltpu.VMEM((tok_rows, channels), F32),
        ],
        name="front",
    )(packed, resid, pick)


def ring_gather(value, work):
    size = lax.axis_size("tp")
    steps = size // 4
    ring = [(i, (i + (2 if i % 2 == 0 else -2)) % size) for i in range(size)]
    swap = [(i, i ^ 1) for i in range(size)]

    def moved(v):
        return lax.ppermute(v, "tp", ring)

    def swapped(v):
        return lax.ppermute(v, "tp", swap)

    own = value[None]
    pair = jnp.concatenate([own, swapped(own)], axis=0)
    arrays = [pair]
    for step in range(1, steps):
        before, pair = pair, moved(pair)
        if step > 1:
            pair, other = lax.optimization_barrier((pair, swapped(before)))
            arrays.append(other)
        arrays.append(pair)
    far, other = moved(pair[:1]), swapped(pair)
    made = work(arrays)
    far, other, *made = lax.optimization_barrier((far, other, *made))
    return made, [other, far, swapped(far)]


def places_of(place, size):
    chips = size // 2
    chip, core = place // 2, place % 2
    way = 2 * core - 1
    at = [2 * chip + core, 2 * chip + 1 - core]
    there = []
    for step in range(1, chips // 2):
        here = 2 * lax.rem(chip + way * step + chips, chips)
        at += [*there, here + core, here + 1 - core]
        beyond = 2 * lax.rem(chip - way * step + chips, chips)
        there = [beyond + 1 - core, beyond + core]
    far = 2 * lax.rem(chip + chips // 2, chips)
    return [*at, *there, far + core, far + 1 - core]


def piece(at, width):
    return pl.ds(pl.multiple_of(at * width, width), width)


def split(refs):
    return [x[n] for x in refs for n in range(x.shape[0])]


def products(parts, where, gain, weights, scratch):
    squares = jnp.zeros(parts[0].shape, F32)
    for n, (x, at) in enumerate(zip(parts, where)):
        wide = x.astype(F32)
        squares = squares + wide * wide
        scratch[0:x.shape[0], n * LANES : (n + 1) * LANES] = (wide * gain[:, piece(at, LANES)]).astype(BF16)
    total = jnp.sum(squares, axis=1, keepdims=True)
    rows = scratch[0 : parts[0].shape[0], 0 : len(parts) * LANES]
    return total, [
        jnp.dot(rows, w[0 : len(parts) * LANES, :], preferred_element_type=F32) for w in weights
    ]


def slots_kernel(first, count, width, size, place, *refs):
    now, late = refs[:count], refs[count : 2 * count]
    total = sum(x.shape[0] for x in now)
    where = places_of(place[0], size)[first : first + total]
    last = first + total == size
    gain, wg, wu, sg, su = refs[2 * count : 2 * count + 5]
    rest = refs[2 * count + 5 :]
    if last:
        before, rest = rest[:6], rest[6:]
    outs, scratches = rest[: 2 if last else 6], rest[2 if last else 6 :]
    scratch, pg, pu, qg, qu = scratches
    step = pl.program_id(0)

    @pl.when(step == 0)
    def _():
        for n, at in enumerate(where):
            for source, target in ((wg, pg), (wu, pu), (sg, qg), (su, qu)):
                target[n * LANES : (n + 1) * LANES, :] = source[piece(at, LANES), :]

    def block(parts, one, two, prior):
        total, (g, u) = products(split(parts), where, gain, (one, two), scratch)
        if prior is not None:
            g, u, total = g + prior[0][...], u + prior[1][...], total + prior[2][:, 0:1]
        return g, u, total

    def finished(g, u, total):
        inverse = lax.rsqrt(total / width + RMS_EPS)
        return (silu(g * inverse) * (u * inverse)).astype(BF16)

    g, u, total = block(now, pg, pu, before[:3] if last else None)
    if last:
        outs[0][...] = finished(g, u, total)
    else:
        outs[0][...], outs[1][...] = g, u
        outs[2][...] = jnp.broadcast_to(total, outs[2].shape)

    @pl.when(step == 0)
    def _():
        g, u, total = block(late, qg, qu, before[3:] if last else None)
        if last:
            outs[1][...] = finished(g, u, total)
        else:
            outs[3][...], outs[4][...] = g, u
            outs[5][...] = jnp.broadcast_to(total, outs[5].shape)


def slots_lot(pieces, first, size, place, rows, gain, wg, wu, sg, su, before=()):
    block = rows // 4
    late_rows = pieces[0].shape[1] - rows
    late_at = rows // late_rows
    width, units = wg.shape
    few = sg.shape[1]
    count = len(pieces)
    lanes = sum(p.shape[0] for p in pieces) * LANES

    def kernel(*refs):
        slots_kernel(first, count, width, size, *refs)

    def whole(shape):
        return pl.BlockSpec(shape, lambda i, p: (0, 0))

    def by_rows(lanes):
        return pl.BlockSpec((block, lanes), lambda i, p: (i, 0))

    sums = [by_rows(units), by_rows(units), by_rows(LANES)]
    sums += [whole((late_rows, few)), whole((late_rows, few)), whole((late_rows, LANES))]
    shapes = [(rows, units), (rows, units), (rows, LANES)]
    shapes += [(late_rows, few), (late_rows, few), (late_rows, LANES)]
    if before:
        out_specs = [by_rows(units), whole((late_rows, few))]
        out_shape = [
            jax.ShapeDtypeStruct((rows, units), BF16),
            jax.ShapeDtypeStruct((late_rows, few), BF16),
        ]
    else:
        out_specs, out_shape = sums, [jax.ShapeDtypeStruct(s, F32) for s in shapes]
    return pl.pallas_call(
        kernel,
        grid_spec=pltpu.PrefetchScalarGridSpec(
            num_scalar_prefetch=1,
            grid=(4,),
            in_specs=[pl.BlockSpec((p.shape[0], block, LANES), lambda i, p: (0, i, 0)) for p in pieces]
            + [
                pl.BlockSpec((p.shape[0], late_rows, LANES), lambda i, p: (0, late_at, 0))
                for p in pieces
            ]
            + [whole(gain.shape), whole(wg.shape), whole(wu.shape), whole(sg.shape), whole(su.shape)]
            + (sums if before else []),
            out_specs=out_specs,
            scratch_shapes=[pltpu.VMEM((block, lanes), BF16)]
            + [pltpu.VMEM((lanes, n), BF16) for n in (units, units, few, few)],
        ),
        out_shape=out_shape,
        name="slots_lot",
    )(place, *pieces, *pieces, gain, wg, wu, sg, su, *before)


def down_kernel(first, count, size, place, *refs):
    pieces, wd, rest = refs[:count], refs[count], refs[count + 1 :]
    where = places_of(place[0], size)[first : first + sum(x.shape[0] for x in pieces)]
    before = rest[0] if len(rest) == 4 else None
    out, rows, weights = rest[-3:]
    units = pieces[0].shape[2]

    @pl.when(pl.program_id(0) == 0)
    def _():
        for n, at in enumerate(where):
            weights[n * units : (n + 1) * units, :] = wd[piece(at, units), :]

    for n, x in enumerate(split(pieces)):
        rows[:, n * units : (n + 1) * units] = x
    total = jnp.dot(rows[...], weights[...], preferred_element_type=F32)
    if before is not None:
        total = total + before[...]
    out[...] = total.astype(out.dtype)


def down_lot(pieces, first, size, place, wd, before=None):
    _, rows, units = pieces[0].shape
    block = rows // 4
    count = len(pieces)
    lanes = sum(p.shape[0] for p in pieces) * units
    cols = wd.shape[1]

    def kernel(*refs):
        down_kernel(first, count, size, *refs)

    given = [] if before is None else [before]
    return pl.pallas_call(
        kernel,
        grid_spec=pltpu.PrefetchScalarGridSpec(
            num_scalar_prefetch=1,
            grid=(4,),
            in_specs=[pl.BlockSpec((p.shape[0], block, units), lambda i, p: (0, i, 0)) for p in pieces]
            + [pl.BlockSpec(wd.shape, lambda i, p: (0, 0))]
            + [pl.BlockSpec((block, cols), lambda i, p: (i, 0)) for _ in given],
            out_specs=pl.BlockSpec((block, cols), lambda i, p: (i, 0)),
            scratch_shapes=[
                pltpu.VMEM((block, lanes), BF16),
                pltpu.VMEM((lanes, cols), BF16),
            ],
        ),
        out_shape=jax.ShapeDtypeStruct((rows, cols), F32 if before is None else BF16),
        name="down_lot",
    )(place, *pieces, wd, *given)


def combine_kernel(returned, table, middle, shared_hidden, sh_down, out):
    units = shared_hidden.shape[2]
    total = middle[...].astype(F32)
    for n in range(shared_hidden.shape[0]):
        part = sh_down[n * units : (n + 1) * units, :]
        total = total + jnp.dot(shared_hidden[n], part, preferred_element_type=F32)
    rows = returned[...]
    for n in range(table.shape[0]):
        total = total + jnp.dot(table[n], rows, preferred_element_type=F32)
    out[...] = total.astype(BF16)


def combine(returned, table, middle, shared_hidden, sh_down):
    return pl.pallas_call(
        combine_kernel,
        out_shape=jax.ShapeDtypeStruct(middle.shape, BF16),
        name="combine",
    )(returned, table, middle, shared_hidden, sh_down)


def body(
    resid,
    a_val,
    a_gate,
    conv_kernel,
    conv_bias,
    ln_gain,
    ln_bias,
    w_out,
    ffn_gain,
    routes,
    route_weights,
    exp_gate,
    exp_up,
    exp_down,
    sh_gate,
    sh_up,
    sh_down,
):
    tp_count = lax.axis_size("tp")
    tp_place = lax.axis_index("tp")
    sp_count = lax.axis_size("sp")
    tok_rows, model_width = resid.shape
    col_width = model_width // tp_count
    span = conv_kernel.shape[0]
    top_count = routes.shape[1]
    experts_all = exp_gate.shape[0] * sp_count
    capacity = max(2 * tok_rows * top_count // experts_all, tp_count)
    slot_count = experts_all * capacity

    halo = span - 1
    late_val, late_gate = a_val[tok_rows - halo :].astype(F32), a_gate[tok_rows - halo :].astype(F32)
    pairs = [(i, i + 1) for i in range(sp_count - 1)]
    before = lax.ppermute((late_val * jax.nn.sigmoid(late_gate)).astype(BF16), "sp", pairs)

    vectors = [v[None, :] for v in (conv_bias, ln_gain, ln_bias)]
    packed = pack(before, a_val, a_gate, conv_kernel, *vectors, w_out, tp_count)
    spread = lax.all_to_all(packed, "tp", split_axis=0, concat_axis=0, tiled=True)

    routes_late, _ = lax.optimization_barrier((routes, packed[0, :1]))
    slots, pick = routing(routes_late, capacity, slot_count)

    resid_cols = lax.dynamic_slice_in_dim(resid, tp_place * col_width, col_width, 1)
    middle, send = front(span, spread, resid_cols, pick)

    landed = lax.all_to_all(
        send.reshape(sp_count, slot_count // sp_count, col_width),
        "sp",
        split_axis=0,
        concat_axis=0,
        tiled=True,
    ).reshape(slot_count, col_width)
    slots_late, weights_late, _ = lax.optimization_barrier((slots, route_weights, middle[:1]))
    table = weight_table(slots_late, weights_late, slot_count)
    landed, table = lax.optimization_barrier((landed, table))
    place = tp_place.reshape(1).astype(jnp.int32)
    fixed = (slot_count, ffn_gain[None, :], exp_gate[0], exp_up[0], sh_gate, sh_up)
    firsts = []

    def slots_begun(pieces):
        firsts.append(sum(p.shape[0] for p in pieces))
        return slots_lot(pieces, 0, tp_count, place, *fixed)

    sums, pieces = ring_gather(jnp.concatenate([landed, middle], axis=0), slots_begun)
    hidden, shared_hidden = slots_lot(pieces, firsts[0], tp_count, place, *fixed, before=sums)

    def down_begun(pieces):
        return (down_lot(pieces, 0, tp_count, place, exp_down[0]),)

    sums, pieces = ring_gather(hidden, down_begun)
    expert_out = down_lot(pieces, firsts[0], tp_count, place, exp_down[0], before=sums[0])
    shared_late, _ = lax.optimization_barrier((shared_hidden, sums[0][:1]))
    shared_all = jnp.broadcast_to(shared_late, (tp_count, *shared_late.shape))
    shared_all = lax.all_to_all(shared_all, "tp", split_axis=0, concat_axis=0, tiled=True)
    returned = lax.all_to_all(
        expert_out.reshape(sp_count, slot_count // sp_count, col_width),
        "sp",
        split_axis=0,
        concat_axis=0,
        tiled=True,
    ).reshape(slot_count, col_width)
    return combine(returned, table, middle, shared_all, sh_down)


def solution(mesh):
    in_specs = (
        P("sp", None),
        P("sp", "tp"),
        P("sp", "tp"),
        P(None, "tp"),
        P("tp"),
        P("tp"),
        P("tp"),
        P("tp", None),
        P(),
        P("sp", None),
        P("sp", None),
        P("sp", None, "tp"),
        P("sp", None, "tp"),
        P("sp", None, "tp"),
        P(None, "tp"),
        P(None, "tp"),
        P(None, "tp"),
    )
    out_specs = P("sp", "tp")
    return jax.shard_map(body, mesh=mesh, in_specs=in_specs, out_specs=out_specs, check_vma=False)
```

```python
import jax
import jax.numpy as jnp
from jax import lax
from jax.experimental import pallas as pl
from jax.experimental.pallas import tpu as pltpu
from jax.sharding import PartitionSpec as P

LN_EPS = 1e-05
RMS_EPS = 1e-06
LANES = 128
F32 = jnp.float32
BF16 = jnp.bfloat16


def silu(v):
    return v / (1.0 + jnp.exp(-v))


def pack_kernel(before, a_val, a_gate, taps, bias, gain, shift, w_out, out, win, params):
    peers, _, lanes = out.shape
    halo, half = before.shape
    rows = win.shape[0]
    win[...] = jnp.zeros(win.shape, F32)
    params[...] = jnp.zeros(params.shape, F32)
    gate = 1.0 / (1.0 + jnp.exp(-a_gate[...].astype(F32)))
    win[0:halo, :] = before[...].astype(F32)
    win[halo : halo + a_val.shape[0], :] = a_val[...].astype(F32) * gate
    span = taps.shape[0]
    params[0:span, :] = taps[...].astype(F32)
    for n, vector in enumerate((bias, gain, shift)):
        rest = vector[...]
        for part in range(3):
            kept = rest.astype(BF16).astype(F32)
            at = span + 3 * n + part
            params[at : at + 1, :] = kept
            rest = rest - kept

    def folded(v):
        n = v.shape[0] // 2
        return jnp.concatenate([v[0:n, :], v[n : 2 * n, :]], axis=1).astype(BF16)

    head, tail = folded(win[...]), folded(params[...])
    top = rows // 2
    low = top + tail.shape[0]
    for t in range(peers):
        out[t, 0:top, :] = head
        out[t, top:low, :] = tail
        out[t, low : low + w_out.shape[0], :] = w_out[:, t * lanes : (t + 1) * lanes]


PARAM_ROWS = 64
FOLDED = 16
ASIDE = (96, 112)


def window_rows(span, tok_rows):
    return -(-(span - 1 + tok_rows) // 32) * 32


def pack(before, a_val, a_gate, taps, bias, gain, shift, w_out, peers):
    rows = window_rows(taps.shape[0], a_val.shape[0])
    lanes = w_out.shape[1] // peers
    total = rows // 2 + PARAM_ROWS // 2 + w_out.shape[0]
    return pl.pallas_call(
        pack_kernel,
        out_shape=jax.ShapeDtypeStruct((peers, total, lanes), BF16),
        scratch_shapes=[
            pltpu.VMEM((rows, a_val.shape[1]), F32),
            pltpu.VMEM((PARAM_ROWS, a_val.shape[1]), F32),
        ],
        name="pack",
    )(before, a_val, a_gate, taps, bias, gain, shift, w_out)


def routing_kernel(capacity, routes, slots_out, pick_out):
    tok_rows, top_count = routes.shape
    slot_count = pick_out.shape[0]
    experts = slot_count // capacity
    ids = lax.broadcasted_iota(jnp.int32, (tok_rows, experts), 1)
    hits = [ids == routes[:, k : k + 1] for k in range(top_count)]
    named = sum(jnp.where(h, 1.0, 0.0) for h in hits).astype(BF16)
    square = (tok_rows, tok_rows)
    below = lax.broadcasted_iota(jnp.int32, square, 0) > lax.broadcasted_iota(jnp.int32, square, 1)
    earlier = jnp.dot(jnp.where(below, 1.0, 0.0).astype(BF16), named, preferred_element_type=F32)
    wide = lax.broadcasted_iota(jnp.int32, (tok_rows, slot_count), 1)
    lane = lax.broadcasted_iota(jnp.int32, slots_out.shape, 1)
    slots = jnp.zeros(slots_out.shape, jnp.int32)
    pick = jnp.zeros(wide.shape, F32)
    for k in range(top_count):
        place = jnp.sum(jnp.where(hits[k], earlier, 0.0), axis=1, keepdims=True).astype(jnp.int32)
        slot = routes[:, k : k + 1] * capacity + place
        slots = jnp.where(lane == k, slot, slots)
        pick = jnp.where(wide == slot, 1.0, pick)
    slots_out[...] = slots
    for at in range(0, slot_count, tok_rows):
        pick_out[at : at + tok_rows, :] = pick[:, at : at + tok_rows].T.astype(BF16)


def routing(routes, capacity, slot_count):
    tok_rows, top_count = routes.shape

    def kernel(*refs):
        routing_kernel(capacity, *refs)

    return pl.pallas_call(
        kernel,
        out_shape=(
            jax.ShapeDtypeStruct((tok_rows, top_count), jnp.int32),
            jax.ShapeDtypeStruct((slot_count, tok_rows), BF16),
        ),
        name="routing",
    )(routes)


def table_kernel(slots, weights, out):
    shape = out.shape[1:]
    ids = lax.broadcasted_iota(jnp.int32, shape, 1)
    table = jnp.zeros(shape, F32)
    for k in range(slots.shape[1]):
        table = jnp.where(ids == slots[:, k : k + 1], weights[:, k : k + 1], table)
    for n in range(out.shape[0]):
        part = table.astype(BF16)
        out[n] = part
        table = table - part.astype(F32)


def weight_table(slots, weights, slot_count):
    return pl.pallas_call(
        table_kernel,
        out_shape=jax.ShapeDtypeStruct((3, slots.shape[0], slot_count), BF16),
        name="table",
    )(slots, weights)


def front_kernel(span, packed, resid, pick, middle_out, send_out, win, params, conv):
    peers = packed.shape[0]
    tok_rows = resid.shape[0]
    half = LANES // 2
    channels = peers * half
    top = win.shape[0] // 2
    fold = PARAM_ROWS // 2
    for pair in range(peers // 2):
        at = slice(pair * LANES, (pair + 1) * LANES)
        one, two = packed[2 * pair, 0 : top + fold, :], packed[2 * pair + 1, 0 : top + fold, :]
        left = jnp.concatenate([one[:, :half], two[:, :half]], axis=1).astype(F32)
        right = jnp.concatenate([one[:, half:], two[:, half:]], axis=1).astype(F32)
        win[0:top, at], win[top : 2 * top, at] = left[0:top], right[0:top]
        params[0:fold, at], params[fold : 2 * fold, at] = left[top:], right[top:]

    def vector(first, cols=slice(None)):
        return sum(params[first + i : first + i + 1, cols] for i in range(3))

    conv_rows = 64

    def one_block(i, _):
        cols = pl.ds(pl.multiple_of(i * LANES, LANES), LANES)
        taps = params[0:span, cols]
        b = vector(span, cols)
        for r in range(0, tok_rows, conv_rows):
            acc = jnp.broadcast_to(b, (conv_rows, LANES))
            for j in range(span):
                acc = acc + taps[j : j + 1, :] * win[r + j : r + j + conv_rows, cols]
            conv[r : r + conv_rows, cols] = acc
        return 0

    lax.fori_loop(0, channels // LANES, one_block, 0)
    gain = vector(span + 3)
    shift = vector(span + 6)
    wcol = packed[:, top + fold :, :].reshape(channels, packed.shape[2])
    for r in range(0, tok_rows, 64):
        c = conv[r : r + 64, :]
        mean = jnp.sum(c, axis=1, keepdims=True) * (1.0 / channels)
        var = jnp.sum(c * c, axis=1, keepdims=True) * (1.0 / channels) - mean * mean
        scaled = (c - mean) * lax.rsqrt(var + LN_EPS) * gain + shift
        mixed = silu(scaled).astype(BF16)
        proj = jnp.dot(mixed, wcol, preferred_element_type=F32)
        middle_out[r : r + 64, :] = (resid[r : r + 64, :].astype(F32) + proj).astype(BF16)
    middle = middle_out[...]
    send_out[...] = jnp.dot(pick[...], middle, preferred_element_type=F32).astype(BF16)


def front(span, packed, resid, pick):
    tok_rows, cols = resid.shape
    channels = packed.shape[0] * LANES // 2

    def kernel(*refs):
        front_kernel(span, *refs)

    return pl.pallas_call(
        kernel,
        out_shape=(
            jax.ShapeDtypeStruct((tok_rows, cols), BF16),
            jax.ShapeDtypeStruct((pick.shape[0], cols), BF16),
        ),
        scratch_shapes=[
            pltpu.VMEM((window_rows(span, tok_rows), channels), F32),
            pltpu.VMEM((PARAM_ROWS, channels), F32),
            pltpu.VMEM((tok_rows, channels), F32),
        ],
        name="front",
    )(packed, resid, pick)


def normed_rows(pieces, width, gain):
    squares = jnp.zeros(pieces[0].shape, F32)
    for x in pieces:
        squares = squares + x.astype(F32) * x.astype(F32)
    mean = jnp.sum(squares, axis=1, keepdims=True) / width
    inverse = lax.rsqrt(mean + RMS_EPS)
    cols = [gain[:, n * LANES : (n + 1) * LANES] for n in range(len(pieces))]
    scaled = [(x.astype(F32) * inverse * c).astype(BF16) for x, c in zip(pieces, cols)]
    return jnp.concatenate(scaled, axis=1)


def gated_units(rows, w_gate, w_up):
    g = jnp.dot(rows, w_gate, preferred_element_type=F32)
    u = jnp.dot(rows, w_up, preferred_element_type=F32)
    return (silu(g) * u).astype(BF16)


def hidden_kernel(rows_in, gain, wg, wu, aside_out, out):
    step = pl.program_id(0)
    block = rows_in.shape[1]
    aside = aside_out.shape[0]
    rows = normed_rows([rows_in[t] for t in range(rows_in.shape[0])], wg.shape[0], gain)
    units = gated_units(rows, wg[...], wu[...])

    @pl.when(step == 0)
    def _():
        aside_out[...] = units[0:aside, :]
        out[0 : block - aside, :] = units[aside:, :]

    @pl.when(step > 0)
    def _():
        out[pl.ds(pl.multiple_of(step * block - aside, 16), block), :] = units


def hidden_units(rows_in, gain, wg, wu, blocks, aside):
    pieces, rows, lanes = rows_in.shape
    width, units = wg.shape
    block = rows // blocks
    return pl.pallas_call(
        hidden_kernel,
        grid=(blocks,),
        in_specs=[
            pl.BlockSpec((pieces, block, lanes), lambda i: (0, i, 0)),
            pl.BlockSpec((1, width), lambda i: (0, 0)),
            pl.BlockSpec((width, units), lambda i: (0, 0)),
            pl.BlockSpec((width, units), lambda i: (0, 0)),
        ],
        out_specs=[
            pl.BlockSpec((aside, units), lambda i: (0, 0)),
            pl.BlockSpec((rows - aside, units), lambda i: (0, 0)),
        ],
        out_shape=(
            jax.ShapeDtypeStruct((aside, units), BF16),
            jax.ShapeDtypeStruct((rows - aside, units), BF16),
        ),
        name="hidden",
    )(rows_in, gain, wg, wu)


def side_hidden_kernel(one, gain, wg, wu, sg, su, out):
    width, units = wg.shape
    few = sg.shape[1]
    slots = out.shape[0] - FOLDED
    rows = normed_rows([one[t] for t in range(one.shape[0])], width, gain)
    out[0:slots, :] = gated_units(rows[0:slots, :], wg[...], wu[...])
    shared = gated_units(rows[slots:, :], sg[...], su[...])
    parts = [shared[j * FOLDED : (j + 1) * FOLDED, :].astype(F32) for j in range(units // few)]
    out[slots:, :] = jnp.concatenate(parts, axis=1).astype(BF16)


def side_hidden(one, gain, wg, wu, sg, su, tok_rows):
    slots = one.shape[1] - tok_rows
    return pl.pallas_call(
        side_hidden_kernel,
        out_shape=jax.ShapeDtypeStruct((slots + FOLDED, wg.shape[1]), BF16),
        name="side_hidden",
    )(one, gain, wg, wu, sg, su)


def side_down_kernel(one, two, wd, sh_down, out, shared_out):
    peers, rows, units = one.shape
    slots = rows - FOLDED
    few = sh_down.shape[0] // peers
    folds = units // few
    whole = jnp.concatenate([one[t, 0:slots, :] for t in range(peers)], axis=1)
    out[0:slots, :] = jnp.dot(whole, wd[...], preferred_element_type=F32).astype(BF16)
    whole = jnp.concatenate([two[t] for t in range(peers)], axis=1)
    out[slots:, :] = jnp.dot(whole, wd[...], preferred_element_type=F32).astype(BF16)
    shape = (folds * FOLDED, units)
    own = lax.broadcasted_iota(jnp.int32, shape, 0) // FOLDED == lax.broadcasted_iota(jnp.int32, shape, 1) // few
    shared = jnp.zeros(shared_out.shape, F32)
    for t in range(peers):
        packed = one[t, slots:, :].astype(F32)
        spread = jnp.where(own, jnp.concatenate([packed] * folds, axis=0), 0.0).astype(BF16)
        weights = jnp.concatenate([sh_down[t * few : (t + 1) * few, :]] * folds, axis=0)
        shared = shared + jnp.dot(spread, weights, preferred_element_type=F32)
    shared_out[...] = shared


def side_down(one, two, wd, sh_down, tok_rows):
    slots = one.shape[1] - FOLDED + two.shape[1]
    return pl.pallas_call(
        side_down_kernel,
        out_shape=(
            jax.ShapeDtypeStruct((slots, wd.shape[1]), BF16),
            jax.ShapeDtypeStruct((tok_rows, wd.shape[1]), F32),
        ),
        name="side_down",
    )(one, two, wd, sh_down)


def down_kernel(hidden, wd, out):
    whole = jnp.concatenate([hidden[t] for t in range(hidden.shape[0])], axis=1)
    out[...] = jnp.dot(whole, wd[...], preferred_element_type=F32).astype(BF16)


def down(hidden, wd, blocks):
    pieces, rows, units = hidden.shape
    block = rows // blocks
    return pl.pallas_call(
        down_kernel,
        grid=(blocks,),
        in_specs=[
            pl.BlockSpec((pieces, block, units), lambda i: (0, i, 0)),
            pl.BlockSpec(wd.shape, lambda i: (0, 0)),
        ],
        out_specs=pl.BlockSpec((block, wd.shape[1]), lambda i: (i, 0)),
        out_shape=jax.ShapeDtypeStruct((rows, wd.shape[1]), BF16),
        name="down",
    )(hidden, wd)


def combine_kernel(returned, table, middle, shared, out):
    total = middle[...].astype(F32) + shared[...]
    rows = returned[...]
    for n in range(table.shape[0]):
        total = total + jnp.dot(table[n], rows, preferred_element_type=F32)
    out[...] = total.astype(BF16)


def combine(returned, table, middle, shared):
    return pl.pallas_call(
        combine_kernel,
        out_shape=jax.ShapeDtypeStruct(middle.shape, BF16),
        name="combine",
    )(returned, table, middle, shared)


def body(
    resid,
    a_val,
    a_gate,
    conv_kernel,
    conv_bias,
    ln_gain,
    ln_bias,
    w_out,
    ffn_gain,
    routes,
    route_weights,
    exp_gate,
    exp_up,
    exp_down,
    sh_gate,
    sh_up,
    sh_down,
):
    tp_count = lax.axis_size("tp")
    tp_place = lax.axis_index("tp")
    sp_count = lax.axis_size("sp")
    tok_rows, model_width = resid.shape
    col_width = model_width // tp_count
    span = conv_kernel.shape[0]
    top_count = routes.shape[1]
    experts_all = exp_gate.shape[0] * sp_count
    capacity = max(2 * tok_rows * top_count // experts_all, tp_count)
    slot_count = experts_all * capacity

    halo = span - 1
    late_val, late_gate = a_val[tok_rows - halo :].astype(F32), a_gate[tok_rows - halo :].astype(F32)
    pairs = [(i, i + 1) for i in range(sp_count - 1)]
    before = lax.ppermute((late_val * jax.nn.sigmoid(late_gate)).astype(BF16), "sp", pairs)

    vectors = [v[None, :] for v in (conv_bias, ln_gain, ln_bias)]
    packed = pack(before, a_val, a_gate, conv_kernel, *vectors, w_out, tp_count)
    spread = lax.all_to_all(packed, "tp", split_axis=0, concat_axis=0, tiled=True)

    routes_late, _ = lax.optimization_barrier((routes, packed[0, :1]))
    slots, pick = routing(routes_late, capacity, slot_count)

    resid_cols = lax.dynamic_slice_in_dim(resid, tp_place * col_width, col_width, 1)
    middle, send = front(span, spread, resid_cols, pick)

    landed = lax.all_to_all(
        send.reshape(sp_count, slot_count // sp_count, col_width),
        "sp",
        split_axis=0,
        concat_axis=0,
        tiled=True,
    ).reshape(slot_count, col_width)
    slots_late, weights_late, _ = lax.optimization_barrier((slots, route_weights, middle[:1]))
    table = weight_table(slots_late, weights_late, slot_count)
    landed, table = lax.optimization_barrier((landed, table))
    first = ASIDE[0]
    gain = ffn_gain[None, :]
    experts = (gain, exp_gate[0], exp_up[0])
    arrived = lax.all_gather(landed[first:], "tp")
    one = lax.all_gather(jnp.concatenate([landed[:first], middle], axis=0), "tp")
    one = side_hidden(one, *experts, sh_gate, sh_up, tok_rows)
    arrived, one = lax.optimization_barrier((arrived, one))
    two, hidden = hidden_units(arrived, *experts, 2, ASIDE[1])

    hidden_all = lax.all_gather(hidden, "tp")
    one, two = lax.optimization_barrier((one, two))
    side_out, shared = side_down(
        lax.all_gather(one, "tp"), lax.all_gather(two, "tp"), exp_down[0], sh_down, tok_rows
    )
    hidden_all, side_out = lax.optimization_barrier((hidden_all, side_out))
    expert_out = jnp.concatenate([side_out, down(hidden_all, exp_down[0], 3)], axis=0)
    returned = lax.all_to_all(
        expert_out.reshape(sp_count, slot_count // sp_count, col_width),
        "sp",
        split_axis=0,
        concat_axis=0,
        tiled=True,
    ).reshape(slot_count, col_width)
    return combine(returned, table, middle, shared)


def solution(mesh):
    in_specs = (
        P("sp", None),
        P("sp", "tp"),
        P("sp", "tp"),
        P(None, "tp"),
        P("tp"),
        P("tp"),
        P("tp"),
        P("tp", None),
        P(),
        P("sp", None),
        P("sp", None),
        P("sp", None, "tp"),
        P("sp", None, "tp"),
        P("sp", None, "tp"),
        P(None, "tp"),
        P(None, "tp"),
        P(None, "tp"),
    )
    out_specs = P("sp", "tp")
    return jax.shard_map(body, mesh=mesh, in_specs=in_specs, out_specs=out_specs, check_vma=False)
```

```python
import jax
import jax.numpy as jnp
from jax import lax
from jax.experimental import pallas as pl
from jax.experimental.pallas import tpu as pltpu
from jax.sharding import PartitionSpec as P

LN_EPS = 1e-05
RMS_EPS = 1e-06
LANES = 128
F32 = jnp.float32
BF16 = jnp.bfloat16


def near(v):
    return pltpu.with_memory_space_constraint(v, pltpu.VMEM)


def silu(v):
    return v / (1.0 + jnp.exp(-v))


def pack_kernel(before, a_val, a_gate, taps, bias, gain, shift, w_out, out, win, params, wide):
    peers, _, lanes = out.shape
    half, halo = before.shape
    tok_rows = a_val.shape[1]
    rows = win.shape[0]
    win[...] = jnp.zeros(win.shape, F32)
    params[...] = jnp.zeros(params.shape, F32)
    gate = 1.0 / (1.0 + jnp.exp(-a_gate[...].astype(F32)))
    wide[...] = jnp.zeros(wide.shape, F32)
    wide[:, 0:halo] = before[...].astype(F32)
    win[0:halo, :] = wide[...].T[0:halo, :]
    win[halo : halo + tok_rows, :] = (a_val[...].astype(F32) * gate).T
    span = taps.shape[0]
    params[0:span, :] = taps[...].astype(F32)
    for n, vector in enumerate((bias, gain, shift)):
        rest = vector[...]
        for part in range(3):
            kept = rest.astype(BF16).astype(F32)
            at = span + 3 * n + part
            params[at : at + 1, :] = kept
            rest = rest - kept

    def folded(v):
        n = v.shape[0] // 2
        return jnp.concatenate([v[0:n, :], v[n : 2 * n, :]], axis=1).astype(BF16)

    head, tail = folded(win[...]), folded(params[...])
    top = rows // 2
    low = top + tail.shape[0]
    for t in range(peers):
        out[t, 0:top, :] = head
        out[t, top:low, :] = tail
        out[t, low : low + w_out.shape[0], :] = w_out[:, t * lanes : (t + 1) * lanes]


PARAM_ROWS = 64
FOLDED = 16
ASIDE = (96, 112)


def window_rows(span, tok_rows):
    return -(-(span - 1 + tok_rows) // 32) * 32


def pack(before, a_val, a_gate, taps, bias, gain, shift, w_out, peers):
    half, tok_rows = a_val.shape
    rows = window_rows(taps.shape[0], tok_rows)
    lanes = w_out.shape[1] // peers
    total = rows // 2 + PARAM_ROWS // 2 + w_out.shape[0]
    return pl.pallas_call(
        pack_kernel,
        out_shape=jax.ShapeDtypeStruct((peers, total, lanes), BF16),
        scratch_shapes=[
            pltpu.VMEM((rows, half), F32),
            pltpu.VMEM((PARAM_ROWS, half), F32),
            pltpu.VMEM((half, LANES), F32),
        ],
        name="pack",
    )(near(before), a_val, a_gate, taps, bias, gain, shift, near(w_out))


def routing_kernel(capacity, routes, slots_out, pick_out):
    tok_rows, top_count = routes.shape
    slot_count = pick_out.shape[0]
    experts = slot_count // capacity
    ids = lax.broadcasted_iota(jnp.int32, (tok_rows, experts), 1)
    hits = [ids == routes[:, k : k + 1] for k in range(top_count)]
    named = sum(jnp.where(h, 1.0, 0.0) for h in hits).astype(BF16)
    square = (tok_rows, tok_rows)
    below = lax.broadcasted_iota(jnp.int32, square, 0) > lax.broadcasted_iota(jnp.int32, square, 1)
    earlier = jnp.dot(jnp.where(below, 1.0, 0.0).astype(BF16), named, preferred_element_type=F32)
    wide = lax.broadcasted_iota(jnp.int32, (tok_rows, slot_count), 1)
    lane = lax.broadcasted_iota(jnp.int32, slots_out.shape, 1)
    slots = jnp.zeros(slots_out.shape, jnp.int32)
    pick = jnp.zeros(wide.shape, F32)
    for k in range(top_count):
        place = jnp.sum(jnp.where(hits[k], earlier, 0.0), axis=1, keepdims=True).astype(jnp.int32)
        slot = routes[:, k : k + 1] * capacity + place
        slots = jnp.where(lane == k, slot, slots)
        pick = jnp.where(wide == slot, 1.0, pick)
    slots_out[...] = slots
    for at in range(0, slot_count, tok_rows):
        pick_out[at : at + tok_rows, :] = pick[:, at : at + tok_rows].T.astype(BF16)


def routing(routes, capacity, slot_count):
    tok_rows, top_count = routes.shape

    def kernel(*refs):
        routing_kernel(capacity, *refs)

    return pl.pallas_call(
        kernel,
        out_shape=(
            jax.ShapeDtypeStruct((tok_rows, top_count), jnp.int32),
            jax.ShapeDtypeStruct((slot_count, tok_rows), BF16),
        ),
        name="routing",
    )(routes)


def table_kernel(slots, weights, out):
    shape = out.shape[1:]
    ids = lax.broadcasted_iota(jnp.int32, shape, 1)
    table = jnp.zeros(shape, F32)
    for k in range(slots.shape[1]):
        table = jnp.where(ids == slots[:, k : k + 1], weights[:, k : k + 1], table)
    for n in range(out.shape[0]):
        part = table.astype(BF16)
        out[n] = part
        table = table - part.astype(F32)


def weight_table(slots, weights, slot_count):
    return pl.pallas_call(
        table_kernel,
        out_shape=jax.ShapeDtypeStruct((3, slots.shape[0], slot_count), BF16),
        name="table",
    )(slots, weights)


def front_kernel(span, packed, resid, pick, middle_out, send_out, win, params, conv):
    peers = packed.shape[0]
    tok_rows = resid.shape[0]
    half = LANES // 2
    channels = peers * half
    top = win.shape[0] // 2
    fold = PARAM_ROWS // 2
    for pair in range(peers // 2):
        at = slice(pair * LANES, (pair + 1) * LANES)
        one, two = packed[2 * pair, 0 : top + fold, :], packed[2 * pair + 1, 0 : top + fold, :]
        left = jnp.concatenate([one[:, :half], two[:, :half]], axis=1).astype(F32)
        right = jnp.concatenate([one[:, half:], two[:, half:]], axis=1).astype(F32)
        win[0:top, at], win[top : 2 * top, at] = left[0:top], right[0:top]
        params[0:fold, at], params[fold : 2 * fold, at] = left[top:], right[top:]

    def vector(first, cols=slice(None)):
        return sum(params[first + i : first + i + 1, cols] for i in range(3))

    conv_rows = 64

    def one_block(i, _):
        cols = pl.ds(pl.multiple_of(i * LANES, LANES), LANES)
        taps = params[0:span, cols]
        b = vector(span, cols)
        for r in range(0, tok_rows, conv_rows):
            acc = jnp.broadcast_to(b, (conv_rows, LANES))
            for j in range(span):
                acc = acc + taps[j : j + 1, :] * win[r + j : r + j + conv_rows, cols]
            conv[r : r + conv_rows, cols] = acc
        return 0

    lax.fori_loop(0, channels // LANES, one_block, 0)
    gain = vector(span + 3)
    shift = vector(span + 6)
    wcol = packed[:, top + fold :, :].reshape(channels, packed.shape[2])
    for r in range(0, tok_rows, 64):
        c = conv[r : r + 64, :]
        mean = jnp.sum(c, axis=1, keepdims=True) * (1.0 / channels)
        var = jnp.sum(c * c, axis=1, keepdims=True) * (1.0 / channels) - mean * mean
        scaled = (c - mean) * lax.rsqrt(var + LN_EPS) * gain + shift
        mixed = silu(scaled).astype(BF16)
        proj = jnp.dot(mixed, wcol, preferred_element_type=F32)
        middle_out[r : r + 64, :] = (resid[r : r + 64, :].astype(F32) + proj).astype(BF16)
    middle = middle_out[...]
    send_out[...] = jnp.dot(pick[...], middle, preferred_element_type=F32).astype(BF16)


def front(span, packed, resid, pick):
    tok_rows, cols = resid.shape
    channels = packed.shape[0] * LANES // 2

    def kernel(*refs):
        front_kernel(span, *refs)

    return pl.pallas_call(
        kernel,
        out_shape=(
            jax.ShapeDtypeStruct((tok_rows, cols), BF16),
            jax.ShapeDtypeStruct((pick.shape[0], cols), BF16),
        ),
        scratch_shapes=[
            pltpu.VMEM((window_rows(span, tok_rows), channels), F32),
            pltpu.VMEM((PARAM_ROWS, channels), F32),
            pltpu.VMEM((tok_rows, channels), F32),
        ],
        name="front",
    )(near(packed), resid, near(pick))


def normed_rows(pieces, width, gain):
    squares = jnp.zeros(pieces[0].shape, F32)
    for x in pieces:
        squares = squares + x.astype(F32) * x.astype(F32)
    mean = jnp.sum(squares, axis=1, keepdims=True) / width
    inverse = lax.rsqrt(mean + RMS_EPS)
    cols = [gain[:, n * LANES : (n + 1) * LANES] for n in range(len(pieces))]
    scaled = [(x.astype(F32) * inverse * c).astype(BF16) for x, c in zip(pieces, cols)]
    return jnp.concatenate(scaled, axis=1)


def gated_units(rows, w_gate, w_up):
    g = jnp.dot(rows, w_gate, preferred_element_type=F32)
    u = jnp.dot(rows, w_up, preferred_element_type=F32)
    return (silu(g) * u).astype(BF16)


def hidden_kernel(rows_in, gain, wg, wu, aside_out, out):
    step = pl.program_id(0)
    block = rows_in.shape[1]
    aside = aside_out.shape[0]
    rows = normed_rows([rows_in[t] for t in range(rows_in.shape[0])], wg.shape[0], gain)
    units = gated_units(rows, wg[...], wu[...])

    @pl.when(step == 0)
    def _():
        aside_out[...] = units[0:aside, :]
        out[0 : block - aside, :] = units[aside:, :]

    @pl.when(step > 0)
    def _():
        out[pl.ds(pl.multiple_of(step * block - aside, 16), block), :] = units


def hidden_units(rows_in, gain, wg, wu, blocks, aside):
    pieces, rows, lanes = rows_in.shape
    width, units = wg.shape
    block = rows // blocks
    return pl.pallas_call(
        hidden_kernel,
        grid=(blocks,),
        in_specs=[
            pl.BlockSpec((pieces, block, lanes), lambda i: (0, i, 0)),
            pl.BlockSpec((1, width), lambda i: (0, 0)),
            pl.BlockSpec(memory_space=pltpu.VMEM),
            pl.BlockSpec(memory_space=pltpu.VMEM),
        ],
        out_specs=[
            pl.BlockSpec((aside, units), lambda i: (0, 0)),
            pl.BlockSpec((rows - aside, units), lambda i: (0, 0)),
        ],
        out_shape=(
            jax.ShapeDtypeStruct((aside, units), BF16),
            jax.ShapeDtypeStruct((rows - aside, units), BF16),
        ),
        name="hidden",
    )(rows_in, gain, near(wg), near(wu))


def side_hidden_kernel(one, gain, wg, wu, sg, su, out):
    width, units = wg.shape
    few = sg.shape[1]
    slots = out.shape[0] - FOLDED
    rows = normed_rows([one[t] for t in range(one.shape[0])], width, gain)
    out[0:slots, :] = gated_units(rows[0:slots, :], wg[...], wu[...])
    shared = gated_units(rows[slots:, :], sg[...], su[...])
    parts = [shared[j * FOLDED : (j + 1) * FOLDED, :].astype(F32) for j in range(units // few)]
    out[slots:, :] = jnp.concatenate(parts, axis=1).astype(BF16)


def side_hidden(one, gain, wg, wu, sg, su, tok_rows):
    slots = one.shape[1] - tok_rows
    return pl.pallas_call(
        side_hidden_kernel,
        out_shape=jax.ShapeDtypeStruct((slots + FOLDED, wg.shape[1]), BF16),
        name="side_hidden",
    )(one, gain, wg, wu, sg, su)


def side_down_kernel(one, two, wd, sh_down, out, shared_out):
    peers, rows, units = one.shape
    slots = rows - FOLDED
    few = sh_down.shape[0] // peers
    folds = units // few
    whole = jnp.concatenate([one[t, 0:slots, :] for t in range(peers)], axis=1)
    out[0:slots, :] = jnp.dot(whole, wd[...], preferred_element_type=F32).astype(BF16)
    whole = jnp.concatenate([two[t] for t in range(peers)], axis=1)
    out[slots:, :] = jnp.dot(whole, wd[...], preferred_element_type=F32).astype(BF16)
    shape = (folds * FOLDED, units)
    own = lax.broadcasted_iota(jnp.int32, shape, 0) // FOLDED == lax.broadcasted_iota(jnp.int32, shape, 1) // few
    shared = jnp.zeros(shared_out.shape, F32)
    for t in range(peers):
        packed = one[t, slots:, :].astype(F32)
        spread = jnp.where(own, jnp.concatenate([packed] * folds, axis=0), 0.0).astype(BF16)
        weights = jnp.concatenate([sh_down[t * few : (t + 1) * few, :]] * folds, axis=0)
        shared = shared + jnp.dot(spread, weights, preferred_element_type=F32)
    shared_out[...] = shared


def side_down(one, two, wd, sh_down, tok_rows):
    slots = one.shape[1] - FOLDED + two.shape[1]
    return pl.pallas_call(
        side_down_kernel,
        out_shape=(
            jax.ShapeDtypeStruct((slots, wd.shape[1]), BF16),
            jax.ShapeDtypeStruct((tok_rows, wd.shape[1]), F32),
        ),
        name="side_down",
    )(one, two, wd, sh_down)


def down_kernel(hidden, wd, out):
    whole = jnp.concatenate([hidden[t] for t in range(hidden.shape[0])], axis=1)
    out[...] = jnp.dot(whole, wd[...], preferred_element_type=F32).astype(BF16)


def down(hidden, wd, blocks):
    pieces, rows, units = hidden.shape
    block = rows // blocks
    return pl.pallas_call(
        down_kernel,
        grid=(blocks,),
        in_specs=[
            pl.BlockSpec((pieces, block, units), lambda i: (0, i, 0)),
            pl.BlockSpec(memory_space=pltpu.VMEM),
        ],
        out_specs=pl.BlockSpec((block, wd.shape[1]), lambda i: (i, 0)),
        out_shape=jax.ShapeDtypeStruct((rows, wd.shape[1]), BF16),
        name="down",
    )(hidden, near(wd))


def combine_kernel(returned, table, middle, shared, out):
    total = middle[...].astype(F32) + shared[...]
    rows = returned[...]
    for n in range(table.shape[0]):
        total = total + jnp.dot(table[n], rows, preferred_element_type=F32)
    out[...] = total.astype(BF16)


def combine(returned, table, middle, shared):
    return pl.pallas_call(
        combine_kernel,
        out_shape=jax.ShapeDtypeStruct(middle.shape, BF16),
        name="combine",
    )(near(returned), near(table), middle, shared)


def body(
    resid,
    a_val,
    a_gate,
    conv_kernel,
    conv_bias,
    ln_gain,
    ln_bias,
    w_out,
    ffn_gain,
    routes,
    route_weights,
    exp_gate,
    exp_up,
    exp_down,
    sh_gate,
    sh_up,
    sh_down,
):
    tp_count = lax.axis_size("tp")
    tp_place = lax.axis_index("tp")
    sp_count = lax.axis_size("sp")
    tok_rows, model_width = resid.shape
    col_width = model_width // tp_count
    span = conv_kernel.shape[0]
    top_count = routes.shape[1]
    experts_all = exp_gate.shape[0] * sp_count
    capacity = max(2 * tok_rows * top_count // experts_all, tp_count)
    slot_count = experts_all * capacity

    halo = span - 1
    late_val, late_gate = a_val[tok_rows - halo :].astype(F32), a_gate[tok_rows - halo :].astype(F32)
    pairs = [(i, i + 1) for i in range(sp_count - 1)]
    before = lax.ppermute((late_val * jax.nn.sigmoid(late_gate)).astype(BF16), "sp", pairs)

    vectors = [v[None, :] for v in (conv_bias, ln_gain, ln_bias)]
    packed = pack(before.T, a_val.T, a_gate.T, conv_kernel, *vectors, w_out, tp_count)
    spread = lax.all_to_all(packed, "tp", split_axis=0, concat_axis=0, tiled=True)

    routes_late, _ = lax.optimization_barrier((routes, packed[0, :1]))
    slots, pick = routing(routes_late, capacity, slot_count)

    resid_cols = lax.dynamic_slice_in_dim(resid, tp_place * col_width, col_width, 1)
    middle, send = front(span, spread, resid_cols, pick)

    landed = lax.all_to_all(
        send.reshape(sp_count, slot_count // sp_count, col_width),
        "sp",
        split_axis=0,
        concat_axis=0,
        tiled=True,
    ).reshape(slot_count, col_width)
    slots_late, weights_late, _ = lax.optimization_barrier((slots, route_weights, middle[:1]))
    table = weight_table(slots_late, weights_late, slot_count)
    landed, table = lax.optimization_barrier((landed, table))
    first = ASIDE[0]
    gain = ffn_gain[None, :]
    experts = (gain, exp_gate[0], exp_up[0])
    arrived = lax.all_gather(landed[first:], "tp")
    one = lax.all_gather(jnp.concatenate([landed[:first], middle], axis=0), "tp")
    one = side_hidden(one, *experts, sh_gate, sh_up, tok_rows)
    arrived, one = lax.optimization_barrier((arrived, one))
    two, hidden = hidden_units(arrived, *experts, 2, ASIDE[1])

    hidden_all = lax.all_gather(hidden, "tp")
    one, two = lax.optimization_barrier((one, two))
    side_out, shared = side_down(
        lax.all_gather(one, "tp"), lax.all_gather(two, "tp"), exp_down[0], sh_down, tok_rows
    )
    hidden_all, side_out = lax.optimization_barrier((hidden_all, side_out))
    expert_out = jnp.concatenate([side_out, down(hidden_all, exp_down[0], 3)], axis=0)
    returned = lax.all_to_all(
        expert_out.reshape(sp_count, slot_count // sp_count, col_width),
        "sp",
        split_axis=0,
        concat_axis=0,
        tiled=True,
    ).reshape(slot_count, col_width)
    return combine(returned, table, middle, shared)


def solution(mesh):
    in_specs = (
        P("sp", None),
        P("sp", "tp"),
        P("sp", "tp"),
        P(None, "tp"),
        P("tp"),
        P("tp"),
        P("tp"),
        P("tp", None),
        P(),
        P("sp", None),
        P("sp", None),
        P("sp", None, "tp"),
        P("sp", None, "tp"),
        P("sp", None, "tp"),
        P(None, "tp"),
        P(None, "tp"),
        P(None, "tp"),
    )
    out_specs = P("sp", "tp")
    return jax.shard_map(body, mesh=mesh, in_specs=in_specs, out_specs=out_specs, check_vma=False)
```

```python
import jax
import jax.numpy as jnp
from jax import lax
from jax.experimental import pallas as pl
from jax.experimental.pallas import tpu as pltpu
from jax.sharding import PartitionSpec as P

LN_EPS = 1e-05
RMS_EPS = 1e-06
LANES = 128
F32 = jnp.float32
BF16 = jnp.bfloat16


def near(v):
    return pltpu.with_memory_space_constraint(v, pltpu.VMEM)


def silu(v):
    return v / (1.0 + jnp.exp(-v))


def pack_kernel(before, a_val, a_gate, taps, bias, gain, shift, w_out, out, win, params, wide):
    peers, _, lanes = out.shape
    half, halo = before.shape
    tok_rows = a_val.shape[1]
    rows = win.shape[0]
    win[...] = jnp.zeros(win.shape, F32)
    params[...] = jnp.zeros(params.shape, F32)
    gate = 1.0 / (1.0 + jnp.exp(-a_gate[...].astype(F32)))
    wide[...] = jnp.zeros(wide.shape, F32)
    wide[:, 0:halo] = before[...].astype(F32)
    win[0:halo, :] = wide[...].T[0:halo, :]
    win[halo : halo + tok_rows, :] = (a_val[...].astype(F32) * gate).T
    span = taps.shape[0]
    params[0:span, :] = taps[...].astype(F32)
    for n, vector in enumerate((bias, gain, shift)):
        rest = vector[...]
        for part in range(3):
            kept = rest.astype(BF16).astype(F32)
            at = span + 3 * n + part
            params[at : at + 1, :] = kept
            rest = rest - kept

    def folded(v):
        n = v.shape[0] // 2
        return jnp.concatenate([v[0:n, :], v[n : 2 * n, :]], axis=1).astype(BF16)

    head, tail = folded(win[...]), folded(params[...])
    top = rows // 2
    low = top + tail.shape[0]
    for t in range(peers):
        out[t, 0:top, :] = head
        out[t, top:low, :] = tail
        out[t, low : low + w_out.shape[0], :] = w_out[:, t * lanes : (t + 1) * lanes]


PARAM_ROWS = 64
FOLDED = 16
ASIDE = (96, 112)


def window_rows(span, tok_rows):
    return -(-(span - 1 + tok_rows) // 32) * 32


def pack(before, a_val, a_gate, taps, bias, gain, shift, w_out, peers):
    half, tok_rows = a_val.shape
    rows = window_rows(taps.shape[0], tok_rows)
    lanes = w_out.shape[1] // peers
    total = rows // 2 + PARAM_ROWS // 2 + w_out.shape[0]
    return pl.pallas_call(
        pack_kernel,
        out_shape=jax.ShapeDtypeStruct((peers, total, lanes), BF16),
        scratch_shapes=[
            pltpu.VMEM((rows, half), F32),
            pltpu.VMEM((PARAM_ROWS, half), F32),
            pltpu.VMEM((half, LANES), F32),
        ],
        name="pack",
    )(near(before), a_val, a_gate, taps, bias, gain, shift, near(w_out))


def routing_kernel(capacity, routes, slots_out, pick_out):
    tok_rows, top_count = routes.shape
    slot_count = pick_out.shape[0]
    experts = slot_count // capacity
    ids = lax.broadcasted_iota(jnp.int32, (tok_rows, experts), 1)
    hits = [ids == routes[:, k : k + 1] for k in range(top_count)]
    named = sum(jnp.where(h, 1.0, 0.0) for h in hits).astype(BF16)
    square = (tok_rows, tok_rows)
    below = lax.broadcasted_iota(jnp.int32, square, 0) > lax.broadcasted_iota(jnp.int32, square, 1)
    earlier = jnp.dot(jnp.where(below, 1.0, 0.0).astype(BF16), named, preferred_element_type=F32)
    wide = lax.broadcasted_iota(jnp.int32, (tok_rows, slot_count), 1)
    lane = lax.broadcasted_iota(jnp.int32, slots_out.shape, 1)
    slots = jnp.zeros(slots_out.shape, jnp.int32)
    pick = jnp.zeros(wide.shape, F32)
    for k in range(top_count):
        place = jnp.sum(jnp.where(hits[k], earlier, 0.0), axis=1, keepdims=True).astype(jnp.int32)
        slot = routes[:, k : k + 1] * capacity + place
        slots = jnp.where(lane == k, slot, slots)
        pick = jnp.where(wide == slot, 1.0, pick)
    slots_out[...] = slots
    for at in range(0, slot_count, tok_rows):
        pick_out[at : at + tok_rows, :] = pick[:, at : at + tok_rows].T.astype(BF16)


def routing(routes, capacity, slot_count):
    tok_rows, top_count = routes.shape

    def kernel(*refs):
        routing_kernel(capacity, *refs)

    return pl.pallas_call(
        kernel,
        out_shape=(
            jax.ShapeDtypeStruct((tok_rows, top_count), jnp.int32),
            jax.ShapeDtypeStruct((slot_count, tok_rows), BF16),
        ),
        name="routing",
    )(routes)


def table_kernel(slots, weights, out):
    shape = out.shape[1:]
    ids = lax.broadcasted_iota(jnp.int32, shape, 1)
    table = jnp.zeros(shape, F32)
    for k in range(slots.shape[1]):
        table = jnp.where(ids == slots[:, k : k + 1], weights[:, k : k + 1], table)
    for n in range(out.shape[0]):
        part = table.astype(BF16)
        out[n] = part
        table = table - part.astype(F32)


def weight_table(slots, weights, slot_count):
    return pl.pallas_call(
        table_kernel,
        out_shape=jax.ShapeDtypeStruct((3, slots.shape[0], slot_count), BF16),
        name="table",
    )(slots, weights)


def front_kernel(span, packed, resid, pick, middle_out, send_out, win, params, conv):
    peers = packed.shape[0]
    tok_rows = resid.shape[0]
    half = LANES // 2
    channels = peers * half
    top = win.shape[0] // 2
    fold = PARAM_ROWS // 2
    for pair in range(peers // 2):
        at = slice(pair * LANES, (pair + 1) * LANES)
        one, two = packed[2 * pair, 0 : top + fold, :], packed[2 * pair + 1, 0 : top + fold, :]
        left = jnp.concatenate([one[:, :half], two[:, :half]], axis=1).astype(F32)
        right = jnp.concatenate([one[:, half:], two[:, half:]], axis=1).astype(F32)
        win[0:top, at], win[top : 2 * top, at] = left[0:top], right[0:top]
        params[0:fold, at], params[fold : 2 * fold, at] = left[top:], right[top:]

    def vector(first, cols=slice(None)):
        return sum(params[first + i : first + i + 1, cols] for i in range(3))

    conv_rows = 64

    def one_block(i, _):
        cols = pl.ds(pl.multiple_of(i * LANES, LANES), LANES)
        taps = params[0:span, cols]
        b = vector(span, cols)
        for r in range(0, tok_rows, conv_rows):
            acc = jnp.broadcast_to(b, (conv_rows, LANES))
            for j in range(span):
                acc = acc + taps[j : j + 1, :] * win[r + j : r + j + conv_rows, cols]
            conv[r : r + conv_rows, cols] = acc
        return 0

    lax.fori_loop(0, channels // LANES, one_block, 0)
    gain = vector(span + 3)
    shift = vector(span + 6)
    wcol = packed[:, top + fold :, :].reshape(channels, packed.shape[2])
    for r in range(0, tok_rows, 64):
        c = conv[r : r + 64, :]
        mean = jnp.sum(c, axis=1, keepdims=True) * (1.0 / channels)
        var = jnp.sum(c * c, axis=1, keepdims=True) * (1.0 / channels) - mean * mean
        scaled = (c - mean) * lax.rsqrt(var + LN_EPS) * gain + shift
        mixed = silu(scaled).astype(BF16)
        proj = jnp.dot(mixed, wcol, preferred_element_type=F32)
        middle_out[r : r + 64, :] = (resid[r : r + 64, :].astype(F32) + proj).astype(BF16)
    middle = middle_out[...]
    send_out[...] = jnp.dot(pick[...], middle, preferred_element_type=F32).astype(BF16)


def front(span, packed, resid, pick):
    tok_rows, cols = resid.shape
    channels = packed.shape[0] * LANES // 2

    def kernel(*refs):
        front_kernel(span, *refs)

    return pl.pallas_call(
        kernel,
        out_shape=(
            jax.ShapeDtypeStruct((tok_rows, cols), BF16),
            jax.ShapeDtypeStruct((pick.shape[0], cols), BF16),
        ),
        scratch_shapes=[
            pltpu.VMEM((window_rows(span, tok_rows), channels), F32),
            pltpu.VMEM((PARAM_ROWS, channels), F32),
            pltpu.VMEM((tok_rows, channels), F32),
        ],
        name="front",
    )(near(packed), resid, pick)


def normed_rows(pieces, width, gain):
    squares = jnp.zeros(pieces[0].shape, F32)
    for x in pieces:
        squares = squares + x.astype(F32) * x.astype(F32)
    mean = jnp.sum(squares, axis=1, keepdims=True) / width
    inverse = lax.rsqrt(mean + RMS_EPS)
    cols = [gain[:, n * LANES : (n + 1) * LANES] for n in range(len(pieces))]
    scaled = [(x.astype(F32) * inverse * c).astype(BF16) for x, c in zip(pieces, cols)]
    return jnp.concatenate(scaled, axis=1)


def gated_units(rows, w_gate, w_up):
    g = jnp.dot(rows, w_gate, preferred_element_type=F32)
    u = jnp.dot(rows, w_up, preferred_element_type=F32)
    return (silu(g) * u).astype(BF16)


def hidden_kernel(rows_in, gain, wg, wu, aside_out, out):
    step = pl.program_id(0)
    block = rows_in.shape[1]
    aside = aside_out.shape[0]
    rows = normed_rows([rows_in[t] for t in range(rows_in.shape[0])], wg.shape[0], gain)
    units = gated_units(rows, wg[...], wu[...])

    @pl.when(step == 0)
    def _():
        aside_out[...] = units[0:aside, :]
        out[0 : block - aside, :] = units[aside:, :]

    @pl.when(step > 0)
    def _():
        out[pl.ds(pl.multiple_of(step * block - aside, 16), block), :] = units


def hidden_units(rows_in, gain, wg, wu, blocks, aside):
    pieces, rows, lanes = rows_in.shape
    width, units = wg.shape
    block = rows // blocks
    return pl.pallas_call(
        hidden_kernel,
        grid=(blocks,),
        in_specs=[
            pl.BlockSpec((pieces, block, lanes), lambda i: (0, i, 0)),
            pl.BlockSpec((1, width), lambda i: (0, 0)),
            pl.BlockSpec(memory_space=pltpu.VMEM),
            pl.BlockSpec(memory_space=pltpu.VMEM),
        ],
        out_specs=[
            pl.BlockSpec((aside, units), lambda i: (0, 0)),
            pl.BlockSpec((rows - aside, units), lambda i: (0, 0)),
        ],
        out_shape=(
            jax.ShapeDtypeStruct((aside, units), BF16),
            jax.ShapeDtypeStruct((rows - aside, units), BF16),
        ),
        name="hidden",
    )(rows_in, gain, near(wg), near(wu))


def side_hidden_kernel(one, gain, wg, wu, sg, su, out):
    width, units = wg.shape
    few = sg.shape[1]
    slots = out.shape[0] - FOLDED
    rows = normed_rows([one[t] for t in range(one.shape[0])], width, gain)
    out[0:slots, :] = gated_units(rows[0:slots, :], wg[...], wu[...])
    shared = gated_units(rows[slots:, :], sg[...], su[...])
    parts = [shared[j * FOLDED : (j + 1) * FOLDED, :].astype(F32) for j in range(units // few)]
    out[slots:, :] = jnp.concatenate(parts, axis=1).astype(BF16)


def side_hidden(one, gain, wg, wu, sg, su, tok_rows):
    slots = one.shape[1] - tok_rows
    return pl.pallas_call(
        side_hidden_kernel,
        out_shape=jax.ShapeDtypeStruct((slots + FOLDED, wg.shape[1]), BF16),
        name="side_hidden",
    )(one, gain, wg, wu, sg, su)


def side_down_kernel(one, two, wd, sh_down, out, shared_out):
    peers, rows, units = one.shape
    slots = rows - FOLDED
    few = sh_down.shape[0] // peers
    folds = units // few
    whole = jnp.concatenate([one[t, 0:slots, :] for t in range(peers)], axis=1)
    out[0:slots, :] = jnp.dot(whole, wd[...], preferred_element_type=F32).astype(BF16)
    whole = jnp.concatenate([two[t] for t in range(peers)], axis=1)
    out[slots:, :] = jnp.dot(whole, wd[...], preferred_element_type=F32).astype(BF16)
    shape = (folds * FOLDED, units)
    own = lax.broadcasted_iota(jnp.int32, shape, 0) // FOLDED == lax.broadcasted_iota(jnp.int32, shape, 1) // few
    shared = jnp.zeros(shared_out.shape, F32)
    for t in range(peers):
        packed = one[t, slots:, :].astype(F32)
        spread = jnp.where(own, jnp.concatenate([packed] * folds, axis=0), 0.0).astype(BF16)
        weights = jnp.concatenate([sh_down[t * few : (t + 1) * few, :]] * folds, axis=0)
        shared = shared + jnp.dot(spread, weights, preferred_element_type=F32)
    shared_out[...] = shared


def side_down(one, two, wd, sh_down, tok_rows):
    slots = one.shape[1] - FOLDED + two.shape[1]
    return pl.pallas_call(
        side_down_kernel,
        out_shape=(
            jax.ShapeDtypeStruct((slots, wd.shape[1]), BF16),
            jax.ShapeDtypeStruct((tok_rows, wd.shape[1]), F32),
        ),
        name="side_down",
    )(one, two, wd, sh_down)


def down_kernel(hidden, wd, aside, out, total):
    step = pl.program_id(0)
    pair = jnp.concatenate([hidden[n] for n in range(hidden.shape[0])], axis=1)
    part = jnp.dot(pair, wd[...], preferred_element_type=F32)

    @pl.when(step == 0)
    def _():
        out[0 : aside.shape[0], :] = aside[...]
        total[...] = part

    @pl.when(step > 0)
    def _():
        total[...] = total[...] + part

    @pl.when(step == pl.num_programs(0) - 1)
    def _():
        out[aside.shape[0] :, :] = total[...].astype(BF16)


def down(hidden, wd, aside):
    pieces, rows, units = hidden.shape
    cols = wd.shape[1]
    return pl.pallas_call(
        down_kernel,
        grid=(pieces // 2,),
        in_specs=[
            pl.BlockSpec((2, rows, units), lambda i: (i, 0, 0)),
            pl.BlockSpec((2 * units, cols), lambda i: (i, 0)),
            pl.BlockSpec(aside.shape, lambda i: (0, 0)),
        ],
        out_specs=pl.BlockSpec((aside.shape[0] + rows, cols), lambda i: (0, 0)),
        out_shape=jax.ShapeDtypeStruct((aside.shape[0] + rows, cols), BF16),
        scratch_shapes=[pltpu.VMEM((rows, cols), F32)],
        name="down",
    )(hidden, wd, aside)


def combine_kernel(returned, table, middle, shared, out):
    total = middle[...].astype(F32) + shared[...]
    rows = returned[...]
    for n in range(table.shape[0]):
        total = total + jnp.dot(table[n], rows, preferred_element_type=F32)
    out[...] = total.astype(BF16)


def combine(returned, table, middle, shared):
    return pl.pallas_call(
        combine_kernel,
        out_shape=jax.ShapeDtypeStruct(middle.shape, BF16),
        name="combine",
    )(near(returned), near(table), middle, shared)


def body(
    resid,
    a_val,
    a_gate,
    conv_kernel,
    conv_bias,
    ln_gain,
    ln_bias,
    w_out,
    ffn_gain,
    routes,
    route_weights,
    exp_gate,
    exp_up,
    exp_down,
    sh_gate,
    sh_up,
    sh_down,
):
    tp_count = lax.axis_size("tp")
    tp_place = lax.axis_index("tp")
    sp_count = lax.axis_size("sp")
    tok_rows, model_width = resid.shape
    col_width = model_width // tp_count
    span = conv_kernel.shape[0]
    top_count = routes.shape[1]
    experts_all = exp_gate.shape[0] * sp_count
    capacity = max(2 * tok_rows * top_count // experts_all, tp_count)
    slot_count = experts_all * capacity

    halo = span - 1
    late_val, late_gate = a_val[tok_rows - halo :].astype(F32), a_gate[tok_rows - halo :].astype(F32)
    pairs = [(i, i + 1) for i in range(sp_count - 1)]
    before = lax.ppermute((late_val * jax.nn.sigmoid(late_gate)).astype(BF16), "sp", pairs)

    vectors = [v[None, :] for v in (conv_bias, ln_gain, ln_bias)]
    packed = pack(before.T, a_val.T, a_gate.T, conv_kernel, *vectors, w_out, tp_count)
    spread = lax.all_to_all(packed, "tp", split_axis=0, concat_axis=0, tiled=True)

    routes_late, _ = lax.optimization_barrier((routes, packed[0, :1]))
    slots, pick = routing(routes_late, capacity, slot_count)

    resid_cols = lax.dynamic_slice_in_dim(resid, tp_place * col_width, col_width, 1)
    middle, send = front(span, spread, resid_cols, pick)

    landed = lax.all_to_all(
        send.reshape(sp_count, slot_count // sp_count, col_width),
        "sp",
        split_axis=0,
        concat_axis=0,
        tiled=True,
    ).reshape(slot_count, col_width)
    slots_late, weights_late, _ = lax.optimization_barrier((slots, route_weights, middle[:1]))
    table = weight_table(slots_late, weights_late, slot_count)
    landed, table = lax.optimization_barrier((landed, table))
    first = ASIDE[0]
    gain = ffn_gain[None, :]
    experts = (gain, exp_gate[0], exp_up[0])
    arrived = lax.all_gather(landed[first:], "tp")
    one = lax.all_gather(jnp.concatenate([landed[:first], middle], axis=0), "tp")
    one = side_hidden(one, *experts, sh_gate, sh_up, tok_rows)
    arrived, one = lax.optimization_barrier((arrived, one))
    two, hidden = hidden_units(arrived, *experts, 2, ASIDE[1])

    hidden_all = lax.all_gather(hidden, "tp")
    one, two = lax.optimization_barrier((one, two))
    side_out, shared = side_down(
        lax.all_gather(one, "tp"), lax.all_gather(two, "tp"), exp_down[0], sh_down, tok_rows
    )
    hidden_all, side_out = lax.optimization_barrier((hidden_all, side_out))
    expert_out = down(hidden_all, exp_down[0], side_out)
    returned = lax.all_to_all(
        expert_out.reshape(sp_count, slot_count // sp_count, col_width),
        "sp",
        split_axis=0,
        concat_axis=0,
        tiled=True,
    ).reshape(slot_count, col_width)
    return combine(returned, table, middle, shared)


def solution(mesh):
    in_specs = (
        P("sp", None),
        P("sp", "tp"),
        P("sp", "tp"),
        P(None, "tp"),
        P("tp"),
        P("tp"),
        P("tp"),
        P("tp", None),
        P(),
        P("sp", None),
        P("sp", None),
        P("sp", None, "tp"),
        P("sp", None, "tp"),
        P("sp", None, "tp"),
        P(None, "tp"),
        P(None, "tp"),
        P(None, "tp"),
    )
    out_specs = P("sp", "tp")
    return jax.shard_map(body, mesh=mesh, in_specs=in_specs, out_specs=out_specs, check_vma=False)
```

```python
import jax
import jax.numpy as jnp
from jax import lax
from jax.experimental import pallas as pl
from jax.experimental.pallas import tpu as pltpu
from jax.sharding import PartitionSpec as P

LN_EPS = 1e-05
RMS_EPS = 1e-06
LANES = 128
F32 = jnp.float32
BF16 = jnp.bfloat16


def near(v):
    return pltpu.with_memory_space_constraint(v, pltpu.VMEM)


def silu(v):
    return v / (1.0 + jnp.exp(-v))


def pack_kernel(before, a_val, a_gate, taps, bias, gain, shift, w_out, out, win, params, wide):
    peers, _, lanes = out.shape
    half, halo = before.shape
    tok_rows = a_val.shape[1]
    rows = win.shape[0]
    win[...] = jnp.zeros(win.shape, F32)
    params[...] = jnp.zeros(params.shape, F32)
    gate = 1.0 / (1.0 + jnp.exp(-a_gate[...].astype(F32)))
    wide[...] = jnp.zeros(wide.shape, F32)
    wide[:, 0:halo] = before[...].astype(F32)
    win[0:halo, :] = wide[...].T[0:halo, :]
    win[halo : halo + tok_rows, :] = (a_val[...].astype(F32) * gate).T
    span = taps.shape[0]
    params[0:span, :] = taps[...].astype(F32)
    for n, vector in enumerate((bias, gain, shift)):
        rest = vector[...]
        for part in range(3):
            kept = rest.astype(BF16).astype(F32)
            at = span + 3 * n + part
            params[at : at + 1, :] = kept
            rest = rest - kept

    def folded(v):
        n = v.shape[0] // 2
        return jnp.concatenate([v[0:n, :], v[n : 2 * n, :]], axis=1).astype(BF16)

    head, tail = folded(win[...]), folded(params[...])
    top = rows // 2
    low = top + tail.shape[0]
    for t in range(peers):
        out[t, 0:top, :] = head
        out[t, top:low, :] = tail
        out[t, low : low + w_out.shape[0], :] = w_out[:, t * lanes : (t + 1) * lanes]


PARAM_ROWS = 64
FOLDED = 16
ASIDE = (96, 112)


def window_rows(span, tok_rows):
    return -(-(span - 1 + tok_rows) // 32) * 32


def pack(before, a_val, a_gate, taps, bias, gain, shift, w_out, peers):
    half, tok_rows = a_val.shape
    rows = window_rows(taps.shape[0], tok_rows)
    lanes = w_out.shape[1] // peers
    total = rows // 2 + PARAM_ROWS // 2 + w_out.shape[0]
    return pl.pallas_call(
        pack_kernel,
        out_shape=jax.ShapeDtypeStruct((peers, total, lanes), BF16),
        scratch_shapes=[
            pltpu.VMEM((rows, half), F32),
            pltpu.VMEM((PARAM_ROWS, half), F32),
            pltpu.VMEM((half, LANES), F32),
        ],
        name="pack",
    )(near(before), a_val, a_gate, taps, bias, gain, shift, w_out)


def routing_kernel(capacity, routes, slots_out, pick_out):
    tok_rows, top_count = routes.shape
    slot_count = pick_out.shape[0]
    experts = slot_count // capacity
    ids = lax.broadcasted_iota(jnp.int32, (tok_rows, experts), 1)
    hits = [ids == routes[:, k : k + 1] for k in range(top_count)]
    named = sum(jnp.where(h, 1.0, 0.0) for h in hits).astype(BF16)
    square = (tok_rows, tok_rows)
    below = lax.broadcasted_iota(jnp.int32, square, 0) > lax.broadcasted_iota(jnp.int32, square, 1)
    earlier = jnp.dot(jnp.where(below, 1.0, 0.0).astype(BF16), named, preferred_element_type=F32)
    wide = lax.broadcasted_iota(jnp.int32, (tok_rows, slot_count), 1)
    lane = lax.broadcasted_iota(jnp.int32, slots_out.shape, 1)
    slots = jnp.zeros(slots_out.shape, jnp.int32)
    pick = jnp.zeros(wide.shape, F32)
    for k in range(top_count):
        place = jnp.sum(jnp.where(hits[k], earlier, 0.0), axis=1, keepdims=True).astype(jnp.int32)
        slot = routes[:, k : k + 1] * capacity + place
        slots = jnp.where(lane == k, slot, slots)
        pick = jnp.where(wide == slot, 1.0, pick)
    slots_out[...] = slots
    for at in range(0, slot_count, tok_rows):
        pick_out[at : at + tok_rows, :] = pick[:, at : at + tok_rows].T.astype(BF16)


def routing(routes, capacity, slot_count):
    tok_rows, top_count = routes.shape

    def kernel(*refs):
        routing_kernel(capacity, *refs)

    return pl.pallas_call(
        kernel,
        out_shape=(
            jax.ShapeDtypeStruct((tok_rows, top_count), jnp.int32),
            jax.ShapeDtypeStruct((slot_count, tok_rows), BF16),
        ),
        name="routing",
    )(routes)


def table_kernel(slots, weights, out):
    shape = out.shape[1:]
    ids = lax.broadcasted_iota(jnp.int32, shape, 1)
    table = jnp.zeros(shape, F32)
    for k in range(slots.shape[1]):
        table = jnp.where(ids == slots[:, k : k + 1], weights[:, k : k + 1], table)
    for n in range(out.shape[0]):
        part = table.astype(BF16)
        out[n] = part
        table = table - part.astype(F32)


def weight_table(slots, weights, slot_count):
    return pl.pallas_call(
        table_kernel,
        out_shape=jax.ShapeDtypeStruct((3, slots.shape[0], slot_count), BF16),
        name="table",
    )(slots, weights)


def front_kernel(span, packed, resid, pick, middle_out, send_out, win, params, conv):
    peers = packed.shape[0]
    tok_rows = resid.shape[0]
    half = LANES // 2
    channels = peers * half
    top = win.shape[0] // 2
    fold = PARAM_ROWS // 2
    for pair in range(peers // 2):
        at = slice(pair * LANES, (pair + 1) * LANES)
        one, two = packed[2 * pair, 0 : top + fold, :], packed[2 * pair + 1, 0 : top + fold, :]
        left = jnp.concatenate([one[:, :half], two[:, :half]], axis=1).astype(F32)
        right = jnp.concatenate([one[:, half:], two[:, half:]], axis=1).astype(F32)
        win[0:top, at], win[top : 2 * top, at] = left[0:top], right[0:top]
        params[0:fold, at], params[fold : 2 * fold, at] = left[top:], right[top:]

    def vector(first, cols=slice(None)):
        return sum(params[first + i : first + i + 1, cols] for i in range(3))

    conv_rows = 64

    def one_block(i, _):
        cols = pl.ds(pl.multiple_of(i * LANES, LANES), LANES)
        taps = params[0:span, cols]
        b = vector(span, cols)
        for r in range(0, tok_rows, conv_rows):
            acc = jnp.broadcast_to(b, (conv_rows, LANES))
            for j in range(span):
                acc = acc + taps[j : j + 1, :] * win[r + j : r + j + conv_rows, cols]
            conv[r : r + conv_rows, cols] = acc
        return 0

    lax.fori_loop(0, channels // LANES, one_block, 0)
    gain = vector(span + 3)
    shift = vector(span + 6)
    wcol = packed[:, top + fold :, :].reshape(channels, packed.shape[2])
    for r in range(0, tok_rows, 64):
        c = conv[r : r + 64, :]
        mean = jnp.sum(c, axis=1, keepdims=True) * (1.0 / channels)
        var = jnp.sum(c * c, axis=1, keepdims=True) * (1.0 / channels) - mean * mean
        scaled = (c - mean) * lax.rsqrt(var + LN_EPS) * gain + shift
        mixed = silu(scaled).astype(BF16)
        proj = jnp.dot(mixed, wcol, preferred_element_type=F32)
        middle_out[r : r + 64, :] = (resid[r : r + 64, :].astype(F32) + proj).astype(BF16)
    middle = middle_out[...]
    send_out[...] = jnp.dot(pick[...], middle, preferred_element_type=F32).astype(BF16)


def front(span, packed, resid, pick):
    tok_rows, cols = resid.shape
    channels = packed.shape[0] * LANES // 2

    def kernel(*refs):
        front_kernel(span, *refs)

    return pl.pallas_call(
        kernel,
        out_shape=(
            jax.ShapeDtypeStruct((tok_rows, cols), BF16),
            jax.ShapeDtypeStruct((pick.shape[0], cols), BF16),
        ),
        scratch_shapes=[
            pltpu.VMEM((window_rows(span, tok_rows), channels), F32),
            pltpu.VMEM((PARAM_ROWS, channels), F32),
            pltpu.VMEM((tok_rows, channels), F32),
        ],
        name="front",
    )(near(packed), resid, pick)


def normed_rows(pieces, width, gain):
    squares = jnp.zeros(pieces[0].shape, F32)
    for x in pieces:
        squares = squares + x.astype(F32) * x.astype(F32)
    mean = jnp.sum(squares, axis=1, keepdims=True) / width
    inverse = lax.rsqrt(mean + RMS_EPS)
    cols = [gain[:, n * LANES : (n + 1) * LANES] for n in range(len(pieces))]
    scaled = [(x.astype(F32) * inverse * c).astype(BF16) for x, c in zip(pieces, cols)]
    return jnp.concatenate(scaled, axis=1)


def gated_units(rows, w_gate, w_up):
    g = jnp.dot(rows, w_gate, preferred_element_type=F32)
    u = jnp.dot(rows, w_up, preferred_element_type=F32)
    return (silu(g) * u).astype(BF16)


def hidden_kernel(rows_in, gain, wg, wu, aside_out, out):
    step = pl.program_id(0)
    block = rows_in.shape[1]
    aside = aside_out.shape[0]
    rows = normed_rows([rows_in[t] for t in range(rows_in.shape[0])], wg.shape[0], gain)
    units = gated_units(rows, wg[...], wu[...])

    @pl.when(step == 0)
    def _():
        aside_out[...] = units[0:aside, :]
        out[0 : block - aside, :] = units[aside:, :]

    @pl.when(step > 0)
    def _():
        out[pl.ds(pl.multiple_of(step * block - aside, 16), block), :] = units


def hidden_units(rows_in, gain, wg, wu, blocks, aside):
    pieces, rows, lanes = rows_in.shape
    width, units = wg.shape
    block = rows // blocks
    return pl.pallas_call(
        hidden_kernel,
        grid=(blocks,),
        in_specs=[
            pl.BlockSpec((pieces, block, lanes), lambda i: (0, i, 0)),
            pl.BlockSpec((1, width), lambda i: (0, 0)),
            pl.BlockSpec(memory_space=pltpu.VMEM),
            pl.BlockSpec(memory_space=pltpu.VMEM),
        ],
        out_specs=[
            pl.BlockSpec((aside, units), lambda i: (0, 0)),
            pl.BlockSpec((rows - aside, units), lambda i: (0, 0)),
        ],
        out_shape=(
            jax.ShapeDtypeStruct((aside, units), BF16),
            jax.ShapeDtypeStruct((rows - aside, units), BF16),
        ),
        name="hidden",
    )(rows_in, gain, near(wg), near(wu))


def side_hidden_kernel(one, gain, wg, wu, sg, su, out):
    width, units = wg.shape
    few = sg.shape[1]
    slots = out.shape[0] - FOLDED
    rows = normed_rows([one[t] for t in range(one.shape[0])], width, gain)
    out[0:slots, :] = gated_units(rows[0:slots, :], wg[...], wu[...])
    shared = gated_units(rows[slots:, :], sg[...], su[...])
    parts = [shared[j * FOLDED : (j + 1) * FOLDED, :].astype(F32) for j in range(units // few)]
    out[slots:, :] = jnp.concatenate(parts, axis=1).astype(BF16)


def side_hidden(one, gain, wg, wu, sg, su, tok_rows):
    slots = one.shape[1] - tok_rows
    return pl.pallas_call(
        side_hidden_kernel,
        out_shape=jax.ShapeDtypeStruct((slots + FOLDED, wg.shape[1]), BF16),
        name="side_hidden",
    )(one, gain, wg, wu, sg, su)


def side_down_kernel(one, two, wd, sh_down, out, shared_out):
    peers, rows, units = one.shape
    slots = rows - FOLDED
    few = sh_down.shape[0] // peers
    folds = units // few
    whole = jnp.concatenate([one[t, 0:slots, :] for t in range(peers)], axis=1)
    out[0:slots, :] = jnp.dot(whole, wd[...], preferred_element_type=F32).astype(BF16)
    whole = jnp.concatenate([two[t] for t in range(peers)], axis=1)
    out[slots:, :] = jnp.dot(whole, wd[...], preferred_element_type=F32).astype(BF16)
    shape = (folds * FOLDED, units)
    own = lax.broadcasted_iota(jnp.int32, shape, 0) // FOLDED == lax.broadcasted_iota(jnp.int32, shape, 1) // few
    shared = jnp.zeros(shared_out.shape, F32)
    for t in range(peers):
        packed = one[t, slots:, :].astype(F32)
        spread = jnp.where(own, jnp.concatenate([packed] * folds, axis=0), 0.0).astype(BF16)
        weights = jnp.concatenate([sh_down[t * few : (t + 1) * few, :]] * folds, axis=0)
        shared = shared + jnp.dot(spread, weights, preferred_element_type=F32)
    shared_out[...] = shared


def side_down(one, two, wd, sh_down, tok_rows):
    slots = one.shape[1] - FOLDED + two.shape[1]
    return pl.pallas_call(
        side_down_kernel,
        out_shape=(
            jax.ShapeDtypeStruct((slots, wd.shape[1]), BF16),
            jax.ShapeDtypeStruct((tok_rows, wd.shape[1]), F32),
        ),
        name="side_down",
    )(one, two, wd, sh_down)


def down_kernel(hidden, wd, aside, out):
    slots = aside.shape[0]
    block = hidden.shape[1]
    step = pl.program_id(0)

    @pl.when(step == 0)
    def _():
        out[0:slots, :] = aside[...]

    whole = jnp.concatenate([hidden[t] for t in range(hidden.shape[0])], axis=1)
    at = pl.ds(pl.multiple_of(slots + step * block, 16), block)
    out[at, :] = jnp.dot(whole, wd[...], preferred_element_type=F32).astype(BF16)


def down(hidden, wd, aside, blocks):
    pieces, rows, units = hidden.shape
    block = rows // blocks
    total = (aside.shape[0] + rows, wd.shape[1])
    return pl.pallas_call(
        down_kernel,
        grid=(blocks,),
        in_specs=[
            pl.BlockSpec((pieces, block, units), lambda i: (0, i, 0)),
            pl.BlockSpec(wd.shape, lambda i: (0, 0)),
            pl.BlockSpec(aside.shape, lambda i: (0, 0)),
        ],
        out_specs=pl.BlockSpec(total, lambda i: (0, 0)),
        out_shape=jax.ShapeDtypeStruct(total, BF16),
        name="down",
    )(hidden, wd, aside)


def combine_kernel(returned, table, middle, shared, out):
    total = middle[...].astype(F32) + shared[...]
    rows = returned[...]
    for n in range(table.shape[0]):
        total = total + jnp.dot(table[n], rows, preferred_element_type=F32)
    out[...] = total.astype(BF16)


def combine(returned, table, middle, shared):
    return pl.pallas_call(
        combine_kernel,
        out_shape=jax.ShapeDtypeStruct(middle.shape, BF16),
        name="combine",
    )(near(returned), near(table), middle, shared)


def body(
    resid,
    a_val,
    a_gate,
    conv_kernel,
    conv_bias,
    ln_gain,
    ln_bias,
    w_out,
    ffn_gain,
    routes,
    route_weights,
    exp_gate,
    exp_up,
    exp_down,
    sh_gate,
    sh_up,
    sh_down,
):
    tp_count = lax.axis_size("tp")
    tp_place = lax.axis_index("tp")
    sp_count = lax.axis_size("sp")
    tok_rows, model_width = resid.shape
    col_width = model_width // tp_count
    span = conv_kernel.shape[0]
    top_count = routes.shape[1]
    experts_all = exp_gate.shape[0] * sp_count
    capacity = max(2 * tok_rows * top_count // experts_all, tp_count)
    slot_count = experts_all * capacity

    halo = span - 1
    late_val, late_gate = a_val[tok_rows - halo :].astype(F32), a_gate[tok_rows - halo :].astype(F32)
    pairs = [(i, i + 1) for i in range(sp_count - 1)]
    before = lax.ppermute((late_val * jax.nn.sigmoid(late_gate)).astype(BF16), "sp", pairs)

    vectors = [v[None, :] for v in (conv_bias, ln_gain, ln_bias)]
    packed = pack(before.T, a_val.T, a_gate.T, conv_kernel, *vectors, w_out, tp_count)
    spread = lax.all_to_all(packed, "tp", split_axis=0, concat_axis=0, tiled=True)

    routes_late, _ = lax.optimization_barrier((routes, packed[0, :1]))
    slots, pick = routing(routes_late, capacity, slot_count)

    resid_cols = lax.dynamic_slice_in_dim(resid, tp_place * col_width, col_width, 1)
    middle, send = front(span, spread, resid_cols, pick)

    landed = lax.all_to_all(
        send.reshape(sp_count, slot_count // sp_count, col_width),
        "sp",
        split_axis=0,
        concat_axis=0,
        tiled=True,
    ).reshape(slot_count, col_width)
    slots_late, weights_late, _ = lax.optimization_barrier((slots, route_weights, middle[:1]))
    table = weight_table(slots_late, weights_late, slot_count)
    landed, table = lax.optimization_barrier((landed, table))
    first = ASIDE[0]
    gain = ffn_gain[None, :]
    experts = (gain, exp_gate[0], exp_up[0])
    arrived = lax.all_gather(landed[first:], "tp")
    one = lax.all_gather(jnp.concatenate([landed[:first], middle], axis=0), "tp")
    one = side_hidden(one, *experts, sh_gate, sh_up, tok_rows)
    arrived, one = lax.optimization_barrier((arrived, one))
    two, hidden = hidden_units(arrived, *experts, 2, ASIDE[1])

    hidden_all = lax.all_gather(hidden, "tp")
    one, two = lax.optimization_barrier((one, two))
    side_out, shared = side_down(
        lax.all_gather(one, "tp"), lax.all_gather(two, "tp"), exp_down[0], sh_down, tok_rows
    )
    hidden_all, side_out = lax.optimization_barrier((hidden_all, side_out))
    expert_out = down(hidden_all, exp_down[0], side_out, 3)
    returned = lax.all_to_all(
        expert_out.reshape(sp_count, slot_count // sp_count, col_width),
        "sp",
        split_axis=0,
        concat_axis=0,
        tiled=True,
    ).reshape(slot_count, col_width)
    return combine(returned, table, middle, shared)


def solution(mesh):
    in_specs = (
        P("sp", None),
        P("sp", "tp"),
        P("sp", "tp"),
        P(None, "tp"),
        P("tp"),
        P("tp"),
        P("tp"),
        P("tp", None),
        P(),
        P("sp", None),
        P("sp", None),
        P("sp", None, "tp"),
        P("sp", None, "tp"),
        P("sp", None, "tp"),
        P(None, "tp"),
        P(None, "tp"),
        P(None, "tp"),
    )
    out_specs = P("sp", "tp")
    return jax.shard_map(body, mesh=mesh, in_specs=in_specs, out_specs=out_specs, check_vma=False)
```

```python
import jax
import jax.numpy as jnp
from jax import lax
from jax.experimental import pallas as pl
from jax.experimental.pallas import tpu as pltpu
from jax.sharding import PartitionSpec as P

LN_EPS = 1e-05
RMS_EPS = 1e-06
LANES = 128
F32 = jnp.float32
BF16 = jnp.bfloat16


def near(v):
    return pltpu.with_memory_space_constraint(v, pltpu.VMEM)


def silu(v):
    return v / (1.0 + jnp.exp(-v))


def pack_kernel(before, a_val, a_gate, taps, bias, gain, shift, w_out, out, win, params, wide):
    peers, _, lanes = out.shape
    half, halo = before.shape
    tok_rows = a_val.shape[1]
    rows = win.shape[0]
    win[...] = jnp.zeros(win.shape, F32)
    params[...] = jnp.zeros(params.shape, F32)
    gate = 1.0 / (1.0 + jnp.exp(-a_gate[...].astype(F32)))
    wide[...] = jnp.zeros(wide.shape, F32)
    wide[:, 0:halo] = before[...].astype(F32)
    win[0:halo, :] = wide[...].T[0:halo, :]
    win[halo : halo + tok_rows, :] = (a_val[...].astype(F32) * gate).T
    span = taps.shape[0]
    params[0:span, :] = taps[...].astype(F32)
    for n, vector in enumerate((bias, gain, shift)):
        rest = vector[...]
        for part in range(3):
            kept = rest.astype(BF16).astype(F32)
            at = span + 3 * n + part
            params[at : at + 1, :] = kept
            rest = rest - kept

    def folded(v):
        n = v.shape[0] // 2
        return jnp.concatenate([v[0:n, :], v[n : 2 * n, :]], axis=1).astype(BF16)

    head, tail = folded(win[...]), folded(params[...])
    top = rows // 2
    low = top + tail.shape[0]
    for t in range(peers):
        out[t, 0:top, :] = head
        out[t, top:low, :] = tail
        out[t, low : low + w_out.shape[0], :] = w_out[:, t * lanes : (t + 1) * lanes]


PARAM_ROWS = 64
FOLDED = 16
ASIDE = (96, 112)


def window_rows(span, tok_rows):
    return -(-(span - 1 + tok_rows) // 32) * 32


def pack(before, a_val, a_gate, taps, bias, gain, shift, w_out, peers):
    half, tok_rows = a_val.shape
    rows = window_rows(taps.shape[0], tok_rows)
    lanes = w_out.shape[1] // peers
    total = rows // 2 + PARAM_ROWS // 2 + w_out.shape[0]
    return pl.pallas_call(
        pack_kernel,
        out_shape=jax.ShapeDtypeStruct((peers, total, lanes), BF16),
        scratch_shapes=[
            pltpu.VMEM((rows, half), F32),
            pltpu.VMEM((PARAM_ROWS, half), F32),
            pltpu.VMEM((half, LANES), F32),
        ],
        name="pack",
    )(near(before), a_val, a_gate, taps, bias, gain, shift, w_out)


def routing_kernel(capacity, routes, slots_out, pick_out):
    tok_rows, top_count = routes.shape
    slot_count = pick_out.shape[0]
    experts = slot_count // capacity
    ids = lax.broadcasted_iota(jnp.int32, (tok_rows, experts), 1)
    hits = [ids == routes[:, k : k + 1] for k in range(top_count)]
    named = sum(jnp.where(h, 1.0, 0.0) for h in hits).astype(BF16)
    square = (tok_rows, tok_rows)
    below = lax.broadcasted_iota(jnp.int32, square, 0) > lax.broadcasted_iota(jnp.int32, square, 1)
    earlier = jnp.dot(jnp.where(below, 1.0, 0.0).astype(BF16), named, preferred_element_type=F32)
    wide = lax.broadcasted_iota(jnp.int32, (tok_rows, slot_count), 1)
    lane = lax.broadcasted_iota(jnp.int32, slots_out.shape, 1)
    slots = jnp.zeros(slots_out.shape, jnp.int32)
    pick = jnp.zeros(wide.shape, F32)
    for k in range(top_count):
        place = jnp.sum(jnp.where(hits[k], earlier, 0.0), axis=1, keepdims=True).astype(jnp.int32)
        slot = routes[:, k : k + 1] * capacity + place
        slots = jnp.where(lane == k, slot, slots)
        pick = jnp.where(wide == slot, 1.0, pick)
    slots_out[...] = slots
    for at in range(0, slot_count, tok_rows):
        pick_out[at : at + tok_rows, :] = pick[:, at : at + tok_rows].T.astype(BF16)


def routing(routes, capacity, slot_count):
    tok_rows, top_count = routes.shape

    def kernel(*refs):
        routing_kernel(capacity, *refs)

    return pl.pallas_call(
        kernel,
        out_shape=(
            jax.ShapeDtypeStruct((tok_rows, top_count), jnp.int32),
            jax.ShapeDtypeStruct((slot_count, tok_rows), BF16),
        ),
        name="routing",
    )(routes)


def table_kernel(slots, weights, out):
    shape = out.shape[1:]
    ids = lax.broadcasted_iota(jnp.int32, shape, 1)
    table = jnp.zeros(shape, F32)
    for k in range(slots.shape[1]):
        table = jnp.where(ids == slots[:, k : k + 1], weights[:, k : k + 1], table)
    for n in range(out.shape[0]):
        part = table.astype(BF16)
        out[n] = part
        table = table - part.astype(F32)


def weight_table(slots, weights, slot_count):
    return pl.pallas_call(
        table_kernel,
        out_shape=jax.ShapeDtypeStruct((3, slots.shape[0], slot_count), BF16),
        name="table",
    )(slots, weights)


def front_kernel(span, packed, resid, pick, middle_out, send_out, win, params, conv):
    peers = packed.shape[0]
    tok_rows = resid.shape[0]
    half = LANES // 2
    channels = peers * half
    top = win.shape[1] // 2
    fold = PARAM_ROWS // 2
    for pair in range(peers // 2):
        at = slice(pair * LANES, (pair + 1) * LANES)
        one, two = packed[2 * pair, 0 : top + fold, :], packed[2 * pair + 1, 0 : top + fold, :]
        left = jnp.concatenate([one[:, :half], two[:, :half]], axis=1).astype(F32)
        right = jnp.concatenate([one[:, half:], two[:, half:]], axis=1).astype(F32)
        win[pair, 0:top, :], win[pair, top : 2 * top, :] = left[0:top], right[0:top]
        params[0:fold, at], params[fold : 2 * fold, at] = left[top:], right[top:]

    def vector(first, cols=slice(None)):
        return sum(params[first + i : first + i + 1, cols] for i in range(3))

    conv_rows = 64

    def one_block(i, _):
        cols = pl.ds(pl.multiple_of(i * LANES, LANES), LANES)
        taps = params[0:span, cols]
        b = vector(span, cols)
        for r in range(0, tok_rows, conv_rows):
            acc = jnp.broadcast_to(b, (conv_rows, LANES))
            for j in range(span):
                acc = acc + taps[j : j + 1, :] * win[i, r + j : r + j + conv_rows, :]
            conv[r : r + conv_rows, cols] = acc
        return 0

    lax.fori_loop(0, channels // LANES, one_block, 0)
    gain = vector(span + 3)
    shift = vector(span + 6)
    wcol = packed[:, top + fold :, :].reshape(channels, packed.shape[2])
    for r in range(0, tok_rows, 64):
        c = conv[r : r + 64, :]
        mean = jnp.sum(c, axis=1, keepdims=True) * (1.0 / channels)
        var = jnp.sum(c * c, axis=1, keepdims=True) * (1.0 / channels) - mean * mean
        scaled = (c - mean) * lax.rsqrt(var + LN_EPS) * gain + shift
        mixed = silu(scaled).astype(BF16)
        proj = jnp.dot(mixed, wcol, preferred_element_type=F32)
        middle_out[r : r + 64, :] = (resid[r : r + 64, :].astype(F32) + proj).astype(BF16)
    middle = middle_out[...]
    send_out[...] = jnp.dot(pick[...], middle, preferred_element_type=F32).astype(BF16)


def front(span, packed, resid, pick):
    tok_rows, cols = resid.shape
    channels = packed.shape[0] * LANES // 2

    def kernel(*refs):
        front_kernel(span, *refs)

    return pl.pallas_call(
        kernel,
        out_shape=(
            jax.ShapeDtypeStruct((tok_rows, cols), BF16),
            jax.ShapeDtypeStruct((pick.shape[0], cols), BF16),
        ),
        scratch_shapes=[
            pltpu.VMEM((channels // LANES, window_rows(span, tok_rows), LANES), F32),
            pltpu.VMEM((PARAM_ROWS, channels), F32),
            pltpu.VMEM((tok_rows, channels), F32),
        ],
        name="front",
    )(near(packed), resid, pick)


def normed_rows(pieces, width, gain):
    squares = jnp.zeros(pieces[0].shape, F32)
    for x in pieces:
        squares = squares + x.astype(F32) * x.astype(F32)
    mean = jnp.sum(squares, axis=1, keepdims=True) / width
    inverse = lax.rsqrt(mean + RMS_EPS)
    cols = [gain[:, n * LANES : (n + 1) * LANES] for n in range(len(pieces))]
    scaled = [(x.astype(F32) * inverse * c).astype(BF16) for x, c in zip(pieces, cols)]
    return jnp.concatenate(scaled, axis=1)


def gated_units(rows, w_gate, w_up):
    g = jnp.dot(rows, w_gate, preferred_element_type=F32)
    u = jnp.dot(rows, w_up, preferred_element_type=F32)
    return (silu(g) * u).astype(BF16)


def hidden_kernel(rows_in, gain, wg, wu, aside_out, out):
    step = pl.program_id(0)
    block = rows_in.shape[1]
    aside = aside_out.shape[0]
    rows = normed_rows([rows_in[t] for t in range(rows_in.shape[0])], wg.shape[0], gain)
    units = gated_units(rows, wg[...], wu[...])

    @pl.when(step == 0)
    def _():
        aside_out[...] = units[0:aside, :]
        out[0 : block - aside, :] = units[aside:, :]

    @pl.when(step > 0)
    def _():
        out[pl.ds(pl.multiple_of(step * block - aside, 16), block), :] = units


def hidden_units(rows_in, gain, wg, wu, blocks, aside):
    pieces, rows, lanes = rows_in.shape
    width, units = wg.shape
    block = rows // blocks
    return pl.pallas_call(
        hidden_kernel,
        grid=(blocks,),
        in_specs=[
            pl.BlockSpec((pieces, block, lanes), lambda i: (0, i, 0)),
            pl.BlockSpec((1, width), lambda i: (0, 0)),
            pl.BlockSpec(memory_space=pltpu.VMEM),
            pl.BlockSpec(memory_space=pltpu.VMEM),
        ],
        out_specs=[
            pl.BlockSpec((aside, units), lambda i: (0, 0)),
            pl.BlockSpec((rows - aside, units), lambda i: (0, 0)),
        ],
        out_shape=(
            jax.ShapeDtypeStruct((aside, units), BF16),
            jax.ShapeDtypeStruct((rows - aside, units), BF16),
        ),
        name="hidden",
    )(rows_in, gain, near(wg), near(wu))


def side_hidden_kernel(one, gain, wg, wu, sg, su, out):
    width, units = wg.shape
    few = sg.shape[1]
    slots = out.shape[0] - FOLDED
    rows = normed_rows([one[t] for t in range(one.shape[0])], width, gain)
    out[0:slots, :] = gated_units(rows[0:slots, :], wg[...], wu[...])
    shared = gated_units(rows[slots:, :], sg[...], su[...])
    parts = [shared[j * FOLDED : (j + 1) * FOLDED, :].astype(F32) for j in range(units // few)]
    out[slots:, :] = jnp.concatenate(parts, axis=1).astype(BF16)


def side_hidden(one, gain, wg, wu, sg, su, tok_rows):
    slots = one.shape[1] - tok_rows
    return pl.pallas_call(
        side_hidden_kernel,
        out_shape=jax.ShapeDtypeStruct((slots + FOLDED, wg.shape[1]), BF16),
        name="side_hidden",
    )(one, gain, wg, wu, sg, su)


def side_down_kernel(one, two, wd, sh_down, out, shared_out):
    peers, rows, units = one.shape
    slots = rows - FOLDED
    few = sh_down.shape[0] // peers
    folds = units // few
    whole = jnp.concatenate([one[t, 0:slots, :] for t in range(peers)], axis=1)
    out[0:slots, :] = jnp.dot(whole, wd[...], preferred_element_type=F32).astype(BF16)
    whole = jnp.concatenate([two[t] for t in range(peers)], axis=1)
    out[slots:, :] = jnp.dot(whole, wd[...], preferred_element_type=F32).astype(BF16)
    shape = (folds * FOLDED, units)
    own = lax.broadcasted_iota(jnp.int32, shape, 0) // FOLDED == lax.broadcasted_iota(jnp.int32, shape, 1) // few
    shared = jnp.zeros(shared_out.shape, F32)
    for t in range(peers):
        packed = one[t, slots:, :].astype(F32)
        spread = jnp.where(own, jnp.concatenate([packed] * folds, axis=0), 0.0).astype(BF16)
        weights = jnp.concatenate([sh_down[t * few : (t + 1) * few, :]] * folds, axis=0)
        shared = shared + jnp.dot(spread, weights, preferred_element_type=F32)
    shared_out[...] = shared


def side_down(one, two, wd, sh_down, tok_rows):
    slots = one.shape[1] - FOLDED + two.shape[1]
    return pl.pallas_call(
        side_down_kernel,
        out_shape=(
            jax.ShapeDtypeStruct((slots, wd.shape[1]), BF16),
            jax.ShapeDtypeStruct((tok_rows, wd.shape[1]), F32),
        ),
        name="side_down",
    )(one, two, wd, sh_down)


def down_kernel(hidden, wd, aside, out):
    slots = aside.shape[0]
    block = hidden.shape[1]
    step = pl.program_id(0)

    @pl.when(step == 0)
    def _():
        out[0:slots, :] = aside[...]

    whole = jnp.concatenate([hidden[t] for t in range(hidden.shape[0])], axis=1)
    at = pl.ds(pl.multiple_of(slots + step * block, 16), block)
    out[at, :] = jnp.dot(whole, wd[...], preferred_element_type=F32).astype(BF16)


def down(hidden, wd, aside, blocks):
    pieces, rows, units = hidden.shape
    block = rows // blocks
    total = (aside.shape[0] + rows, wd.shape[1])
    return pl.pallas_call(
        down_kernel,
        grid=(blocks,),
        in_specs=[
            pl.BlockSpec((pieces, block, units), lambda i: (0, i, 0)),
            pl.BlockSpec(wd.shape, lambda i: (0, 0)),
            pl.BlockSpec(aside.shape, lambda i: (0, 0)),
        ],
        out_specs=pl.BlockSpec(total, lambda i: (0, 0)),
        out_shape=jax.ShapeDtypeStruct(total, BF16),
        name="down",
    )(hidden, wd, aside)


def combine_kernel(returned, table, middle, shared, out):
    total = middle[...].astype(F32) + shared[...]
    rows = returned[...]
    for n in range(table.shape[0]):
        total = total + jnp.dot(table[n], rows, preferred_element_type=F32)
    out[...] = total.astype(BF16)


def combine(returned, table, middle, shared):
    return pl.pallas_call(
        combine_kernel,
        out_shape=jax.ShapeDtypeStruct(middle.shape, BF16),
        name="combine",
    )(near(returned), near(table), middle, shared)


def body(
    resid,
    a_val,
    a_gate,
    conv_kernel,
    conv_bias,
    ln_gain,
    ln_bias,
    w_out,
    ffn_gain,
    routes,
    route_weights,
    exp_gate,
    exp_up,
    exp_down,
    sh_gate,
    sh_up,
    sh_down,
):
    tp_count = lax.axis_size("tp")
    tp_place = lax.axis_index("tp")
    sp_count = lax.axis_size("sp")
    tok_rows, model_width = resid.shape
    col_width = model_width // tp_count
    span = conv_kernel.shape[0]
    top_count = routes.shape[1]
    experts_all = exp_gate.shape[0] * sp_count
    capacity = max(2 * tok_rows * top_count // experts_all, tp_count)
    slot_count = experts_all * capacity

    halo = span - 1
    late_val, late_gate = a_val[tok_rows - halo :].astype(F32), a_gate[tok_rows - halo :].astype(F32)
    pairs = [(i, i + 1) for i in range(sp_count - 1)]
    before = lax.ppermute((late_val * jax.nn.sigmoid(late_gate)).astype(BF16), "sp", pairs)

    vectors = [v[None, :] for v in (conv_bias, ln_gain, ln_bias)]
    packed = pack(before.T, a_val.T, a_gate.T, conv_kernel, *vectors, w_out, tp_count)
    spread = lax.all_to_all(packed, "tp", split_axis=0, concat_axis=0, tiled=True)

    routes_late, _ = lax.optimization_barrier((routes, packed[0, :1]))
    slots, pick = routing(routes_late, capacity, slot_count)

    resid_cols = lax.dynamic_slice_in_dim(resid, tp_place * col_width, col_width, 1)
    middle, send = front(span, spread, resid_cols, pick)

    landed = lax.all_to_all(
        send.reshape(sp_count, slot_count // sp_count, col_width),
        "sp",
        split_axis=0,
        concat_axis=0,
        tiled=True,
    ).reshape(slot_count, col_width)
    slots_late, weights_late, _ = lax.optimization_barrier((slots, route_weights, middle[:1]))
    table = weight_table(slots_late, weights_late, slot_count)
    landed, table = lax.optimization_barrier((landed, table))
    first = ASIDE[0]
    gain = ffn_gain[None, :]
    experts = (gain, exp_gate[0], exp_up[0])
    arrived = lax.all_gather(landed[first:], "tp")
    one = lax.all_gather(jnp.concatenate([landed[:first], middle], axis=0), "tp")
    one = side_hidden(one, *experts, sh_gate, sh_up, tok_rows)
    arrived, one = lax.optimization_barrier((arrived, one))
    two, hidden = hidden_units(arrived, *experts, 2, ASIDE[1])

    hidden_all = lax.all_gather(hidden, "tp")
    one, two = lax.optimization_barrier((one, two))
    side_out, shared = side_down(
        lax.all_gather(one, "tp"), lax.all_gather(two, "tp"), exp_down[0], sh_down, tok_rows
    )
    hidden_all, side_out = lax.optimization_barrier((hidden_all, side_out))
    expert_out = down(hidden_all, exp_down[0], side_out, 3)
    returned = lax.all_to_all(
        expert_out.reshape(sp_count, slot_count // sp_count, col_width),
        "sp",
        split_axis=0,
        concat_axis=0,
        tiled=True,
    ).reshape(slot_count, col_width)
    return combine(returned, table, middle, shared)


def solution(mesh):
    in_specs = (
        P("sp", None),
        P("sp", "tp"),
        P("sp", "tp"),
        P(None, "tp"),
        P("tp"),
        P("tp"),
        P("tp"),
        P("tp", None),
        P(),
        P("sp", None),
        P("sp", None),
        P("sp", None, "tp"),
        P("sp", None, "tp"),
        P("sp", None, "tp"),
        P(None, "tp"),
        P(None, "tp"),
        P(None, "tp"),
    )
    out_specs = P("sp", "tp")
    return jax.shard_map(body, mesh=mesh, in_specs=in_specs, out_specs=out_specs, check_vma=False)
```

```python
import jax
import jax.numpy as jnp
from jax import lax
from jax.experimental import pallas as pl
from jax.experimental.pallas import tpu as pltpu
from jax.sharding import PartitionSpec as P

LN_EPS = 1e-05
RMS_EPS = 1e-06
LANES = 128
F32 = jnp.float32
BF16 = jnp.bfloat16


def near(v):
    return pltpu.with_memory_space_constraint(v, pltpu.VMEM)


def silu(v):
    return v / (1.0 + jnp.exp(-v))


def pack_kernel(before, a_val, a_gate, taps, bias, gain, shift, w_out, out, win, params, wide):
    peers, _, lanes = out.shape
    half, halo = before.shape
    tok_rows = a_val.shape[1]
    rows = win.shape[0]
    win[...] = jnp.zeros(win.shape, F32)
    params[...] = jnp.zeros(params.shape, F32)
    gate = 1.0 / (1.0 + jnp.exp(-a_gate[...].astype(F32)))
    wide[...] = jnp.zeros(wide.shape, F32)
    wide[:, 0:halo] = before[...].astype(F32)
    win[0:halo, :] = wide[...].T[0:halo, :]
    win[halo : halo + tok_rows, :] = (a_val[...].astype(F32) * gate).T
    span = taps.shape[0]
    params[0:span, :] = taps[...].astype(F32)
    for n, vector in enumerate((bias, gain, shift)):
        rest = vector[...]
        for part in range(3):
            kept = rest.astype(BF16).astype(F32)
            at = span + 3 * n + part
            params[at : at + 1, :] = kept
            rest = rest - kept

    def folded(v):
        n = v.shape[0] // 2
        return jnp.concatenate([v[0:n, :], v[n : 2 * n, :]], axis=1).astype(BF16)

    head, tail = folded(win[...]), folded(params[...])
    top = rows // 2
    low = top + tail.shape[0]
    for t in range(peers):
        out[t, 0:top, :] = head
        out[t, top:low, :] = tail
        out[t, low : low + w_out.shape[0], :] = w_out[:, t * lanes : (t + 1) * lanes]


PARAM_ROWS = 64
FOLDED = 16
ASIDE = (96, 112)


def window_rows(span, tok_rows):
    return -(-(span - 1 + tok_rows) // 32) * 32


def pack(before, a_val, a_gate, taps, bias, gain, shift, w_out, peers):
    half, tok_rows = a_val.shape
    rows = window_rows(taps.shape[0], tok_rows)
    lanes = w_out.shape[1] // peers
    total = rows // 2 + PARAM_ROWS // 2 + w_out.shape[0]
    return pl.pallas_call(
        pack_kernel,
        out_shape=jax.ShapeDtypeStruct((peers, total, lanes), BF16),
        scratch_shapes=[
            pltpu.VMEM((rows, half), F32),
            pltpu.VMEM((PARAM_ROWS, half), F32),
            pltpu.VMEM((half, LANES), F32),
        ],
        name="pack",
    )(near(before), a_val, a_gate, taps, bias, gain, shift, w_out)


def routing_kernel(capacity, routes, slots_out, pick_out):
    tok_rows, top_count = routes.shape
    slot_count = pick_out.shape[0]
    experts = slot_count // capacity
    ids = lax.broadcasted_iota(jnp.int32, (tok_rows, experts), 1)
    hits = [ids == routes[:, k : k + 1] for k in range(top_count)]
    named = sum(jnp.where(h, 1.0, 0.0) for h in hits).astype(BF16)
    square = (tok_rows, tok_rows)
    below = lax.broadcasted_iota(jnp.int32, square, 0) > lax.broadcasted_iota(jnp.int32, square, 1)
    earlier = jnp.dot(jnp.where(below, 1.0, 0.0).astype(BF16), named, preferred_element_type=F32)
    wide = lax.broadcasted_iota(jnp.int32, (tok_rows, slot_count), 1)
    lane = lax.broadcasted_iota(jnp.int32, slots_out.shape, 1)
    slots = jnp.zeros(slots_out.shape, jnp.int32)
    pick = jnp.zeros(wide.shape, F32)
    for k in range(top_count):
        place = jnp.sum(jnp.where(hits[k], earlier, 0.0), axis=1, keepdims=True).astype(jnp.int32)
        slot = routes[:, k : k + 1] * capacity + place
        slots = jnp.where(lane == k, slot, slots)
        pick = jnp.where(wide == slot, 1.0, pick)
    slots_out[...] = slots
    for at in range(0, slot_count, tok_rows):
        pick_out[at : at + tok_rows, :] = pick[:, at : at + tok_rows].T.astype(BF16)


def routing(routes, capacity, slot_count):
    tok_rows, top_count = routes.shape

    def kernel(*refs):
        routing_kernel(capacity, *refs)

    return pl.pallas_call(
        kernel,
        out_shape=(
            jax.ShapeDtypeStruct((tok_rows, top_count), jnp.int32),
            jax.ShapeDtypeStruct((slot_count, tok_rows), BF16),
        ),
        name="routing",
    )(routes)


def table_kernel(slots, weights, out):
    shape = out.shape[1:]
    ids = lax.broadcasted_iota(jnp.int32, shape, 1)
    table = jnp.zeros(shape, F32)
    for k in range(slots.shape[1]):
        table = jnp.where(ids == slots[:, k : k + 1], weights[:, k : k + 1], table)
    for n in range(out.shape[0]):
        part = table.astype(BF16)
        out[n] = part
        table = table - part.astype(F32)


def weight_table(slots, weights, slot_count):
    return pl.pallas_call(
        table_kernel,
        out_shape=jax.ShapeDtypeStruct((3, slots.shape[0], slot_count), BF16),
        name="table",
    )(slots, weights)


def front_kernel(span, packed, resid, pick, middle_out, send_out, win, params, conv):
    peers = packed.shape[0]
    tok_rows = resid.shape[0]
    half = LANES // 2
    channels = peers * half
    top = win.shape[1] // 2
    fold = PARAM_ROWS // 2
    for pair in range(peers // 2):
        at = slice(pair * LANES, (pair + 1) * LANES)
        one, two = packed[2 * pair, 0 : top + fold, :], packed[2 * pair + 1, 0 : top + fold, :]
        left = jnp.concatenate([one[:, :half], two[:, :half]], axis=1).astype(F32)
        right = jnp.concatenate([one[:, half:], two[:, half:]], axis=1).astype(F32)
        win[pair, 0:top, :], win[pair, top : 2 * top, :] = left[0:top], right[0:top]
        params[0:fold, at], params[fold : 2 * fold, at] = left[top:], right[top:]

    def vector(first, cols=slice(None)):
        return sum(params[first + i : first + i + 1, cols] for i in range(3))

    conv_rows = tok_rows

    def one_block(i, _):
        cols = pl.ds(pl.multiple_of(i * LANES, LANES), LANES)
        taps = params[0:span, cols]
        b = vector(span, cols)
        for r in range(0, tok_rows, conv_rows):
            acc = jnp.broadcast_to(b, (conv_rows, LANES))
            for j in range(span):
                acc = acc + taps[j : j + 1, :] * win[i, r + j : r + j + conv_rows, :]
            conv[r : r + conv_rows, cols] = acc
        return 0

    lax.fori_loop(0, channels // LANES, one_block, 0)
    gain = vector(span + 3)
    shift = vector(span + 6)
    wcol = packed[:, top + fold :, :].reshape(channels, packed.shape[2])
    for r in range(0, tok_rows, 64):
        c = conv[r : r + 64, :]
        mean = jnp.sum(c, axis=1, keepdims=True) * (1.0 / channels)
        var = jnp.sum(c * c, axis=1, keepdims=True) * (1.0 / channels) - mean * mean
        scaled = (c - mean) * lax.rsqrt(var + LN_EPS) * gain + shift
        mixed = silu(scaled).astype(BF16)
        proj = jnp.dot(mixed, wcol, preferred_element_type=F32)
        middle_out[r : r + 64, :] = (resid[r : r + 64, :].astype(F32) + proj).astype(BF16)
    middle = middle_out[...]
    send_out[...] = jnp.dot(pick[...], middle, preferred_element_type=F32).astype(BF16)


def front(span, packed, resid, pick):
    tok_rows, cols = resid.shape
    channels = packed.shape[0] * LANES // 2

    def kernel(*refs):
        front_kernel(span, *refs)

    return pl.pallas_call(
        kernel,
        out_shape=(
            jax.ShapeDtypeStruct((tok_rows, cols), BF16),
            jax.ShapeDtypeStruct((pick.shape[0], cols), BF16),
        ),
        scratch_shapes=[
            pltpu.VMEM((channels // LANES, window_rows(span, tok_rows), LANES), F32),
            pltpu.VMEM((PARAM_ROWS, channels), F32),
            pltpu.VMEM((tok_rows, channels), F32),
        ],
        name="front",
    )(near(packed), resid, pick)


def normed_rows(pieces, width, gain):
    squares = jnp.zeros(pieces[0].shape, F32)
    for x in pieces:
        squares = squares + x.astype(F32) * x.astype(F32)
    mean = jnp.sum(squares, axis=1, keepdims=True) / width
    inverse = lax.rsqrt(mean + RMS_EPS)
    cols = [gain[:, n * LANES : (n + 1) * LANES] for n in range(len(pieces))]
    scaled = [(x.astype(F32) * inverse * c).astype(BF16) for x, c in zip(pieces, cols)]
    return jnp.concatenate(scaled, axis=1)


def gated_units(rows, w_gate, w_up):
    g = jnp.dot(rows, w_gate, preferred_element_type=F32)
    u = jnp.dot(rows, w_up, preferred_element_type=F32)
    return (silu(g) * u).astype(BF16)


def hidden_kernel(rows_in, gain, wg, wu, aside_out, out):
    step = pl.program_id(0)
    block = rows_in.shape[1]
    aside = aside_out.shape[0]
    rows = normed_rows([rows_in[t] for t in range(rows_in.shape[0])], wg.shape[0], gain)
    units = gated_units(rows, wg[...], wu[...])

    @pl.when(step == 0)
    def _():
        aside_out[...] = units[0:aside, :]
        out[0 : block - aside, :] = units[aside:, :]

    @pl.when(step > 0)
    def _():
        out[pl.ds(pl.multiple_of(step * block - aside, 16), block), :] = units


def hidden_units(rows_in, gain, wg, wu, blocks, aside):
    pieces, rows, lanes = rows_in.shape
    width, units = wg.shape
    block = rows // blocks
    return pl.pallas_call(
        hidden_kernel,
        grid=(blocks,),
        in_specs=[
            pl.BlockSpec((pieces, block, lanes), lambda i: (0, i, 0)),
            pl.BlockSpec((1, width), lambda i: (0, 0)),
            pl.BlockSpec(memory_space=pltpu.VMEM),
            pl.BlockSpec(memory_space=pltpu.VMEM),
        ],
        out_specs=[
            pl.BlockSpec((aside, units), lambda i: (0, 0)),
            pl.BlockSpec((rows - aside, units), lambda i: (0, 0)),
        ],
        out_shape=(
            jax.ShapeDtypeStruct((aside, units), BF16),
            jax.ShapeDtypeStruct((rows - aside, units), BF16),
        ),
        name="hidden",
    )(rows_in, gain, near(wg), near(wu))


def side_hidden_kernel(one, gain, wg, wu, sg, su, out):
    width, units = wg.shape
    few = sg.shape[1]
    slots = out.shape[0] - FOLDED
    rows = normed_rows([one[t] for t in range(one.shape[0])], width, gain)
    out[0:slots, :] = gated_units(rows[0:slots, :], wg[...], wu[...])
    shared = gated_units(rows[slots:, :], sg[...], su[...])
    parts = [shared[j * FOLDED : (j + 1) * FOLDED, :].astype(F32) for j in range(units // few)]
    out[slots:, :] = jnp.concatenate(parts, axis=1).astype(BF16)


def side_hidden(one, gain, wg, wu, sg, su, tok_rows):
    slots = one.shape[1] - tok_rows
    return pl.pallas_call(
        side_hidden_kernel,
        out_shape=jax.ShapeDtypeStruct((slots + FOLDED, wg.shape[1]), BF16),
        name="side_hidden",
    )(one, gain, wg, wu, sg, su)


def side_down_kernel(one, two, wd, sh_down, out, shared_out):
    peers, rows, units = one.shape
    slots = rows - FOLDED
    few = sh_down.shape[0] // peers
    folds = units // few
    whole = jnp.concatenate([one[t, 0:slots, :] for t in range(peers)], axis=1)
    out[0:slots, :] = jnp.dot(whole, wd[...], preferred_element_type=F32).astype(BF16)
    whole = jnp.concatenate([two[t] for t in range(peers)], axis=1)
    out[slots:, :] = jnp.dot(whole, wd[...], preferred_element_type=F32).astype(BF16)
    shape = (folds * FOLDED, units)
    own = lax.broadcasted_iota(jnp.int32, shape, 0) // FOLDED == lax.broadcasted_iota(jnp.int32, shape, 1) // few
    shared = jnp.zeros(shared_out.shape, F32)
    for t in range(peers):
        packed = one[t, slots:, :].astype(F32)
        spread = jnp.where(own, jnp.concatenate([packed] * folds, axis=0), 0.0).astype(BF16)
        weights = jnp.concatenate([sh_down[t * few : (t + 1) * few, :]] * folds, axis=0)
        shared = shared + jnp.dot(spread, weights, preferred_element_type=F32)
    shared_out[...] = shared


def side_down(one, two, wd, sh_down, tok_rows):
    slots = one.shape[1] - FOLDED + two.shape[1]
    return pl.pallas_call(
        side_down_kernel,
        out_shape=(
            jax.ShapeDtypeStruct((slots, wd.shape[1]), BF16),
            jax.ShapeDtypeStruct((tok_rows, wd.shape[1]), F32),
        ),
        name="side_down",
    )(one, two, wd, sh_down)


def down_kernel(hidden, wd, aside, out):
    slots = aside.shape[0]
    block = hidden.shape[1]
    step = pl.program_id(0)

    @pl.when(step == 0)
    def _():
        out[0:slots, :] = aside[...]

    whole = jnp.concatenate([hidden[t] for t in range(hidden.shape[0])], axis=1)
    at = pl.ds(pl.multiple_of(slots + step * block, 16), block)
    out[at, :] = jnp.dot(whole, wd[...], preferred_element_type=F32).astype(BF16)


def down(hidden, wd, aside, blocks):
    pieces, rows, units = hidden.shape
    block = rows // blocks
    total = (aside.shape[0] + rows, wd.shape[1])
    return pl.pallas_call(
        down_kernel,
        grid=(blocks,),
        in_specs=[
            pl.BlockSpec((pieces, block, units), lambda i: (0, i, 0)),
            pl.BlockSpec(wd.shape, lambda i: (0, 0)),
            pl.BlockSpec(aside.shape, lambda i: (0, 0)),
        ],
        out_specs=pl.BlockSpec(total, lambda i: (0, 0)),
        out_shape=jax.ShapeDtypeStruct(total, BF16),
        name="down",
    )(hidden, wd, aside)


def combine_kernel(returned, table, middle, shared, out):
    total = middle[...].astype(F32) + shared[...]
    rows = returned[...]
    for n in range(table.shape[0]):
        total = total + jnp.dot(table[n], rows, preferred_element_type=F32)
    out[...] = total.astype(BF16)


def combine(returned, table, middle, shared):
    return pl.pallas_call(
        combine_kernel,
        out_shape=jax.ShapeDtypeStruct(middle.shape, BF16),
        name="combine",
    )(near(returned), near(table), middle, shared)


def body(
    resid,
    a_val,
    a_gate,
    conv_kernel,
    conv_bias,
    ln_gain,
    ln_bias,
    w_out,
    ffn_gain,
    routes,
    route_weights,
    exp_gate,
    exp_up,
    exp_down,
    sh_gate,
    sh_up,
    sh_down,
):
    tp_count = lax.axis_size("tp")
    tp_place = lax.axis_index("tp")
    sp_count = lax.axis_size("sp")
    tok_rows, model_width = resid.shape
    col_width = model_width // tp_count
    span = conv_kernel.shape[0]
    top_count = routes.shape[1]
    experts_all = exp_gate.shape[0] * sp_count
    capacity = max(2 * tok_rows * top_count // experts_all, tp_count)
    slot_count = experts_all * capacity

    halo = span - 1
    late_val, late_gate = a_val[tok_rows - halo :].astype(F32), a_gate[tok_rows - halo :].astype(F32)
    pairs = [(i, i + 1) for i in range(sp_count - 1)]
    before = lax.ppermute((late_val * jax.nn.sigmoid(late_gate)).astype(BF16), "sp", pairs)

    vectors = [v[None, :] for v in (conv_bias, ln_gain, ln_bias)]
    packed = pack(before.T, a_val.T, a_gate.T, conv_kernel, *vectors, w_out, tp_count)
    spread = lax.all_to_all(packed, "tp", split_axis=0, concat_axis=0, tiled=True)

    routes_late, _ = lax.optimization_barrier((routes, packed[0, :1]))
    slots, pick = routing(routes_late, capacity, slot_count)

    resid_cols = lax.dynamic_slice_in_dim(resid, tp_place * col_width, col_width, 1)
    middle, send = front(span, spread, resid_cols, pick)

    landed = lax.all_to_all(
        send.reshape(sp_count, slot_count // sp_count, col_width),
        "sp",
        split_axis=0,
        concat_axis=0,
        tiled=True,
    ).reshape(slot_count, col_width)
    slots_late, weights_late, _ = lax.optimization_barrier((slots, route_weights, middle[:1]))
    table = weight_table(slots_late, weights_late, slot_count)
    landed, table = lax.optimization_barrier((landed, table))
    first = ASIDE[0]
    gain = ffn_gain[None, :]
    experts = (gain, exp_gate[0], exp_up[0])
    arrived = lax.all_gather(landed[first:], "tp")
    one = lax.all_gather(jnp.concatenate([landed[:first], middle], axis=0), "tp")
    one = side_hidden(one, *experts, sh_gate, sh_up, tok_rows)
    arrived, one = lax.optimization_barrier((arrived, one))
    two, hidden = hidden_units(arrived, *experts, 2, ASIDE[1])

    hidden_all = lax.all_gather(hidden, "tp")
    one, two = lax.optimization_barrier((one, two))
    side_out, shared = side_down(
        lax.all_gather(one, "tp"), lax.all_gather(two, "tp"), exp_down[0], sh_down, tok_rows
    )
    hidden_all, side_out = lax.optimization_barrier((hidden_all, side_out))
    expert_out = down(hidden_all, exp_down[0], side_out, 3)
    returned = lax.all_to_all(
        expert_out.reshape(sp_count, slot_count // sp_count, col_width),
        "sp",
        split_axis=0,
        concat_axis=0,
        tiled=True,
    ).reshape(slot_count, col_width)
    return combine(returned, table, middle, shared)


def solution(mesh):
    in_specs = (
        P("sp", None),
        P("sp", "tp"),
        P("sp", "tp"),
        P(None, "tp"),
        P("tp"),
        P("tp"),
        P("tp"),
        P("tp", None),
        P(),
        P("sp", None),
        P("sp", None),
        P("sp", None, "tp"),
        P("sp", None, "tp"),
        P("sp", None, "tp"),
        P(None, "tp"),
        P(None, "tp"),
        P(None, "tp"),
    )
    out_specs = P("sp", "tp")
    return jax.shard_map(body, mesh=mesh, in_specs=in_specs, out_specs=out_specs, check_vma=False)
```
